512 devices in a mesh: sp: 64 (over z, y), fs: 4 (over x), tp: 2 (over core).
Axes of the slice: x: 4, y: 8, z: 8, core: 2. Of those that a mesh axis runs over, the one named last changes fastest.
Arguments:
- tokens: bfloat16 [4, 16384, 2048], P('fs', 'sp', 'tp'), may hold values from -6 to 6
- norm_gain: float32 [2048], replicated, may hold values from 0.1 to 1.9
- ret_query: bfloat16 [2048, 1024], P('sp', 'tp'), may hold values from -0.125 to 0.125
- ret_key: bfloat16 [2048, 1024], P('sp', 'tp'), may hold values from -0.125 to 0.125
- ret_value: bfloat16 [2048, 1024], P('sp', 'tp'), may hold values from -0.125 to 0.125
- att_query: bfloat16 [2048, 1024], P('sp', 'tp'), may hold values from -0.125 to 0.125
- att_key: bfloat16 [2048, 256], P('sp', 'tp'), may hold values from -0.125 to 0.125
- att_value: bfloat16 [2048, 256], P('sp', 'tp'), may hold values from -0.125 to 0.125
- log_decay: float32 [4, 4, 16384], P('fs', 'tp', 'sp'), may hold values from -1 to 0
- start_state: float32 [4, 4, 256, 256], P('fs', 'tp'), may hold values from -12 to 12
- ret_gain: float32 [1024], P('tp'), may hold values from 0.1 to 1.9
- sink_logits: float32 [16], P('tp'), may hold values from 1 to 5
- ret_out: bfloat16 [1024, 2048], P('tp', 'fs'), may hold values from -0.1875 to 0.1875
- att_out: bfloat16 [1024, 2048], P('tp', 'fs'), may hold values from -1.5 to 1.5
Outputs:
- mixed: bfloat16 [4, 16384, 2048], P('fs', 'sp', 'tp')
The draws below stay inside these ranges and needn't reach their ends.
All inputs are finite; a program needn't handle non-finite values.
Results may differ from the reference program's by a relative error of at most 0.015.
Values may be sent and summed in bfloat16 or wider, within the bound.
A program may use at most 128 MiB of HBM per device.

```python
import jax
import jax.numpy as jnp
from jax import lax

D = 2048
RETENTION_HEADS = 4
DK = 256
DV = 256
AQH = 16
AKH = 4
HD = 64
WINDOW = 128
BLOCK = 128
TOK_DEV = 256
SEQUENCE_COUNT = 4
SEQUENCE_LENGTH = 16384
N_TP = 2


def draw_log_decay(key, part):
    random_subkeys = jax.random.split(jax.random.fold_in(key, 17), 5)
    blocks = SEQUENCE_LENGTH // TOK_DEV
    ranking = jax.vmap(lambda inner: jax.random.permutation(inner, RETENTION_HEADS))(jax.random.split(random_subkeys[0], SEQUENCE_COUNT))
    fast_heads = (ranking < RETENTION_HEADS // 2).astype(jnp.float32)
    baseline_decay = fast_heads * (3.0 / BLOCK) + (1.0 - fast_heads) * (1.0 / SEQUENCE_LENGTH)
    noise_spread = jax.random.uniform(random_subkeys[1], (SEQUENCE_COUNT, RETENTION_HEADS, blocks), jnp.float32, 0.4, 1.2)
    noise_spread = jnp.repeat(noise_spread, TOK_DEV, axis=-1)
    random_noise = jax.random.uniform(random_subkeys[2], (SEQUENCE_COUNT, RETENTION_HEADS, SEQUENCE_LENGTH), jnp.float32, 0.5, 1.5)
    spike_position = jax.random.randint(random_subkeys[3], (SEQUENCE_COUNT, RETENTION_HEADS, 2), 0, SEQUENCE_LENGTH)
    spike_magnitude = jax.random.uniform(random_subkeys[4], (SEQUENCE_COUNT, RETENTION_HEADS, 2), jnp.float32, 0.2, 0.4)
    position_list = jnp.arange(SEQUENCE_LENGTH, dtype=jnp.int32)
    spike_events = jnp.sum(jnp.where(position_list[None, None, None, :] == spike_position[..., None], jnp.log(1.0 - spike_magnitude)[..., None], 0.0), axis=2)
    return (-baseline_decay[..., None] * noise_spread * random_noise + spike_events).astype(jnp.float32)


def levels(rng, dims, cuts, smallest, high):
    level, own = 1.0, jax.random.fold_in(rng, 6)
    for axis_at, blocks in cuts:
        heights = jnp.exp(jax.random.uniform(jax.random.fold_in(own, axis_at), (blocks,), jnp.float32, smallest / len(cuts), high / len(cuts)))
        level = level * jnp.repeat(heights, dims[axis_at] // blocks).reshape([-1 if axis == axis_at else 1 for axis in range(len(dims))])
    return level


def gaussian(stream_key, dims, deviation, bound, cuts=(), kind=jnp.bfloat16):
    drawn = jax.random.normal(stream_key, dims, jnp.float32) * deviation
    if len(cuts) > 0:
        drawn = levels(stream_key, dims, cuts, -0.22, 0.18) * drawn
    return jnp.clip(drawn, min=-bound, max=bound).astype(kind)


def setup_inputs(seed: int = 0) -> dict:
    key_of = jax.random.split(jax.random.key(seed), 15)
    return {
        "tokens": gaussian(key_of[0], (SEQUENCE_COUNT, SEQUENCE_LENGTH, D), 1.0, 6.0, ((0, 4), (1, 64), (2, 2))),
        "norm_gain": jnp.clip(1.0 + 0.18 * jax.random.normal(key_of[1], (D,), jnp.float32), 0.1, 1.9),
        "ret_query": gaussian(key_of[2], (D, RETENTION_HEADS * DK), D ** -0.5, 0.125, ((0, 64), (1, 2))),
        "ret_key": gaussian(key_of[3], (D, RETENTION_HEADS * DK), D ** -0.5, 0.125, ((0, 64), (1, 2))),
        "ret_value": gaussian(key_of[4], (D, RETENTION_HEADS * DV), D ** -0.5, 0.125, ((0, 64), (1, 2))),
        "att_query": gaussian(key_of[5], (D, AQH * HD), D ** -0.5, 0.125, ((0, 64), (1, 2))),
        "att_key": gaussian(key_of[6], (D, AKH * HD), D ** -0.5, 0.125, ((0, 64), (1, 2))),
        "att_value": gaussian(key_of[7], (D, AKH * HD), D ** -0.5, 0.125, ((0, 64), (1, 2))),
        "log_decay": draw_log_decay(jax.random.fold_in(key_of[14], 71), 0),
        "start_state": gaussian(key_of[9], (SEQUENCE_COUNT, RETENTION_HEADS, DK, DV), (2 * (TOK_DEV // DK) ** 0.5), 12.0, ((0, 4), (1, 2)), jnp.float32),
        "ret_gain": jnp.clip(1.0 + 0.18 * jax.random.normal(key_of[10], (RETENTION_HEADS * DV,), jnp.float32), 0.1, 1.9),
        "sink_logits": jnp.clip(1.0 + 4.0 * jax.random.uniform(key_of[11], (AQH,), jnp.float32) ** levels(key_of[11], (AQH,), ((0, 2),), -0.2, 0.2), 1.0, 5.0),
        "ret_out": gaussian(key_of[12], (RETENTION_HEADS * DV, D), (RETENTION_HEADS * DV) ** -0.5, 0.1875, ((0, 2), (1, 4))),
        "att_out": gaussian(key_of[13], (AQH * HD, D), (AQH * HD // 64) ** -0.5, 1.5, ((0, 2), (1, 4))),
    }


epsilon = 1e-06
exact_result = lax.Precision.HIGHEST

def rotate(values, positions):
    half_dim = values.shape[-1] // 2
    inverse = 1.0 / 10000.0 ** (jnp.arange(half_dim, dtype=jnp.float32) / half_dim)
    angles = positions.astype(jnp.float32)[:, None] * inverse[None, :]
    cosine = jnp.cos(angles)[:, None, :]
    sine_table = jnp.sin(angles)[:, None, :]
    front_half = values[..., :half_dim]
    back_half = values[..., half_dim:]
    return jnp.concatenate([front_half * cosine - back_half * sine_table, front_half * sine_table + back_half * cosine], axis=-1)

def block_step(memory_state, inputs):
    queries, key_matrix_rows, value_matrix_rows, log_rates = inputs
    length_here = log_rates.shape[-1]
    causal = jnp.arange(length_here)[:, None] >= jnp.arange(length_here)[None, :]
    running_totals = jnp.cumsum(log_rates, axis=-1)
    relative = running_totals[:, :, None] - running_totals[:, None, :]
    weight = jnp.where(causal[None], jnp.exp(jnp.where(causal[None], relative, 0.0)), 0.0)
    score_matrix = jnp.einsum('hqd,hkd->hqk', queries, key_matrix_rows, precision=exact_result) * weight
    carried_state = jnp.einsum('hqd,hdv->hqv', queries * jnp.exp(running_totals)[:, :, None], memory_state, precision=exact_result)
    output_rows = jnp.einsum('arf,afu->aru', score_matrix, value_matrix_rows, precision=exact_result) + carried_state
    decay_factors = jnp.exp(running_totals[:, -1:] - running_totals)
    memory_state = memory_state * jnp.exp(running_totals[:, -1])[:, None, None] + jnp.einsum('iwj,iwe->ije', key_matrix_rows * decay_factors[:, :, None], value_matrix_rows, precision=exact_result)
    return (memory_state, output_rows)

def reference(tokens, norm_gain, ret_query, ret_key, ret_value, att_query, att_key, att_value, log_decay, start_state, ret_gain, sink_logits, ret_out, att_out):

    def one_sequence(inputs):
        rows_in, decay_rows, initial = inputs
        as_float = rows_in.astype(jnp.float32)
        normed = (as_float * lax.rsqrt(lax.optimization_barrier(jnp.mean(as_float * as_float, axis=-1, keepdims=True)) + epsilon) * norm_gain).astype(jnp.bfloat16)

        def project(weights):
            return jnp.dot(normed, weights, preferred_element_type=jnp.float32).astype(jnp.bfloat16)
        ret_queries = project(ret_query)
        ret_keys = project(ret_key)
        ret_values = project(ret_value)
        att_queries = project(att_query)
        att_keys = project(att_key)
        att_values = project(att_value)
        positions = jnp.arange(SEQUENCE_LENGTH, dtype=jnp.int32)
        queries = rotate(ret_queries.astype(jnp.float32).reshape(SEQUENCE_LENGTH, RETENTION_HEADS, DK), positions)
        keys_rot = rotate(ret_keys.astype(jnp.float32).reshape(SEQUENCE_LENGTH, RETENTION_HEADS, DK), positions) * DK ** (-0.5)
        values_f = ret_values.astype(jnp.float32).reshape(SEQUENCE_LENGTH, RETENTION_HEADS, DV)
        count = SEQUENCE_LENGTH // BLOCK

        def blocked(array):
            return array.reshape(count, BLOCK, RETENTION_HEADS, array.shape[-1]).transpose(0, 2, 1, 3)
        log_rates = decay_rows.reshape(RETENTION_HEADS, count, BLOCK).transpose(1, 0, 2)
        _, pieces = lax.scan(block_step, initial, (blocked(queries), blocked(keys_rot), blocked(values_f), log_rates))
        retained = pieces.transpose(0, 2, 1, 3).reshape(SEQUENCE_LENGTH, RETENTION_HEADS, DV)
        centred = retained - lax.optimization_barrier(jnp.mean(retained, axis=-1, keepdims=True))
        variance = lax.optimization_barrier(jnp.mean(centred * centred, axis=-1, keepdims=True))
        ret_hidden = ((centred * lax.rsqrt(variance + epsilon)).reshape(SEQUENCE_LENGTH, RETENTION_HEADS * DV) * ret_gain).astype(jnp.bfloat16)
        windows = SEQUENCE_LENGTH // WINDOW
        groups = AQH // AKH
        grouped_q = att_queries.reshape(windows, WINDOW, AKH, groups, HD).astype(jnp.float32)

        def banded(array):
            blocks_now = array.reshape(windows, WINDOW, AKH, HD)
            earlier = jnp.concatenate([jnp.zeros((1, WINDOW, AKH, HD), array.dtype), blocks_now[:-1]], axis=0)
            return jnp.concatenate([earlier, blocks_now], axis=1).astype(jnp.float32)
        key_band = banded(att_keys)
        value_band = banded(att_values)
        score_matrix = jnp.einsum('nqhgd,nkhd->nhgqk', grouped_q, key_band) * HD ** (-0.5)
        query_index = WINDOW + jnp.arange(WINDOW)
        key_index = jnp.arange(2 * WINDOW)
        allowed = (key_index[None, :] <= query_index[:, None]) & (query_index[:, None] - key_index[None, :] < WINDOW)
        present = (jnp.arange(windows)[:, None] > 0) | (key_index >= WINDOW)[None, :]
        visible = (allowed[None] & present[:, None, :])[:, None, None]
        expo = jnp.exp(jnp.where(visible, score_matrix, -1e+30))
        summed = lax.optimization_barrier(jnp.sum(expo, axis=-1, keepdims=True)) + jnp.exp(sink_logits).reshape(1, AKH, groups, 1, 1)
        probs = (expo / summed).astype(jnp.bfloat16)
        att_hidden = jnp.einsum('nhgqk,nkhd->nqhgd', probs.astype(jnp.float32), value_band).astype(jnp.bfloat16).reshape(SEQUENCE_LENGTH, AQH * HD)
        ret_cols = RETENTION_HEADS * DV // N_TP
        att_cols = AQH * HD // N_TP
        mixed = jnp.zeros((SEQUENCE_LENGTH, D), jnp.float32)
        for group_index in range(N_TP):
            partial_value = jnp.dot(ret_hidden[:, group_index * ret_cols:(group_index + 1) * ret_cols], ret_out[group_index * ret_cols:(group_index + 1) * ret_cols], preferred_element_type=jnp.float32)
            partial_value = partial_value + jnp.dot(att_hidden[:, group_index * att_cols:(group_index + 1) * att_cols], att_out[group_index * att_cols:(group_index + 1) * att_cols], preferred_element_type=jnp.float32)
            rounded = lax.optimization_barrier(partial_value.astype(jnp.bfloat16))
            mixed = mixed + rounded.astype(jnp.float32)
        return mixed.astype(jnp.bfloat16)
    return lax.map(one_sequence, (tokens, log_decay, start_state))
```

```python
import jax
import jax.numpy as jnp
from jax import lax
from jax.experimental import pallas as pl
from jax.experimental.pallas import tpu as pltpu
from jax.sharding import Mesh
from jax.sharding import PartitionSpec as P

DK = 256
DV = 256
HD = 64
WINDOW = 128
BLOCK = 128
SP = ("sp_0", "sp_1")


epsilon = 1e-06


def in_order(tiles, dim):
    lengths = list(tiles.shape[1:])
    lengths[dim] *= tiles.shape[0]
    return jnp.moveaxis(tiles, 0, dim).reshape(lengths)


def from_everyone(array, axis):
    peers = lax.axis_size(axis)
    return lax.all_to_all(
        jnp.broadcast_to(array[None], (peers, *array.shape)), axis, 0, 0, tiled=True
    )


def collect(array, axis, dim):
    return in_order(from_everyone(array, axis), dim)


def place(index):
    return {"sp_0": index // 8, "sp_1": index % 8}


def prefix_kernel(own_ref, decay_ref, out_ref, came, rates, back, sems):
    me = lax.axis_index("sp_0") * 8 + lax.axis_index("sp_1")

    def spread(k, _):
        to = (me + k) % 64
        pltpu.make_async_remote_copy(
            src_ref=decay_ref.at[to // 32],
            dst_ref=rates.at[me],
            send_sem=sems.at[0],
            recv_sem=sems.at[1],
            device_id=place(to),
        ).start()
        pltpu.make_async_remote_copy(
            src_ref=own_ref.at[to],
            dst_ref=came.at[me],
            send_sem=sems.at[2],
            recv_sem=sems.at[3],
            device_id=place(to),
        ).start()
        return 0

    lax.fori_loop(1, 64, spread, 0)
    came[me] = own_ref[me]
    rates[me] = decay_ref[me // 32]
    few = pl.ds(0, 63)
    for ref, at in ((rates, 0), (rates, 1), (came, 2), (came, 3)):
        pltpu.make_async_copy(ref.at[few], ref.at[few], sems.at[at]).wait()

    def advance(k, carried):
        back[k] = carried.astype(jnp.bfloat16)
        return carried * rates[k] + came[k].astype(jnp.float32)

    lax.fori_loop(0, 64, advance, jnp.zeros((16, 128), jnp.float32))

    def give_back(k, _):
        to = (me + k) % 64
        pltpu.make_async_remote_copy(
            src_ref=back.at[to],
            dst_ref=out_ref.at[me],
            send_sem=sems.at[4],
            recv_sem=sems.at[5],
            device_id=place(to),
        ).start()
        return 0

    lax.fori_loop(1, 64, give_back, 0)
    out_ref[me] = back[me]
    for ref, at in ((back, 4), (out_ref, 5)):
        pltpu.make_async_copy(ref.at[few], ref.at[few], sems.at[at]).wait()


def state_before(decay, state):
    chunks = state.astype(jnp.bfloat16).reshape(2, 16, 16, 2, 128)
    chunks = chunks.transpose(0, 1, 3, 2, 4).reshape(64, 16, 128)
    rates = jnp.broadcast_to(decay[:, None, None], (2, 1, 128))
    vmem = pl.BlockSpec(memory_space=pltpu.VMEM)
    prefix = pl.pallas_call(
        prefix_kernel,
        out_shape=jax.ShapeDtypeStruct((64, 16, 128), jnp.bfloat16),
        in_specs=[vmem, vmem],
        out_specs=vmem,
        scratch_shapes=[
            pltpu.VMEM((64, 16, 128), jnp.bfloat16),
            pltpu.VMEM((64, 1, 128), jnp.float32),
            pltpu.VMEM((64, 16, 128), jnp.bfloat16),
            pltpu.SemaphoreType.DMA((6,)),
        ],
        compiler_params=pltpu.CompilerParams(has_side_effects=True),
    )(chunks, rates)
    prefix = prefix.reshape(2, 16, 2, 16, 128).transpose(0, 1, 3, 2, 4)
    return prefix.reshape(2, 256, 256).astype(jnp.float32)


def passed_along(block, axis, distance):
    devices = range(lax.axis_size(axis))
    route = [(i - distance, i) for i in devices if i - distance in devices]
    return lax.ppermute(block, axis, route)


def in_one_piece(arrays, axis, dim, along):
    both = jnp.concatenate(arrays, axis=along)
    filled, at, done = (lax.all_gather(both, axis, axis=dim, tiled=True), 0, [])
    for a in arrays:
        done.append(lax.slice_in_dim(filled, at, at + a.shape[along], axis=along))
        at += a.shape[along]
    return tuple(done)


def split_up(array, dim, peers):
    before, after = (array.shape[:dim], array.shape[dim + 1 :])
    return jnp.moveaxis(array.reshape(*before, peers, -1, *after), dim, 0)


def sent_and_summed(array, axis, dim):
    tiles = split_up(array, dim, lax.axis_size(axis))
    arrived = lax.all_to_all(tiles, axis, split_axis=0, concat_axis=0, tiled=True)
    return arrived.astype(jnp.float32).sum(axis=0)


def rotate(values, positions):
    half_dim = values.shape[-1] // 2
    inverse = 1.0 / 10000.0 ** (jnp.arange(half_dim, dtype=jnp.float32) / half_dim)
    angles = positions.astype(jnp.float32)[:, None] * inverse[None, :]
    cosine = jnp.cos(angles)[:, None, :]
    sine_table = jnp.sin(angles)[:, None, :]
    front_half = values[..., :half_dim]
    back_half = values[..., half_dim:]
    return jnp.concatenate(
        [
            front_half * cosine - back_half * sine_table,
            front_half * sine_table + back_half * cosine,
        ],
        axis=-1,
    )


def block_step(memory_state, inputs):
    queries, key_matrix_rows, value_matrix_rows, log_rates = inputs
    length_here = log_rates.shape[-1]
    causal = jnp.arange(length_here)[:, None] >= jnp.arange(length_here)[None, :]
    running_totals = jnp.cumsum(log_rates, axis=-1)
    relative = running_totals[:, :, None] - running_totals[:, None, :]
    weight = jnp.where(causal[None], jnp.exp(jnp.where(causal[None], relative, 0.0)), 0.0)
    score_matrix = jnp.einsum("hqd,hkd->hqk", queries, key_matrix_rows) * weight
    carried_state = jnp.einsum(
        "hqd,hdv->hqv", queries * jnp.exp(running_totals)[:, :, None], memory_state
    )
    output_rows = jnp.einsum("arf,afu->aru", score_matrix, value_matrix_rows) + carried_state
    decay_factors = jnp.exp(running_totals[:, -1:] - running_totals)
    memory_state = memory_state * jnp.exp(running_totals[:, -1])[:, None, None] + jnp.einsum(
        "iwj,iwe->ije", key_matrix_rows * decay_factors[:, :, None], value_matrix_rows
    )
    return (memory_state, output_rows)


def shards(
    tokens,
    norm_gain,
    ret_query,
    ret_key,
    ret_value,
    att_query,
    att_key,
    att_value,
    log_decay,
    start_state,
    ret_gain,
    sink_logits,
    ret_out,
    att_out,
):
    gathered = collect(tokens[0], "tp", 1)
    row_count = gathered.shape[0]
    as_float = gathered.astype(jnp.float32)
    normed = (
        as_float
        * lax.rsqrt(jnp.mean(as_float * as_float, axis=-1, keepdims=True) + epsilon)
        * norm_gain
    ).astype(jnp.bfloat16)
    offset = lax.axis_index(SP) * row_count
    positions = offset + jnp.arange(row_count, dtype=jnp.int32)
    weights = (ret_query, ret_key, ret_value, att_query, att_key, att_value)
    pieces = in_one_piece(
        (weights[0], weights[1], weights[2], weights[3], weights[4], weights[5]), SP, 0, 1
    )
    projected = tuple(
        (jnp.dot(normed, piece, preferred_element_type=jnp.float32) for piece in pieces)
    )
    rounded = tuple((product_f.astype(jnp.bfloat16) for product_f in projected))
    projected = rounded[:3]
    head_count = projected[0].shape[1] // DK
    queries = rotate(projected[0].astype(jnp.float32).reshape(row_count, head_count, DK), positions)
    keys_rot = rotate(
        projected[1].astype(jnp.float32).reshape(row_count, head_count, DK), positions
    ) * DK ** (-0.5)
    values_f = projected[2].astype(jnp.float32).reshape(row_count, head_count, DV)
    log_rates = log_decay[0]
    count = row_count // BLOCK

    def blocked(array):
        return array.reshape(count, BLOCK, head_count, array.shape[-1]).transpose(0, 2, 1, 3)

    rates_blocked = log_rates.reshape(head_count, count, BLOCK).transpose(1, 0, 2)
    local_state, pieces = lax.scan(
        block_step,
        jnp.zeros((head_count, DK, DV), jnp.float32),
        (blocked(queries), blocked(keys_rot), blocked(values_f), rates_blocked),
    )
    local_out = pieces.transpose(0, 2, 1, 3).reshape(row_count, head_count, DV)
    running_totals = jnp.cumsum(log_rates, axis=-1)
    device_decay = jnp.exp(running_totals[:, -1])
    first = (lax.axis_index(SP) == 0).astype(jnp.float32)
    opening = start_state[0] * first
    incoming = opening + state_before(
        device_decay, local_state + device_decay[:, None, None] * opening
    )
    retained = local_out + jnp.einsum(
        "thd,hdv->thv", queries * jnp.exp(running_totals).T[:, :, None], incoming
    )
    centred = retained - jnp.mean(retained, axis=-1, keepdims=True)
    variance = jnp.mean(centred * centred, axis=-1, keepdims=True)
    ret_hidden = (
        (centred * lax.rsqrt(variance + epsilon)).reshape(row_count, head_count * DV) * ret_gain
    ).astype(jnp.bfloat16)
    att_queries, att_keys, att_values = rounded[3:]
    kv_heads = att_keys.shape[1] // HD
    groups = att_queries.shape[1] // HD // kv_heads
    earlier_keys, earlier_values = passed_along(
        (att_keys[row_count - WINDOW :], att_values[row_count - WINDOW :]), SP, 1
    )
    extended_keys = jnp.concatenate([earlier_keys, att_keys], axis=0)
    extended_values = jnp.concatenate([earlier_values, att_values], axis=0)
    windows = row_count // WINDOW

    def banded(array):
        earlier = array[:row_count].reshape(windows, WINDOW, kv_heads, HD)
        current = array[WINDOW:].reshape(windows, WINDOW, kv_heads, HD)
        return jnp.concatenate([earlier, current], axis=1)

    key_band = banded(extended_keys)
    value_band = banded(extended_values)
    grouped_q = att_queries.reshape(windows, WINDOW, kv_heads, groups, HD)
    score_matrix = jnp.einsum(
        "nqhgd,nkhd->nhgqk", grouped_q, key_band, preferred_element_type=jnp.float32
    ) * HD ** (-0.5)
    query_index = WINDOW + jnp.arange(WINDOW)
    key_index = jnp.arange(2 * WINDOW)
    allowed = (key_index[None, :] <= query_index[:, None]) & (
        query_index[:, None] - key_index[None, :] < WINDOW
    )
    key_place = offset - WINDOW + jnp.arange(windows)[:, None] * WINDOW + key_index[None, :]
    visible = (allowed[None] & (key_place >= 0)[:, None, :])[:, None, None]
    expo = jnp.exp(jnp.where(visible, score_matrix, -1e30))
    summed = jnp.sum(expo, axis=-1, keepdims=True) + jnp.exp(sink_logits).reshape(
        1, kv_heads, groups, 1, 1
    )
    probs = (expo / summed).astype(jnp.bfloat16)
    attended = jnp.einsum(
        "nhgqk,nkhd->nqhgd", probs, value_band, preferred_element_type=jnp.float32
    )
    att_hidden = attended.astype(jnp.bfloat16).reshape(row_count, kv_heads * groups * HD)
    ret_width = ret_hidden.shape[1]
    joined = jnp.concatenate([ret_hidden, att_hidden], axis=1)[None]
    piece = collect(joined, "fs", 0)
    product = jnp.einsum(
        "srh,hd->srd", piece[:, :, :ret_width], ret_out, preferred_element_type=jnp.float32
    )
    product = product + jnp.einsum(
        "srh,hd->srd", piece[:, :, ret_width:], att_out, preferred_element_type=jnp.float32
    )
    partial_rows = product.astype(jnp.bfloat16)
    regrouped = lax.all_to_all(partial_rows, "fs", split_axis=0, concat_axis=2, tiled=True)
    mixed = sent_and_summed(regrouped[0].astype(jnp.float32).astype(jnp.bfloat16), "tp", 1)
    return mixed.astype(jnp.bfloat16)[None]


def solution(mesh):
    torus = Mesh(
        mesh.devices.reshape(8, 8, mesh.shape["fs"], mesh.shape["tp"]), ("sp_0", "sp_1", "fs", "tp")
    )
    in_specs = (
        P("fs", SP, "tp"),
        P(),
        P(SP, "tp"),
        P(SP, "tp"),
        P(SP, "tp"),
        P(SP, "tp"),
        P(SP, "tp"),
        P(SP, "tp"),
        P("fs", "tp", SP),
        P("fs", "tp", None, None),
        P("tp"),
        P("tp"),
        P("tp", "fs"),
        P("tp", "fs"),
    )
    out_specs = P("fs", SP, "tp")
    return jax.shard_map(
        shards, mesh=torus, in_specs=in_specs, out_specs=out_specs, check_vma=False
    )
```

```python
import jax
import jax.numpy as jnp
from jax import lax
from jax.experimental import pallas as pl
from jax.experimental.pallas import tpu as pltpu
from jax.sharding import Mesh
from jax.sharding import PartitionSpec as P

D = 2048
DK = 256
HD = 64
ROWS = 256
WINDOW = 128
COLS = 1152
CHUNKS = 4
SP = ("z", "y")
BF = jnp.bfloat16
F32 = jnp.float32
EPS = 1e-06
STEPS = (0, 7, 1, 6, 2, 5, 3, 4)


def dot(a, b, dims=(((1,), (0,)), ((), ())), precision=None):
    return lax.dot_general(a, b, dims, precision=precision, preferred_element_type=F32)


def layer_kernel(
    tok_ref,
    rk_ref,
    rv_ref,
    rq_ref,
    aq_ref,
    kv_ref,
    pack_ref,
    start_ref,
    ro_ref,
    ao_ref,
    gain_ref,
    inverse_ref,
    out_ref,
    tok,
    x_in,
    normed,
    w_all,
    pack,
    start,
    w_out,
    cosine,
    sine,
    keys,
    values,
    queries,
    att_q,
    att_kv,
    state,
    scores,
    pieces,
    came,
    rates,
    own_rate,
    back,
    prior,
    hidden,
    heads,
    s_local,
    s_tok,
    r_tok,
    s_small,
    r_pack,
    r_start,
    s_w,
    r_own,
    r_near,
    r_far,
    s_mirror,
    r_mirror,
    s_scan,
    r_scan,
    s_halo,
    r_halo,
    s_hid,
    r_hid,
    s_out,
    r_out,
):
    z, y = lax.axis_index("z"), lax.axis_index("y")
    x, c = lax.axis_index("x"), lax.axis_index("c")
    me = z * 8 + y
    home = x // 2
    at_home = c == home
    near = 1 - x % 2

    def send(src, dst, send_sem, recv_sem, **to):
        pltpu.make_async_remote_copy(
            src_ref=src, dst_ref=dst, send_sem=send_sem, recv_sem=recv_sem, device_id=to
        ).start()

    def arrived(ref, sem):
        pltpu.make_async_copy(ref, ref, sem).wait()

    def along_first(k):
        return {"z": (z + c * k) % 8, "y": (y + (1 - c) * k) % 8}

    def along_second(k):
        return {"z": (z + (1 - c) * k) % 8, "y": (y + c * k) % 8}

    load_tok = pltpu.make_async_copy(tok_ref, tok, s_local.at[0])
    load_tok.start()
    own = w_all.at[me]
    sources = (rk_ref, rv_ref, rq_ref, aq_ref)
    loads = []
    for n, ref in enumerate(sources):
        cut = pl.ds(pl.multiple_of((x % 2) * 256, 256), 256)
        for half in range(2):
            loads.append(
                pltpu.make_async_copy(
                    ref.at[pl.ds(16 * half, 16), cut],
                    own.at[half, :, pl.ds(256 * n, 256)],
                    s_local.at[1 + 2 * n + half],
                )
            )
    for half in range(2):
        loads.append(
            pltpu.make_async_copy(
                kv_ref.at[x % 2, pl.ds(16 * half, 16)],
                own.at[half, :, pl.ds(1024, 128)],
                s_local.at[9 + half],
            )
        )

    @pl.when(at_home)
    def _():
        for load in loads:
            load.start()

    barrier = pltpu.get_barrier_semaphore()
    friends = [{"x": (x + d) % 4, "c": h} for d in (1, 2, 3) for h in (0, 1)]
    friends += [{"c": 1 - c}]
    friends += [along_first(k) for k in range(1, 8)] + [along_second(k) for k in (1, 7)]
    for friend in friends:
        pl.semaphore_signal(barrier, inc=1, device_id=friend)
    pl.semaphore_wait(barrier, len(friends))

    @pl.when(at_home)
    def _():
        for load in loads:
            load.wait()
        send(own, own, s_small.at[0], r_own, c=1 - c)

    load_tok.wait()
    part = ROWS // CHUNKS

    def token_rows(slot, half, q):
        return x_in.at[slot, half, pl.ds(part * q, part)]

    for q in range(CHUNKS):
        for d in (1, 3):
            send(
                tok.at[pl.ds(part * q, part)],
                token_rows(x % 2, c, q),
                s_tok.at[0],
                r_tok.at[x % 2, c, q],
                x=(x + d) % 4,
                c=home,
            )

    @pl.when(at_home)
    def _():
        for q in range(CHUNKS):
            pltpu.make_async_copy(
                tok.at[pl.ds(part * q, part)], token_rows(x % 2, c, q), r_tok.at[x % 2, c, q]
            ).start()

    @pl.when(jnp.logical_not(at_home))
    def _():
        for q in range(CHUNKS):
            send(
                tok.at[pl.ds(part * q, part)],
                token_rows(x % 2, c, q),
                s_tok.at[1],
                r_tok.at[x % 2, c, q],
                c=1 - c,
            )

    for i in range(2):
        mine = jnp.logical_and(at_home, x % 2 == i)

        @pl.when(mine)
        def _(i=i):
            pltpu.make_async_copy(pack_ref.at[i], pack.at[i], r_pack.at[i]).start()

        @pl.when(jnp.logical_not(mine))
        def _(i=i):
            send(
                pack_ref.at[i],
                pack.at[x % 2],
                s_small.at[1 + i],
                r_pack.at[x % 2],
                x=2 * c + i,
                c=home,
            )

        @pl.when(jnp.logical_and(me == 0, mine))
        def _(i=i):
            pltpu.make_async_copy(start_ref.at[i], start.at[i], r_start.at[i]).start()

        @pl.when(jnp.logical_and(me == 0, jnp.logical_not(mine)))
        def _(i=i):
            send(
                start_ref.at[i],
                start.at[x % 2],
                s_small.at[3 + i],
                r_start.at[x % 2],
                x=2 * c + i,
                c=home,
            )

    def block(ka, kb):
        zz = (z + c * ka + (1 - c) * kb) % 8
        yy = (y + (1 - c) * ka + c * kb) % 8
        return w_all.at[zz * 8 + yy, c]

    def mirror(ref):
        send(ref, ref, s_mirror, r_mirror, c=1 - c)

    @pl.when(jnp.logical_not(at_home))
    def _():
        arrived(own, r_own)

    for k in (1, 7, 2, 6, 3, 5, 4):
        send(block(0, 0), block(0, 0), s_w, r_near.at[8 - k], **along_first(k))

    def limits(n):
        return (4, 3) if n % 2 == 0 else (3, 4)

    def forward(ref, direction, kb, n):
        send(ref, ref, s_w, r_far.at[direction, kb, n], **along_second(7 if direction else 1))

    forward(block(0, 0), 0, 1, 0)
    forward(block(0, 0), 1, 1, 0)

    position = lax.broadcasted_iota(jnp.int32, (ROWS, 128), 0) + me * ROWS
    angle = position.astype(F32) * inverse_ref[...]
    cosine[...] = jnp.cos(angle)
    sine[...] = jnp.sin(angle)

    for n in range(1, 8):
        ka = STEPS[n]
        ref = block(ka, 0)
        arrived(ref, r_near.at[ka])
        forward(ref, 0, 1, n)
        forward(ref, 1, 1, n)
        mirror(ref)

    onward = at_home == (x % 2 == 0)
    relay_half = jnp.where(onward, 1, 0)
    relay_to = (x + jnp.where(onward, 3, 1)) % 4

    def relay(q):
        ref = token_rows(near, relay_half, q)
        arrived(ref, r_tok.at[near, relay_half, q])
        send(ref, ref, s_tok.at[2], r_tok.at[near, relay_half, q], x=relay_to)

    for kb in range(1, 5):
        for n in range(8):
            for direction in range(2):
                limit = limits(n)[direction]
                if kb > limit:
                    continue
                ref = block(STEPS[n], kb if direction else 8 - kb)
                arrived(ref, r_far.at[direction, kb, n])
                if kb < limit:
                    forward(ref, direction, kb + 1, n)
                mirror(ref)
        relay(kb - 1)

    for n, ref in enumerate((ro_ref, ao_ref)):
        rows = pl.ds(pl.multiple_of(c * 512, 512), 512)
        cols = pl.ds(pl.multiple_of((x % 2) * 512, 512), 512)
        dst = w_out.at[n, rows, cols]
        sem = r_out.at[n, x % 2, c]
        for d in (1, 2, 3):
            send(ref, dst, s_out, sem, x=(x + d) % 4, c=home)

        @pl.when(at_home)
        def _(ref=ref, dst=dst, sem=sem):
            pltpu.make_async_copy(ref, dst, sem).start()

        @pl.when(jnp.logical_not(at_home))
        def _(ref=ref, dst=dst, sem=sem):
            send(ref, dst, s_small.at[5], sem, c=1 - c)

    for slot in range(2):
        for half in range(2):
            for q in range(CHUNKS):
                relayed = jnp.logical_and(near == slot, relay_half == half)

                @pl.when(jnp.logical_not(relayed))
                def _(slot=slot, half=half, q=q):
                    arrived(token_rows(slot, half, q), r_tok.at[slot, half, q])

    def norm_rows(t, _):
        slot = t // 8
        rows = pl.ds(pl.multiple_of((t % 8) * 32, 32), 32)
        a = x_in[slot, 0, rows].astype(F32)
        b = x_in[slot, 1, rows].astype(F32)
        total = jnp.sum(a * a, axis=-1, keepdims=True) + jnp.sum(b * b, axis=-1, keepdims=True)
        scale = lax.rsqrt(total * (1.0 / D) + EPS)
        to = pl.ds(pl.multiple_of(t * 32, 32), 32)
        normed[to, 0:1024] = (a * scale * gain_ref[:, 0:1024]).astype(BF)
        normed[to, 1024:2048] = (b * scale * gain_ref[:, 1024:2048]).astype(BF)
        return 0

    lax.fori_loop(0, 16, norm_rows, 0)
    few = pl.ds(0, 63)
    arrived(w_all.at[few, 0], r_mirror)

    def project(at, width):
        w = w_all[:, :, :, at : at + width].reshape(D, width)
        return dot(normed[...], w).astype(BF)

    keys[...] = project(0, 256)
    values[...] = project(256, 256)

    arrived(pack.at[0], r_pack.at[0])
    arrived(pack.at[1], r_pack.at[1])
    ti = lax.broadcasted_iota(jnp.int32, (ROWS, ROWS), 0)
    tj = lax.broadcasted_iota(jnp.int32, (ROWS, ROWS), 1)
    lower = (ti >= tj).astype(F32)
    upper = (ti <= tj).astype(F32)
    exact = lax.Precision.HIGHEST

    def sums(slot):
        rows = pack[slot]
        down = dot(lower, rows, (((1,), (1,)), ((), ())), exact)[:, 0:1]
        across = dot(rows, upper, precision=exact)[0:1, :]
        return down, across

    def rotated(ref, slot):
        rows = ref[pl.ds(ROWS * slot, ROWS)].astype(F32)
        front, rear = rows[:, :128], rows[:, 128:]
        return jnp.concatenate(
            [front * cosine[...] - rear * sine[...], front * sine[...] + rear * cosine[...]], axis=1
        )

    for slot in range(2):
        down, across = sums(slot)
        last = down[ROWS - 1 : ROWS, :]
        key_rows = rotated(keys, slot) * DK ** (-0.5)
        v = values[pl.ds(ROWS * slot, ROWS)]
        own_rate[slot] = jnp.broadcast_to(jnp.exp(last), (1, 128))
        state[slot] = dot((key_rows * jnp.exp(last - down)).astype(BF), v, (((0,), (0,)), ((), ())))
        keys[pl.ds(ROWS * slot, ROWS)] = key_rows.astype(BF)

        @pl.when(me == 0)
        def _(slot=slot):
            arrived(start.at[slot], r_start.at[slot])
            state[slot] = state[slot] + own_rate[slot][:, 0:1] * start[slot]

        for i in range(16):
            for half in range(2):
                pieces[slot * 32 + i * 2 + half] = state[
                    slot, 16 * i : 16 * i + 16, 128 * half : 128 * half + 128
                ].astype(BF)

    def place(index):
        return {"z": index // 8, "y": index % 8}

    def spread(k, _):
        to = (me + k) % 64
        send(own_rate.at[to // 32], rates.at[me], s_scan.at[0], r_scan.at[0], **place(to))
        send(pieces.at[to], came.at[me], s_scan.at[1], r_scan.at[1], **place(to))
        return 0

    lax.fori_loop(1, 64, spread, 0)
    came[me] = pieces[me]
    rates[me] = own_rate[me // 32]

    att_kv[:, pl.ds(WINDOW, ROWS)] = project(1024, 128).reshape(2, ROWS, 128)
    tail = att_kv.at[:, pl.ds(ROWS, WINDOW)]
    lead = att_kv.at[:, pl.ds(0, WINDOW)]

    @pl.when(me < 63)
    def _():
        send(tail, lead, s_halo, r_halo, **place(me + 1))

    @pl.when(me == 0)
    def _():
        att_kv[:, pl.ds(0, WINDOW)] = jnp.zeros((2, WINDOW, 128), BF)

    queries[...] = project(512, 256)
    att_q[...] = project(768, 256)

    for slot in range(2):
        down, across = sums(slot)
        q = rotated(queries, slot)
        weight = jnp.where(ti >= tj, jnp.exp(jnp.where(ti >= tj, down - across, 0.0)), 0.0)
        k = keys[pl.ds(ROWS * slot, ROWS)]
        raw = dot(q.astype(BF), k, (((1,), (1,)), ((), ()))) * weight
        scores[slot] = dot(raw.astype(BF), values[pl.ds(ROWS * slot, ROWS)])
        queries[pl.ds(ROWS * slot, ROWS)] = (q * jnp.exp(down)).astype(BF)

    arrived(rates.at[few], r_scan.at[0])
    arrived(came.at[few], r_scan.at[1])

    def advance(k, carried):
        back[k] = carried.astype(BF)
        return carried * rates[k] + came[k].astype(F32)

    lax.fori_loop(0, 64, advance, jnp.zeros((16, 128), F32))

    def give_back(k, _):
        to = (me + k) % 64
        send(back.at[to], prior.at[me], s_scan.at[2], r_scan.at[2], **place(to))
        return 0

    lax.fori_loop(1, 64, give_back, 0)
    prior[me] = back[me]

    @pl.when(me > 0)
    def _():
        arrived(lead, r_halo)

    qi = lax.broadcasted_iota(jnp.int32, (WINDOW, 2 * WINDOW), 0)
    ki = lax.broadcasted_iota(jnp.int32, (WINDOW, 2 * WINDOW), 1)
    for slot in range(2):
        sink = jnp.exp(pack[slot, 2:3, 0:4])
        for n in range(2):
            allowed = jnp.logical_and(ki > qi, ki <= qi + WINDOW)
            if n == 0:
                allowed = jnp.logical_and(allowed, ki >= jnp.where(me == 0, WINDOW, 0))
            kv = att_kv[slot, pl.ds(WINDOW * n, 2 * WINDOW)]
            rows = att_q[pl.ds(ROWS * slot + WINDOW * n, WINDOW)]
            outs = []
            for g in range(4):
                score = dot(rows[:, HD * g : HD * g + HD], kv[:, :HD], (((1,), (1,)), ((), ())))
                expo = jnp.exp(jnp.where(allowed, score * HD ** (-0.5), -1e30))
                total = jnp.sum(expo, axis=-1, keepdims=True) + sink[:, g : g + 1]
                outs.append(dot((expo / total).astype(BF), kv[:, HD:]))
            hidden[slot, 1, pl.ds(WINDOW * n, WINDOW)] = jnp.concatenate(outs, axis=1).astype(BF)

    def hand_over(kind):
        for i in range(2):
            src = hidden.at[i, kind]
            dst = heads.at[x, kind]
            to = 2 * c + i
            send(src, dst, s_hid.at[kind, i], r_hid.at[kind, x], x=to, c=1 - c)

            @pl.when(to == x)
            def _(src=src, dst=dst):
                pltpu.make_async_copy(src, dst, r_hid.at[kind, x]).start()

            @pl.when(to != x)
            def _(src=src, dst=dst, i=i):
                send(src, dst, s_hid.at[2 + kind, i], r_hid.at[kind, x], x=to)

    hand_over(1)

    arrived(prior.at[few], r_scan.at[2])
    for slot in range(2):
        for i in range(16):
            for half in range(2):
                state[slot, 16 * i : 16 * i + 16, 128 * half : 128 * half + 128] = prior[
                    slot * 32 + i * 2 + half
                ].astype(F32)

        @pl.when(me == 0)
        def _(slot=slot):
            state[slot] = start[slot]

        raw = scores[slot] + dot(queries[pl.ds(ROWS * slot, ROWS)], state[slot].astype(BF))
        centred = raw - jnp.mean(raw, axis=-1, keepdims=True)
        variance = jnp.mean(centred * centred, axis=-1, keepdims=True)
        shaped = centred * lax.rsqrt(variance + EPS) * pack[slot, 1:2, :]
        hidden[slot, 0] = shaped.astype(BF)

    hand_over(0)

    for n in range(2):
        for slot in range(2):
            for half in range(2):
                rows, cols = pl.ds(512 * half, 512), pl.ds(512 * slot, 512)
                arrived(w_out.at[n, rows, cols], r_out.at[n, slot, half])
    total = None
    for kind in (1, 0):
        for j in range(4):
            arrived(heads.at[j, kind], r_hid.at[kind, j])
        rows = jnp.concatenate([heads[j, kind] for j in range(4)], axis=1)
        product = dot(rows, w_out[kind])
        total = product if total is None else total + product
    out_ref[...] = total.astype(BF)

    arrived(x_in.at[0], s_tok.at[0])
    arrived(tok, s_tok.at[2])
    arrived(w_all.at[few, 0], s_w)
    arrived(w_all.at[few, 0], s_mirror)
    arrived(rates.at[few], s_scan.at[0])
    arrived(came.at[few], s_scan.at[1])
    arrived(prior.at[few], s_scan.at[2])

    @pl.when(jnp.logical_not(at_home))
    def _():
        arrived(tok, s_tok.at[1])
        arrived(w_out.at[:, pl.ds(0, 512), pl.ds(0, 512)], s_small.at[5])

    @pl.when(at_home)
    def _():
        arrived(own, s_small.at[0])

    arrived(w_out.at[:, pl.ds(0, 768)], s_out)
    for i in range(2):
        mine = jnp.logical_and(at_home, x % 2 == i)

        @pl.when(jnp.logical_not(mine))
        def _(i=i):
            arrived(pack.at[i], s_small.at[1 + i])

        @pl.when(jnp.logical_and(me == 0, jnp.logical_not(mine)))
        def _(i=i):
            arrived(start.at[i], s_small.at[3 + i])

        for kind in range(2):
            arrived(hidden.at[i, kind], s_hid.at[kind, i])

            @pl.when(2 * c + i != x)
            def _(i=i, kind=kind):
                arrived(hidden.at[i, kind], s_hid.at[2 + kind, i])

    @pl.when(me < 63)
    def _():
        arrived(tail, s_halo)


def shards(
    tokens,
    norm_gain,
    ret_query,
    ret_key,
    ret_value,
    att_query,
    att_key,
    att_value,
    log_decay,
    start_state,
    ret_gain,
    sink_logits,
    ret_out,
    att_out,
):
    kv = jnp.stack(
        [jnp.concatenate([a[:, i : i + HD] for a in (att_key, att_value)], axis=1) for i in (0, HD)]
    )
    pack = jnp.concatenate(
        [
            log_decay[0][:, None, :],
            ret_gain.reshape(2, 1, 256),
            jnp.pad(sink_logits.reshape(2, 1, 4), ((0, 0), (0, 0), (0, 252))),
            jnp.zeros((2, 5, 256), F32),
        ],
        axis=1,
    )
    inverse = (1.0 / 10000.0 ** (jnp.arange(128, dtype=F32) / 128)).reshape(1, 128)
    vmem = pl.BlockSpec(memory_space=pltpu.VMEM)
    hbm = pl.BlockSpec(memory_space=pl.ANY)
    dma = pltpu.SemaphoreType.DMA
    scratch = [
        pltpu.VMEM((ROWS, 1024), BF),
        pltpu.VMEM((2, 2, ROWS, 1024), BF),
        pltpu.VMEM((2 * ROWS, D), BF),
        pltpu.VMEM((64, 2, 16, COLS), BF),
        pltpu.VMEM((2, 8, 256), F32),
        pltpu.VMEM((2, 256, 256), F32),
        pltpu.VMEM((2, 1024, 1024), BF),
        pltpu.VMEM((ROWS, 128), F32),
        pltpu.VMEM((ROWS, 128), F32),
        pltpu.VMEM((2 * ROWS, 256), BF),
        pltpu.VMEM((2 * ROWS, 256), BF),
        pltpu.VMEM((2 * ROWS, 256), BF),
        pltpu.VMEM((2 * ROWS, 256), BF),
        pltpu.VMEM((2, WINDOW + ROWS, 128), BF),
        pltpu.VMEM((2, 256, 256), F32),
        pltpu.VMEM((2, ROWS, 256), F32),
        pltpu.VMEM((64, 16, 128), BF),
        pltpu.VMEM((64, 16, 128), BF),
        pltpu.VMEM((64, 1, 128), F32),
        pltpu.VMEM((2, 1, 128), F32),
        pltpu.VMEM((64, 16, 128), BF),
        pltpu.VMEM((64, 16, 128), BF),
        pltpu.VMEM((2, 2, ROWS, 256), BF),
        pltpu.VMEM((4, 2, ROWS, 256), BF),
        dma((11,)),
        dma((3,)),
        dma((2, 2, CHUNKS)),
        dma((6,)),
        dma((2,)),
        dma((2,)),
        dma,
        dma,
        dma((8,)),
        dma((2, 5, 8)),
        dma,
        dma,
        dma((3,)),
        dma((3,)),
        dma,
        dma,
        dma((4, 2)),
        dma((2, 4)),
        dma,
        dma((2, 2, 2)),
    ]
    mixed = pl.pallas_call(
        layer_kernel,
        out_shape=jax.ShapeDtypeStruct((ROWS, 1024), BF),
        in_specs=[hbm] * 5 + [hbm, hbm, hbm, hbm, hbm, vmem, vmem],
        out_specs=vmem,
        scratch_shapes=scratch,
        compiler_params=pltpu.CompilerParams(
            collective_id=0, has_side_effects=True, vmem_limit_bytes=60 * 1024 * 1024
        ),
    )(
        tokens[0],
        ret_key,
        ret_value,
        ret_query,
        att_query,
        kv,
        pack,
        start_state[0],
        ret_out,
        att_out,
        norm_gain.reshape(1, D),
        inverse,
    )
    return mixed[None]


def solution(mesh):
    torus = Mesh(
        mesh.devices.reshape(8, 8, mesh.shape["fs"], mesh.shape["tp"]), ("z", "y", "x", "c")
    )
    across = P(SP, "c")
    in_specs = (
        P("x", SP, "c"),
        P(),
        across,
        across,
        across,
        across,
        across,
        across,
        P("x", "c", SP),
        P("x", "c", None, None),
        P("c"),
        P("c"),
        P("c", "x"),
        P("c", "x"),
    )
    return jax.shard_map(
        shards, mesh=torus, in_specs=in_specs, out_specs=P("x", SP, "c"), check_vma=False
    )
```

```python
import jax
import jax.numpy as jnp
import numpy as np
from jax import lax
from jax.experimental import pallas as pl
from jax.experimental.pallas import tpu as pltpu
from jax.sharding import Mesh
from jax.sharding import PartitionSpec as P

D = 2048
DK = 256
HD = 64
ROWS = 256
WINDOW = 128
COLS = 1152
CHUNKS = 4
SP = ("z", "y")
BF = jnp.bfloat16
F32 = jnp.float32
EPS = 1e-06
STEPS = (0, 7, 1, 6, 2, 5, 3, 4)


def dot(a, b, dims=(((1,), (0,)), ((), ())), precision=None):
    return lax.dot_general(a, b, dims, precision=precision, preferred_element_type=F32)


def layer_kernel(
    tok_ref,
    rk_ref,
    rv_ref,
    rq_ref,
    aq_ref,
    ak_ref,
    av_ref,
    decay_ref,
    ret_gain_ref,
    sink_ref,
    start_ref,
    ro_ref,
    ao_ref,
    gain_ref,
    inverse_ref,
    out_ref,
    tok,
    x_in,
    normed,
    w_all,
    pack,
    start,
    o_near,
    o_far,
    kv_raw,
    decay_raw,
    ret_gain_raw,
    sink_raw,
    pack_own,
    gain,
    inverse,
    inside,
    grow,
    fall,
    partial,
    cosine,
    sine,
    keys,
    values,
    queries,
    att_q,
    att_kv,
    state,
    scores,
    pieces,
    came,
    rates,
    own_rate,
    back,
    prior,
    hidden,
    heads,
    s_local,
    s_tok,
    r_tok,
    s_small,
    r_pack,
    r_start,
    s_w,
    r_own,
    r_near,
    r_far,
    s_mirror,
    r_mirror,
    s_scan,
    r_scan,
    s_halo,
    r_halo,
    s_hid,
    r_hid,
    s_out,
    r_out,
    r_own_far,
    s_slice,
    r_slice,
    s_o,
    r_o_near,
    r_o_far,
    s_o_mirror,
    r_o_mirror,
):
    z, y = lax.axis_index("z"), lax.axis_index("y")
    x, c = lax.axis_index("x"), lax.axis_index("c")
    me = z * 8 + y
    home = x // 2
    at_home = c == home
    near = 1 - x % 2

    def send(src, dst, send_sem, recv_sem, **to):
        pltpu.make_async_remote_copy(
            src_ref=src, dst_ref=dst, send_sem=send_sem, recv_sem=recv_sem, device_id=to
        ).start()

    def arrived(ref, sem):
        pltpu.make_async_copy(ref, ref, sem).wait()

    def along_first(k):
        return {"z": (z + c * k) % 8, "y": (y + (1 - c) * k) % 8}

    def along_second(k):
        return {"z": (z + (1 - c) * k) % 8, "y": (y + c * k) % 8}

    barrier = pltpu.get_barrier_semaphore()
    friends = [{"x": (x + d) % 4, "c": h} for d in (1, 2, 3) for h in (0, 1)]
    friends += [{"c": 1 - c}]
    friends += [along_first(k) for k in range(1, 8)] + [along_second(k) for k in (1, 7)]
    for friend in friends:
        pl.semaphore_signal(barrier, inc=1, device_id=friend)

    own = w_all.at[me]
    odd = x % 2
    small = (
        (ak_ref, kv_raw.at[0]),
        (av_ref, kv_raw.at[1]),
        (decay_ref, decay_raw),
        (ret_gain_ref, ret_gain_raw),
        (sink_ref, sink_raw),
        (inverse_ref, inverse),
        (gain_ref, gain),
        (tok_ref, tok),
    )
    small = [
        pltpu.make_async_copy(src, dst, s_local.at[8 + n]) for n, (src, dst) in enumerate(small)
    ]
    loads = []
    for n, ref in enumerate((rk_ref, rv_ref, rq_ref, aq_ref)):
        cols = pl.ds(pl.multiple_of(odd * 256, 256), 256)
        for half in range(2):
            loads.append(
                pltpu.make_async_copy(
                    ref.at[pl.ds(16 * half, 16), cols],
                    own.at[half, :, pl.ds(256 * n, 256)],
                    s_local.at[2 * n + half],
                )
            )
    for load in small[:2]:
        load.start()

    @pl.when(at_home)
    def _():
        for load in loads:
            load.start()

    for load in small[2:]:
        load.start()
    for load in small[:7]:
        load.wait()
    position = lax.broadcasted_iota(jnp.int32, (ROWS, 128), 0) + me * ROWS
    angle = position.astype(F32) * inverse[...]
    cosine[...] = jnp.cos(angle)
    sine[...] = jnp.sin(angle)
    pack_own[...] = jnp.zeros((2, 8, 256), F32)
    for i in range(2):
        pack_own[i, 0:1, :] = decay_raw[i : i + 1, :]
        pack_own[i, 1:2, :] = ret_gain_raw[:, 256 * i : 256 * i + 256]
        pack_own[i, 2:3, 0:4] = sink_raw[:, 4 * i : 4 * i + 4]

    @pl.when(at_home)
    def _():
        for load in loads:
            load.wait()
        both = [jnp.where(odd == 0, kv_raw[n, :, :HD], kv_raw[n, :, HD:]) for n in range(2)]
        both = jnp.concatenate(both, axis=1)
        for half in range(2):
            w_all[me, half, :, 1024:COLS] = both[16 * half : 16 * half + 16]

    small[7].wait()
    pl.semaphore_wait(barrier, len(friends))

    @pl.when(at_home)
    def _():
        send(own, own, s_small.at[0], r_own, c=1 - c)

    part = ROWS // CHUNKS

    def token_rows(slot, half, q):
        return x_in.at[slot, half, pl.ds(part * q, part)]

    for q in range(CHUNKS):
        for d in (1, 3):
            send(
                tok.at[pl.ds(part * q, part)],
                token_rows(x % 2, c, q),
                s_tok.at[0],
                r_tok.at[x % 2, c, q],
                x=(x + d) % 4,
                c=home,
            )

    @pl.when(at_home)
    def _():
        for q in range(CHUNKS):
            pltpu.make_async_copy(
                tok.at[pl.ds(part * q, part)], token_rows(x % 2, c, q), r_tok.at[x % 2, c, q]
            ).start()

    @pl.when(jnp.logical_not(at_home))
    def _():
        for q in range(CHUNKS):
            send(
                tok.at[pl.ds(part * q, part)],
                token_rows(x % 2, c, q),
                s_tok.at[1],
                r_tok.at[x % 2, c, q],
                c=1 - c,
            )

    for i in range(2):
        mine = jnp.logical_and(at_home, x % 2 == i)

        @pl.when(mine)
        def _(i=i):
            pltpu.make_async_copy(pack_own.at[i], pack.at[i], r_pack.at[i]).start()

        @pl.when(jnp.logical_not(mine))
        def _(i=i):
            send(
                pack_own.at[i],
                pack.at[x % 2],
                s_small.at[1 + i],
                r_pack.at[x % 2],
                x=2 * c + i,
                c=home,
            )

        @pl.when(jnp.logical_and(me == 0, mine))
        def _(i=i):
            pltpu.make_async_copy(start_ref.at[i], start.at[i], r_start.at[i]).start()

        @pl.when(jnp.logical_and(me == 0, jnp.logical_not(mine)))
        def _(i=i):
            send(
                start_ref.at[i],
                start.at[x % 2],
                s_small.at[3 + i],
                r_start.at[x % 2],
                x=2 * c + i,
                c=home,
            )

    def block(ka, kb):
        zz = (z + c * ka + (1 - c) * kb) % 8
        yy = (y + (1 - c) * ka + c * kb) % 8
        return w_all.at[zz * 8 + yy, c]

    def mirror(ref):
        send(ref, ref, s_mirror, r_mirror, c=1 - c)

    @pl.when(jnp.logical_not(at_home))
    def _():
        arrived(own, r_own)

    for k in (1, 7, 2, 6, 3, 5, 4):
        send(block(0, 0), block(0, 0), s_w, r_near.at[8 - k], **along_first(k))

    def limits(n):
        return (4, 3) if n % 2 == 0 else (3, 4)

    def forward(ref, direction, kb, n):
        send(ref, ref, s_w, r_far.at[direction, kb, n], **along_second(7 if direction else 1))

    forward(block(0, 0), 0, 1, 0)
    forward(block(0, 0), 1, 1, 0)

    for n in range(1, 8):
        ka = STEPS[n]
        ref = block(ka, 0)
        arrived(ref, r_near.at[ka])
        forward(ref, 0, 1, n)
        forward(ref, 1, 1, n)
        mirror(ref)

    onward = at_home == (x % 2 == 0)
    relay_half = jnp.where(onward, 1, 0)
    relay_to = (x + jnp.where(onward, 3, 1)) % 4

    def relay(q):
        ref = token_rows(near, relay_half, q)
        arrived(ref, r_tok.at[near, relay_half, q])
        send(ref, ref, s_tok.at[2], r_tok.at[near, relay_half, q], x=relay_to)

    def norm_rows(slot, t):
        if t % 2 == 0:
            q = t // 2

            @pl.when(slot == near)
            def _():
                arrived(token_rows(near, 1 - relay_half, q), r_tok.at[near, 1 - relay_half, q])

            @pl.when(slot != near)
            def _():
                for half in range(2):
                    arrived(token_rows(1 - near, half, q), r_tok.at[1 - near, half, q])

        rows = pl.ds(32 * t, 32)
        a = x_in[slot, 0, rows].astype(F32)
        b = x_in[slot, 1, rows].astype(F32)
        total = jnp.sum(a * a, axis=-1, keepdims=True) + jnp.sum(b * b, axis=-1, keepdims=True)
        scale = lax.rsqrt(total * (1.0 / D) + EPS)
        to = pl.ds(pl.multiple_of(slot * ROWS + 32 * t, 32), 32)
        normed[to, 0:1024] = (a * scale * gain[:, 0:1024]).astype(BF)
        normed[to, 1024:2048] = (b * scale * gain[:, 1024:2048]).astype(BF)

    def ring(kb, n):
        for direction in range(2):
            limit = limits(n)[direction]
            if kb > limit:
                continue
            ref = block(STEPS[n], kb if direction else 8 - kb)
            arrived(ref, r_far.at[direction, kb, n])
            if kb < limit:
                forward(ref, direction, kb + 1, n)
            mirror(ref)

    relay(0)
    for n in range(4):
        ring(1, n)
    relay(1)
    for n in range(4, 8):
        ring(1, n)
    relay(2)

    arrived(pack.at[0], r_pack.at[0])
    arrived(pack.at[1], r_pack.at[1])
    ti = lax.broadcasted_iota(jnp.int32, (ROWS, ROWS), 0)
    tj = lax.broadcasted_iota(jnp.int32, (ROWS, ROWS), 1)
    exact = lax.Precision.HIGHEST

    def decays(slot):
        rows = pack[slot]
        lower = (ti >= tj).astype(F32)
        upper = (ti <= tj).astype(F32)
        down = dot(lower, rows, (((1,), (1,)), ((), ())), exact)[:, 0:1]
        across = dot(rows, upper, precision=exact)[0:1, :]
        last = down[ROWS - 1 : ROWS, :]
        inside[slot] = jnp.where(ti >= tj, jnp.exp(jnp.where(ti >= tj, down - across, 0.0)), 0.0)
        grow[slot] = jnp.broadcast_to(jnp.exp(down), (ROWS, 128))
        fall[slot] = jnp.broadcast_to(jnp.exp(last - down), (ROWS, 128))
        own_rate[slot] = jnp.broadcast_to(jnp.exp(last), (1, 128))

    for n in range(8):
        ring(2, n)
        if n == 1:
            decays(0)
        if n == 3:
            relay(3)
        if n == 5:
            decays(1)

    first_at = c * z + (1 - c) * y
    second_at = (1 - c) * z + c * y
    line = second_at * 8 + first_at

    @pl.when(line < 32)
    def _():
        for d in (1, 2, 3):
            src = ro_ref.at[32 + line % 32]
            send(src, o_far.at[c, line, 3 - d], s_slice, r_slice.at[3 - d], x=(x + d) % 4)

    @pl.when(line >= 32)
    def _():
        for d in (1, 2, 3):
            src = ao_ref.at[32 + line % 32]
            send(src, o_far.at[c, line, 3 - d], s_slice, r_slice.at[3 - d], x=(x + d) % 4)

    low, high, three = pl.ds(0, 32), pl.ds(32, 32), pl.ds(0, 3)
    for n, ref in enumerate((ro_ref, ao_ref)):
        for d in (1, 2, 3):
            send(
                ref.at[low],
                o_near.at[c, n, 3 - d],
                s_out,
                r_out.at[c, n, 3 - d],
                x=(x + d) % 4,
                c=home,
            )
        pairs = (
            (ref.at[low], o_near.at[c, n, 3], r_out.at[c, n, 3]),
            (ref.at[high], o_far.at[c, pl.ds(32 * n, 32), 3], r_own_far.at[c, n]),
        )

        @pl.when(at_home)
        def _(pairs=pairs):
            for src, dst, sem in pairs:
                pltpu.make_async_copy(src, dst, sem).start()

        @pl.when(jnp.logical_not(at_home))
        def _(pairs=pairs):
            for src, dst, sem in pairs:
                send(src, dst, s_small.at[5], sem, c=1 - c)

    def o_block(ka):
        return o_far.at[c, second_at * 8 + (first_at + ka) % 8, three]

    def o_group(kb, g):
        at = pl.multiple_of(((second_at + kb) % 8) * 8 + 4 * g, 4)
        return o_far.at[c, pl.ds(at, 4), three]

    def o_forward(ref, direction, kb, g):
        send(ref, ref, s_o, r_o_far.at[direction, kb, g], **along_second(7 if direction else 1))

    def o_mirror(ref):
        send(ref, ref, s_o_mirror, r_o_mirror, c=1 - c)

    def o_step(kb):
        for g in range(2):
            for direction in range(2):
                limit = limits(g)[direction]
                if kb > limit:
                    continue
                ref = o_group(kb if direction else 8 - kb, g)
                arrived(ref, r_o_far.at[direction, kb, g])
                if kb < limit:
                    o_forward(ref, direction, kb + 1, g)
                o_mirror(ref)

    for n in range(8):
        ring(3, n)
        norm_rows(near, n)
    for d in range(3):
        arrived(o_far.at[c, line, d], r_slice.at[d])
    for k in (4, 3, 5, 2, 6, 1, 7):
        send(o_block(0), o_block(0), s_o, r_o_near.at[8 - k], **along_first(k))
    for n in range(8):
        ring(4, n)
        norm_rows(1 - near, n)
    for k in range(1, 8):
        arrived(o_block(k), r_o_near.at[k])
    for g in range(2):
        o_forward(o_group(0, g), 0, 1, g)
        o_forward(o_group(0, g), 1, 1, g)
        o_mirror(o_group(0, g))
    few = pl.ds(0, 63)
    arrived(w_all.at[few, 0], r_mirror)

    def project(at, width):
        w = w_all[:, :, :, at : at + width].reshape(D, width)
        return dot(normed[...], w).astype(BF)

    keys[...] = project(0, 256)
    values[...] = project(256, 256)

    def rotated(ref, slot):
        rows = ref[pl.ds(ROWS * slot, ROWS)].astype(F32)
        front, rear = rows[:, :128], rows[:, 128:]
        return (
            front * cosine[...] - rear * sine[...],
            front * sine[...] + rear * cosine[...],
        )

    for slot in range(2):
        front, rear = [part * DK ** (-0.5) for part in rotated(keys, slot)]
        v = values[pl.ds(ROWS * slot, ROWS)]
        left = jnp.concatenate(
            [(front * fall[slot]).astype(BF), (rear * fall[slot]).astype(BF)], axis=1
        )
        state[slot] = dot(left, v, (((0,), (0,)), ((), ())))
        keys[pl.ds(ROWS * slot, ROWS)] = jnp.concatenate(
            [front.astype(BF), rear.astype(BF)], axis=1
        )

        @pl.when(me == 0)
        def _(slot=slot):
            arrived(start.at[slot], r_start.at[slot])
            state[slot] = state[slot] + own_rate[slot][:, 0:1] * start[slot]

        for i in range(16):
            for half in range(2):
                pieces[slot * 32 + i * 2 + half] = state[
                    slot, 16 * i : 16 * i + 16, 128 * half : 128 * half + 128
                ].astype(BF)

    def place(index):
        return {"z": index // 8, "y": index % 8}

    def reach(k):
        return min(k // 8, 8 - k // 8) + min(k % 8, 8 - k % 8)

    offsets = sorted(range(1, 64), key=lambda k: (-reach(k), k))

    def peer(k):
        zz, yy = (z + k // 8) % 8, (y + k % 8) % 8
        return zz * 8 + yy, {"z": zz, "y": yy}

    for k in offsets:
        to, at = peer(k)
        send(pieces.at[to], came.at[me], s_scan.at[1], r_scan.at[1], **at)
    for k in offsets:
        to, at = peer(k)
        send(own_rate.at[to // 32], rates.at[me], s_scan.at[0], r_scan.at[0], **at)
    came[me] = pieces[me]
    rates[me] = own_rate[me // 32]

    att_kv[:, pl.ds(WINDOW, ROWS)] = project(1024, 128).reshape(2, ROWS, 128)
    tail = att_kv.at[:, pl.ds(ROWS, WINDOW)]
    lead = att_kv.at[:, pl.ds(0, WINDOW)]

    @pl.when(me < 63)
    def _():
        send(tail, lead, s_halo, r_halo, **place(me + 1))

    @pl.when(me == 0)
    def _():
        att_kv[:, pl.ds(0, WINDOW)] = jnp.zeros((2, WINDOW, 128), BF)

    both = project(512, 512)
    queries[...] = both[:, :256]
    att_q[...] = both[:, 256:]

    o_step(1)
    for slot in range(2):
        front, rear = rotated(queries, slot)
        q = jnp.concatenate([front.astype(BF), rear.astype(BF)], axis=1)
        k = keys[pl.ds(ROWS * slot, ROWS)]
        raw = dot(q, k, (((1,), (1,)), ((), ()))) * inside[slot]
        scores[slot] = dot(raw.astype(BF), values[pl.ds(ROWS * slot, ROWS)])
        queries[pl.ds(ROWS * slot, ROWS)] = jnp.concatenate(
            [(front * grow[slot]).astype(BF), (rear * grow[slot]).astype(BF)], axis=1
        )

    o_step(2)
    arrived(rates.at[few], r_scan.at[0])
    arrived(came.at[few], r_scan.at[1])

    def advance(k, carried):
        back[k] = carried.astype(BF)
        return carried * rates[k] + came[k].astype(F32)

    lax.fori_loop(0, 64, advance, jnp.zeros((16, 128), F32))

    for k in offsets:
        to, at = peer(k)
        send(back.at[to], prior.at[me], s_scan.at[2], r_scan.at[2], **at)
    prior[me] = back[me]

    o_step(3)
    @pl.when(me > 0)
    def _():
        arrived(lead, r_halo)

    qi = lax.broadcasted_iota(jnp.int32, (WINDOW, 2 * WINDOW), 0)
    ki = lax.broadcasted_iota(jnp.int32, (WINDOW, 2 * WINDOW), 1)
    for slot in range(2):
        sink = jnp.exp(pack[slot, 2:3, 0:4])
        for n in range(2):
            allowed = jnp.logical_and(ki > qi, ki <= qi + WINDOW)
            if n == 0:
                allowed = jnp.logical_and(allowed, ki >= jnp.where(me == 0, WINDOW, 0))
            kv = att_kv[slot, pl.ds(WINDOW * n, 2 * WINDOW)]
            rows = att_q[pl.ds(ROWS * slot + WINDOW * n, WINDOW)]
            outs = []
            for g in range(4):
                score = dot(rows[:, HD * g : HD * g + HD], kv[:, :HD], (((1,), (1,)), ((), ())))
                expo = jnp.exp(jnp.where(allowed, score * HD ** (-0.5), -1e30))
                total = jnp.sum(expo, axis=-1, keepdims=True) + sink[:, g : g + 1]
                outs.append(dot((expo / total).astype(BF), kv[:, HD:]))
            hidden[slot, 1, pl.ds(WINDOW * n, WINDOW)] = jnp.concatenate(outs, axis=1).astype(BF)

    def hand_over(kind):
        for i in range(2):
            src = hidden.at[i, kind]
            dst = heads.at[x, kind]
            to = 2 * c + i
            send(src, dst, s_hid.at[kind, i], r_hid.at[kind, x], x=to, c=1 - c)

            @pl.when(to == x)
            def _(src=src, dst=dst):
                pltpu.make_async_copy(src, dst, r_hid.at[kind, x]).start()

            @pl.when(to != x)
            def _(src=src, dst=dst, i=i):
                send(src, dst, s_hid.at[2 + kind, i], r_hid.at[kind, x], x=to)

    o_step(4)
    hand_over(1)

    arrived(prior.at[few], r_scan.at[2])
    for slot in range(2):
        for i in range(16):
            for half in range(2):
                state[slot, 16 * i : 16 * i + 16, 128 * half : 128 * half + 128] = prior[
                    slot * 32 + i * 2 + half
                ].astype(F32)

        @pl.when(me == 0)
        def _(slot=slot):
            state[slot] = start[slot]

        raw = scores[slot] + dot(queries[pl.ds(ROWS * slot, ROWS)], state[slot].astype(BF))
        centred = raw - jnp.mean(raw, axis=-1, keepdims=True)
        variance = jnp.mean(centred * centred, axis=-1, keepdims=True)
        shaped = centred * lax.rsqrt(variance + EPS) * pack[slot, 1:2, :]
        hidden[slot, 0] = shaped.astype(BF)

    hand_over(0)

    for d in range(2):
        for half in range(2):
            for n in range(2):
                rel = (2 * c + d + 3 - x) % 4
                arrived(o_near.at[half, n, rel], r_out.at[half, n, rel])

    @pl.when(at_home)
    def _():
        for half in range(2):
            for n in range(2):
                arrived(o_far.at[half, pl.ds(32 * n, 32), 3], r_own_far.at[half, n])

    arrived(o_far.at[1 - c, :, three], r_o_mirror)

    def product(kind, d):
        rel = (2 * c + d + 3 - x) % 4
        total = None
        for half in range(2):
            near_rows = o_near[half, kind, rel].reshape(256, 512)
            far_rows = o_far[half, pl.ds(32 * kind, 32), rel].reshape(256, 512)
            one = dot(heads[2 * half, kind], near_rows) + dot(heads[2 * half + 1, kind], far_rows)
            total = one if total is None else total + one
        return total

    for j in range(4):
        arrived(heads.at[j, 1], r_hid.at[1, j])
    for d in range(2):
        partial[d] = product(1, d)
    for j in range(4):
        arrived(heads.at[j, 0], r_hid.at[0, j])
    for d in range(2):
        out_ref[:, 512 * d : 512 * d + 512] = (partial[d] + product(0, d)).astype(BF)

    arrived(x_in.at[0], s_tok.at[0])
    arrived(tok, s_tok.at[2])
    arrived(w_all.at[few, 0], s_w)
    arrived(w_all.at[few, 0], s_mirror)
    arrived(rates.at[few], s_scan.at[0])
    arrived(came.at[few], s_scan.at[1])
    arrived(prior.at[few], s_scan.at[2])

    @pl.when(jnp.logical_not(at_home))
    def _():
        arrived(tok, s_tok.at[1])
        arrived(o_near.at[0, :, pl.ds(0, 2)], s_small.at[5])

    @pl.when(at_home)
    def _():
        arrived(own, s_small.at[0])

    arrived(o_near.at[0, :, three], s_out)
    arrived(o_far.at[0, 0, three], s_slice)
    arrived(o_far.at[0, few, three], s_o)
    arrived(o_far.at[0, :, three], s_o_mirror)
    for i in range(2):
        mine = jnp.logical_and(at_home, x % 2 == i)

        @pl.when(jnp.logical_not(mine))
        def _(i=i):
            arrived(pack.at[i], s_small.at[1 + i])

        @pl.when(jnp.logical_and(me == 0, jnp.logical_not(mine)))
        def _(i=i):
            arrived(start.at[i], s_small.at[3 + i])

        for kind in range(2):
            arrived(hidden.at[i, kind], s_hid.at[kind, i])

            @pl.when(2 * c + i != x)
            def _(i=i, kind=kind):
                arrived(hidden.at[i, kind], s_hid.at[2 + kind, i])

    @pl.when(me < 63)
    def _():
        arrived(tail, s_halo)


def shards(
    tokens,
    norm_gain,
    ret_query,
    ret_key,
    ret_value,
    att_query,
    att_key,
    att_value,
    log_decay,
    start_state,
    ret_gain,
    sink_logits,
    ret_out,
    att_out,
):
    steps = np.arange(128, dtype=np.float32) / np.float32(128)
    inverse = jnp.asarray((np.float32(1) / np.float32(10000) ** steps).reshape(1, 128))
    vmem = pl.BlockSpec(memory_space=pltpu.VMEM)
    hbm = pl.BlockSpec(memory_space=pl.ANY)
    dma = pltpu.SemaphoreType.DMA
    scratch = [
        pltpu.VMEM((ROWS, 1024), BF),
        pltpu.VMEM((2, 2, ROWS, 1024), BF),
        pltpu.VMEM((2 * ROWS, D), BF),
        pltpu.VMEM((64, 2, 16, COLS), BF),
        pltpu.VMEM((2, 8, 256), F32),
        pltpu.VMEM((2, 256, 256), F32),
        pltpu.VMEM((2, 2, 4, 32, 8, 512), BF),
        pltpu.VMEM((2, 64, 4, 8, 512), BF),
        pltpu.VMEM((2, 32, 128), BF),
        pltpu.VMEM((2, 256), F32),
        pltpu.VMEM((1, 512), F32),
        pltpu.VMEM((1, 8), F32),
        pltpu.VMEM((2, 8, 256), F32),
        pltpu.VMEM((1, D), F32),
        pltpu.VMEM((1, 128), F32),
        pltpu.VMEM((2, ROWS, ROWS), F32),
        pltpu.VMEM((2, ROWS, 128), F32),
        pltpu.VMEM((2, ROWS, 128), F32),
        pltpu.VMEM((2, ROWS, 512), F32),
        pltpu.VMEM((ROWS, 128), F32),
        pltpu.VMEM((ROWS, 128), F32),
        pltpu.VMEM((2 * ROWS, 256), BF),
        pltpu.VMEM((2 * ROWS, 256), BF),
        pltpu.VMEM((2 * ROWS, 256), BF),
        pltpu.VMEM((2 * ROWS, 256), BF),
        pltpu.VMEM((2, WINDOW + ROWS, 128), BF),
        pltpu.VMEM((2, 256, 256), F32),
        pltpu.VMEM((2, ROWS, 256), F32),
        pltpu.VMEM((64, 16, 128), BF),
        pltpu.VMEM((64, 16, 128), BF),
        pltpu.VMEM((64, 1, 128), F32),
        pltpu.VMEM((2, 1, 128), F32),
        pltpu.VMEM((64, 16, 128), BF),
        pltpu.VMEM((64, 16, 128), BF),
        pltpu.VMEM((2, 2, ROWS, 256), BF),
        pltpu.VMEM((4, 2, ROWS, 256), BF),
        dma((16,)),
        dma((3,)),
        dma((2, 2, CHUNKS)),
        dma((6,)),
        dma((2,)),
        dma((2,)),
        dma,
        dma,
        dma((8,)),
        dma((2, 5, 8)),
        dma,
        dma,
        dma((3,)),
        dma((3,)),
        dma,
        dma,
        dma((4, 2)),
        dma((2, 4)),
        dma,
        dma((2, 2, 4)),
        dma((2, 2)),
        dma,
        dma((3,)),
        dma,
        dma((8,)),
        dma((2, 5, 2)),
        dma,
        dma,
    ]
    mixed = pl.pallas_call(
        layer_kernel,
        out_shape=pltpu.VMEM((ROWS, 1024), BF),
        in_specs=[hbm] * 15,
        out_specs=vmem,
        scratch_shapes=scratch,
        compiler_params=pltpu.CompilerParams(
            collective_id=0, has_side_effects=True, vmem_limit_bytes=60 * 1024 * 1024
        ),
    )(
        tokens[0],
        ret_key,
        ret_value,
        ret_query,
        att_query,
        att_key,
        att_value,
        log_decay[0],
        ret_gain.reshape(1, 512),
        sink_logits.reshape(1, 8),
        start_state[0],
        ret_out.reshape(64, 8, 512),
        att_out.reshape(64, 8, 512),
        norm_gain.reshape(1, D),
        inverse,
    )
    return mixed[None]


def solution(mesh):
    torus = Mesh(
        mesh.devices.reshape(8, 8, mesh.shape["fs"], mesh.shape["tp"]), ("z", "y", "x", "c")
    )
    across = P(SP, "c")
    in_specs = (
        P("x", SP, "c"),
        P(),
        across,
        across,
        across,
        across,
        across,
        across,
        P("x", "c", SP),
        P("x", "c", None, None),
        P("c"),
        P("c"),
        P("c", "x"),
        P("c", "x"),
    )
    return jax.shard_map(
        shards, mesh=torus, in_specs=in_specs, out_specs=P("x", SP, "c"), check_vma=False
    )
```

```python
import jax
import jax.numpy as jnp
import numpy as np
from jax import lax
from jax.experimental import pallas as pl
from jax.experimental.pallas import tpu as pltpu
from jax.sharding import Mesh
from jax.sharding import PartitionSpec as P

D = 2048
DK = 256
HD = 64
ROWS = 256
WINDOW = 128
COLS = 1152
CHUNKS = 4
SP = ("z", "y")
BF = jnp.bfloat16
F32 = jnp.float32
EPS = 1e-06
STEPS = (0, 7, 1, 6, 2, 5, 3, 4)


def dot(a, b, dims=(((1,), (0,)), ((), ())), precision=None):
    return lax.dot_general(a, b, dims, precision=precision, preferred_element_type=F32)


def layer_kernel(
    tok_ref,
    rk_ref,
    rv_ref,
    rq_ref,
    aq_ref,
    ak_ref,
    av_ref,
    decay_ref,
    ret_gain_ref,
    sink_ref,
    start_ref,
    ro_ref,
    ao_ref,
    gain_ref,
    inverse_ref,
    out_ref,
    tok,
    x_in,
    normed,
    w_all,
    pack,
    start,
    o_near,
    o_far,
    kv_raw,
    decay_raw,
    ret_gain_raw,
    sink_raw,
    pack_own,
    gain,
    inverse,
    inside,
    grow,
    fall,
    partial,
    cosine,
    sine,
    keys,
    values,
    queries,
    att_q,
    att_kv,
    state,
    scores,
    pieces,
    came,
    rates,
    own_rate,
    back,
    prior,
    hidden,
    heads,
    s_local,
    s_tok,
    r_tok,
    s_small,
    r_pack,
    r_start,
    s_open,
    s_w,
    r_own,
    r_near,
    r_far,
    s_mirror,
    r_mirror,
    s_scan,
    r_scan,
    s_halo,
    r_halo,
    s_hid,
    r_hid,
    s_pass,
    r_pass,
    s_out,
    r_out,
    r_own_far,
    s_slice,
    r_slice,
    s_o,
    r_o_near,
    r_o_far,
    s_o_mirror,
    r_o_mirror,
):
    z, y = lax.axis_index("z"), lax.axis_index("y")
    x, c = lax.axis_index("x"), lax.axis_index("c")
    me = z * 8 + y
    home = x // 2
    at_home = c == home
    near = 1 - x % 2

    def send(src, dst, send_sem, recv_sem, **to):
        pltpu.make_async_remote_copy(
            src_ref=src, dst_ref=dst, send_sem=send_sem, recv_sem=recv_sem, device_id=to
        ).start()

    def arrived(ref, sem):
        pltpu.make_async_copy(ref, ref, sem).wait()

    def along_first(k):
        return {"z": (z + c * k) % 8, "y": (y + (1 - c) * k) % 8}

    def along_second(k):
        return {"z": (z + (1 - c) * k) % 8, "y": (y + c * k) % 8}

    barrier = pltpu.get_barrier_semaphore()
    friends = [{"x": (x + d) % 4, "c": h} for d in (1, 2, 3) for h in (0, 1)]
    friends += [{"c": 1 - c}]
    for k in range(1, 8):
        friends += [along_first(k), along_first(k) | {"c": home}]
    for k in (1, 7):
        friends += [along_second(k), along_second(k) | {"c": home}]
    for friend in friends:
        pl.semaphore_signal(barrier, inc=1, device_id=friend)

    own = w_all.at[me]
    odd = x % 2
    small = (
        (ak_ref, kv_raw.at[0]),
        (av_ref, kv_raw.at[1]),
        (decay_ref, decay_raw),
        (ret_gain_ref, ret_gain_raw),
        (sink_ref, sink_raw),
        (inverse_ref, inverse),
        (gain_ref, gain),
        (tok_ref, tok),
    )
    small = [
        pltpu.make_async_copy(src, dst, s_local.at[1 + n]) for n, (src, dst) in enumerate(small)
    ]
    loads = []
    for n, ref in enumerate((rk_ref, rv_ref, rq_ref, aq_ref)):
        cols = pl.ds(pl.multiple_of(odd * 256, 256), 256)
        for half in range(2):
            loads.append(
                pltpu.make_async_copy(
                    ref.at[pl.ds(16 * half, 16), cols],
                    own.at[half, :, pl.ds(256 * n, 256)],
                    s_local.at[0],
                )
            )
    for load in small[:2]:
        load.start()

    @pl.when(at_home)
    def _():
        for load in loads:
            load.start()

    for load in small[2:]:
        load.start()
    for load in small[:7]:
        load.wait()
    position = lax.broadcasted_iota(jnp.int32, (ROWS, 128), 0) + me * ROWS
    angle = position.astype(F32) * inverse[...]
    cosine[...] = jnp.cos(angle)
    sine[...] = jnp.sin(angle)
    pack_own[...] = jnp.zeros((2, 8, 256), F32)
    for i in range(2):
        pack_own[i, 0:1, :] = decay_raw[i : i + 1, :]
        pack_own[i, 1:2, :] = ret_gain_raw[:, 256 * i : 256 * i + 256]
        pack_own[i, 2:3, 0:4] = sink_raw[:, 4 * i : 4 * i + 4]

    @pl.when(at_home)
    def _():
        arrived(own.at[:, :, pl.ds(0, 1024)], s_local.at[0])
        both = [jnp.where(odd == 0, kv_raw[n, :, :HD], kv_raw[n, :, HD:]) for n in range(2)]
        both = jnp.concatenate(both, axis=1)
        for half in range(2):
            w_all[me, half, :, 1024:COLS] = both[16 * half : 16 * half + 16]

    small[7].wait()
    pl.semaphore_wait(barrier, jnp.where(at_home, 34, 16))

    @pl.when(at_home)
    def _():
        for k in (1, 7, 2, 6, 3, 5, 4):
            for h in range(2):
                ref = w_all.at[me, h]
                to = {"z": (z + h * k) % 8, "y": (y + (1 - h) * k) % 8, "c": h}
                send(ref, ref, s_open, r_near.at[8 - k], **to)
        for direction, k in ((0, 1), (1, 7)):
            for h in range(2):
                ref = w_all.at[me, h]
                to = {"z": (z + (1 - h) * k) % 8, "y": (y + h * k) % 8, "c": h}
                send(ref, ref, s_open, r_far.at[direction, 0, 0], **to)
        send(own, own, s_small.at[0], r_own, c=1 - c)

    part = ROWS // CHUNKS

    def token_rows(slot, half, q):
        return x_in.at[slot, half, pl.ds(part * q, part)]

    for q in range(CHUNKS):
        for d in (1, 3):
            send(
                tok.at[pl.ds(part * q, part)],
                token_rows(x % 2, c, q),
                s_tok.at[0],
                r_tok.at[x % 2, c, q],
                x=(x + d) % 4,
                c=home,
            )

    @pl.when(at_home)
    def _():
        for q in range(CHUNKS):
            pltpu.make_async_copy(
                tok.at[pl.ds(part * q, part)], token_rows(x % 2, c, q), r_tok.at[x % 2, c, q]
            ).start()

    @pl.when(jnp.logical_not(at_home))
    def _():
        for q in range(CHUNKS):
            send(
                tok.at[pl.ds(part * q, part)],
                token_rows(x % 2, c, q),
                s_tok.at[1],
                r_tok.at[x % 2, c, q],
                c=1 - c,
            )

    three = pl.ds(0, 3)
    first_at = c * z + (1 - c) * y
    second_at = (1 - c) * z + c * y
    line = second_at * 8 + first_at

    @pl.when(line < 32)
    def _():
        for d in (1, 2, 3):
            src = ro_ref.at[32 + line % 32]
            send(src, o_far.at[c, line, 3 - d], s_slice, r_slice.at[3 - d], x=(x + d) % 4)

    @pl.when(line >= 32)
    def _():
        for d in (1, 2, 3):
            src = ao_ref.at[32 + line % 32]
            send(src, o_far.at[c, line, 3 - d], s_slice, r_slice.at[3 - d], x=(x + d) % 4)

    def o_block(ka):
        return o_far.at[c, second_at * 8 + (first_at + ka) % 8, three]

    def o_group(kb, g):
        at = pl.multiple_of(((second_at + kb) % 8) * 8 + 4 * g, 4)
        return o_far.at[c, pl.ds(at, 4), three]

    def o_forward(ref, direction, kb, g):
        send(ref, ref, s_o, r_o_far.at[direction, kb - 1, g], **along_second(7 if direction else 1))

    def o_mirror(ref):
        send(ref, ref, s_o_mirror, r_o_mirror, c=1 - c)

    def o_step(kb):
        for g in range(2):
            for direction in range(2):
                limit = limits(g)[direction]
                if kb > limit:
                    continue
                ref = o_group(kb if direction else 8 - kb, g)
                arrived(ref, r_o_far.at[direction, kb - 1, g])
                if kb < limit:
                    o_forward(ref, direction, kb + 1, g)
                o_mirror(ref)

    for i in range(2):
        mine = jnp.logical_and(at_home, x % 2 == i)

        @pl.when(mine)
        def _(i=i):
            pltpu.make_async_copy(pack_own.at[i], pack.at[i], r_pack.at[i]).start()

        @pl.when(jnp.logical_not(mine))
        def _(i=i):
            send(
                pack_own.at[i],
                pack.at[x % 2],
                s_small.at[1 + i],
                r_pack.at[x % 2],
                x=2 * c + i,
                c=home,
            )

        @pl.when(jnp.logical_and(me == 0, mine))
        def _(i=i):
            pltpu.make_async_copy(start_ref.at[i], start.at[i], r_start.at[i]).start()

        @pl.when(jnp.logical_and(me == 0, jnp.logical_not(mine)))
        def _(i=i):
            send(
                start_ref.at[i],
                start.at[x % 2],
                s_small.at[3 + i],
                r_start.at[x % 2],
                x=2 * c + i,
                c=home,
            )

    def block(ka, kb):
        zz = (z + c * ka + (1 - c) * kb) % 8
        yy = (y + (1 - c) * ka + c * kb) % 8
        return w_all.at[zz * 8 + yy, c]

    def mirror(ref):
        send(ref, ref, s_mirror, r_mirror, c=1 - c)

    def limits(n):
        return (4, 3) if n % 2 == 0 else (3, 4)

    def forward(ref, direction, kb, n):
        send(ref, ref, s_w, r_far.at[direction, kb - 1, n], **along_second(7 if direction else 1))

    for n in range(1, 8):
        ka = STEPS[n]
        ref = block(ka, 0)
        arrived(ref, r_near.at[ka])
        forward(ref, 0, 1, n)
        forward(ref, 1, 1, n)
        mirror(ref)

    onward = at_home == (x % 2 == 0)
    relay_half = jnp.where(onward, 1, 0)
    relay_to = (x + jnp.where(onward, 3, 1)) % 4

    def relay(q):
        ref = token_rows(near, relay_half, q)
        arrived(ref, r_tok.at[near, relay_half, q])
        send(ref, ref, s_tok.at[2], r_tok.at[near, relay_half, q], x=relay_to)

    def norm_rows(slot, t):
        if t % 2 == 0:
            q = t // 2

            @pl.when(slot == near)
            def _():
                arrived(token_rows(near, 1 - relay_half, q), r_tok.at[near, 1 - relay_half, q])

            @pl.when(slot != near)
            def _():
                for half in range(2):
                    arrived(token_rows(1 - near, half, q), r_tok.at[1 - near, half, q])

        rows = pl.ds(32 * t, 32)
        a = x_in[slot, 0, rows].astype(F32)
        b = x_in[slot, 1, rows].astype(F32)
        total = jnp.sum(a * a, axis=-1, keepdims=True) + jnp.sum(b * b, axis=-1, keepdims=True)
        scale = lax.rsqrt(total * (1.0 / D) + EPS)
        to = pl.ds(pl.multiple_of(slot * ROWS + 32 * t, 32), 32)
        normed[to, 0:1024] = (a * scale * gain[:, 0:1024]).astype(BF)
        normed[to, 1024:2048] = (b * scale * gain[:, 1024:2048]).astype(BF)

    def ring(kb, n):
        for direction in range(2):
            limit = limits(n)[direction]
            if kb > limit:
                continue
            ref = block(STEPS[n], kb if direction else 8 - kb)
            arrived(ref, r_far.at[direction, kb - 1, n])
            if kb < limit:
                forward(ref, direction, kb + 1, n)
            mirror(ref)

    relay(0)
    for n in range(8):
        ring(1, n)
    relay(1)

    arrived(pack.at[0], r_pack.at[0])
    arrived(pack.at[1], r_pack.at[1])
    ti = lax.broadcasted_iota(jnp.int32, (ROWS, ROWS), 0)
    tj = lax.broadcasted_iota(jnp.int32, (ROWS, ROWS), 1)
    exact = lax.Precision.HIGHEST

    def decays(slot):
        rows = pack[slot]
        lower = (ti >= tj).astype(F32)
        upper = (ti <= tj).astype(F32)
        down = dot(lower, rows, (((1,), (1,)), ((), ())), exact)[:, 0:1]
        across = dot(rows, upper, precision=exact)[0:1, :]
        last = down[ROWS - 1 : ROWS, :]
        inside[slot] = jnp.where(ti >= tj, jnp.exp(jnp.where(ti >= tj, down - across, 0.0)), 0.0)
        grow[slot] = jnp.broadcast_to(jnp.exp(down), (ROWS, 128))
        fall[slot] = jnp.broadcast_to(jnp.exp(last - down), (ROWS, 128))
        own_rate[slot] = jnp.broadcast_to(jnp.exp(last), (1, 128))

    for n in range(8):
        ring(2, n)
        if n == 1:
            decays(0)
        if n == 3:
            relay(2)
        if n == 5:
            decays(1)
    for n in range(8):
        ring(3, n)
        if n == 3:
            relay(3)
    for d in range(3):
        arrived(o_far.at[c, line, d], r_slice.at[d])
    for k in (4, 3, 5, 2, 6, 1, 7):
        send(o_block(0), o_block(0), s_o, r_o_near.at[8 - k], **along_first(k))
    for n in range(8):
        ring(4, n)
        norm_rows(near, n)
    low, high = pl.ds(0, 32), pl.ds(32, 32)
    for n, ref in enumerate((ro_ref, ao_ref)):
        for d in (1, 2, 3):
            send(
                ref.at[low],
                o_near.at[c, n, 3 - d],
                s_out,
                r_out.at[3 - d],
                x=(x + d) % 4,
                c=home,
            )
        pairs = (
            (ref.at[low], o_near.at[c, n, 3], r_out.at[3]),
            (ref.at[high], o_far.at[c, pl.ds(32 * n, 32), 3], r_own_far),
        )

        @pl.when(at_home)
        def _(pairs=pairs):
            for src, dst, sem in pairs:
                pltpu.make_async_copy(src, dst, sem).start()

        @pl.when(jnp.logical_not(at_home))
        def _(pairs=pairs):
            for src, dst, sem in pairs:
                send(src, dst, s_small.at[5], sem, c=1 - c)

    for n in range(8):
        norm_rows(1 - near, n)
    few = pl.ds(0, 63)
    arrived(w_all.at[few, 0], r_mirror)

    @pl.when(jnp.logical_not(at_home))
    def _():
        arrived(own, r_own)

    def project(at, width):
        w = w_all[:, :, :, at : at + width].reshape(D, width)
        return dot(normed[...], w).astype(BF)

    keys[...] = project(0, 256)
    values[...] = project(256, 256)

    def rotated(ref, slot):
        rows = ref[pl.ds(ROWS * slot, ROWS)].astype(F32)
        front, rear = rows[:, :128], rows[:, 128:]
        return (
            front * cosine[...] - rear * sine[...],
            front * sine[...] + rear * cosine[...],
        )

    for slot in range(2):
        front, rear = [part * DK ** (-0.5) for part in rotated(keys, slot)]
        v = values[pl.ds(ROWS * slot, ROWS)]
        left = jnp.concatenate(
            [(front * fall[slot]).astype(BF), (rear * fall[slot]).astype(BF)], axis=1
        )
        state[slot] = dot(left, v, (((0,), (0,)), ((), ())))
        keys[pl.ds(ROWS * slot, ROWS)] = jnp.concatenate(
            [front.astype(BF), rear.astype(BF)], axis=1
        )

        @pl.when(me == 0)
        def _(slot=slot):
            arrived(start.at[slot], r_start.at[slot])
            state[slot] = state[slot] + own_rate[slot][:, 0:1] * start[slot]

        for i in range(16):
            for half in range(2):
                pieces[slot * 32 + i * 2 + half] = state[
                    slot, 16 * i : 16 * i + 16, 128 * half : 128 * half + 128
                ].astype(BF)

    for k in range(1, 8):
        arrived(o_block(k), r_o_near.at[k])
    for g in range(2):
        o_forward(o_group(0, g), 0, 1, g)
        o_forward(o_group(0, g), 1, 1, g)
        o_mirror(o_group(0, g))
    def place(index):
        return {"z": index // 8, "y": index % 8}

    def reach(k):
        return min(k // 8, 8 - k // 8) + min(k % 8, 8 - k % 8)

    offsets = sorted(range(1, 64), key=lambda k: (-reach(k), k))

    def peer(k):
        zz, yy = (z + k // 8) % 8, (y + k % 8) % 8
        return zz * 8 + yy, {"z": zz, "y": yy}

    for k in offsets:
        to, at = peer(k)
        send(pieces.at[to], came.at[me], s_scan.at[1], r_scan.at[1], **at)
    for k in offsets:
        to, at = peer(k)
        send(own_rate.at[to // 32], rates.at[me], s_scan.at[0], r_scan.at[0], **at)
    came[me] = pieces[me]
    rates[me] = own_rate[me // 32]

    att_kv[:, pl.ds(WINDOW, ROWS)] = project(1024, 128).reshape(2, ROWS, 128)
    tail = att_kv.at[:, pl.ds(ROWS, WINDOW)]
    lead = att_kv.at[:, pl.ds(0, WINDOW)]

    @pl.when(me < 63)
    def _():
        send(tail, lead, s_halo, r_halo, **place(me + 1))

    @pl.when(me == 0)
    def _():
        att_kv[:, pl.ds(0, WINDOW)] = jnp.zeros((2, WINDOW, 128), BF)

    both = project(512, 512)
    queries[...] = both[:, :256]
    att_q[...] = both[:, 256:]

    for slot in range(2):
        front, rear = rotated(queries, slot)
        q = jnp.concatenate([front.astype(BF), rear.astype(BF)], axis=1)
        k = keys[pl.ds(ROWS * slot, ROWS)]
        raw = dot(q, k, (((1,), (1,)), ((), ()))) * inside[slot]
        scores[slot] = dot(raw.astype(BF), values[pl.ds(ROWS * slot, ROWS)])
        queries[pl.ds(ROWS * slot, ROWS)] = jnp.concatenate(
            [(front * grow[slot]).astype(BF), (rear * grow[slot]).astype(BF)], axis=1
        )

    o_step(1)
    arrived(rates.at[few], r_scan.at[0])
    arrived(came.at[few], r_scan.at[1])

    def advance(k, carried):
        back[k] = carried.astype(BF)
        return carried * rates[k] + came[k].astype(F32)

    lax.fori_loop(0, 64, advance, jnp.zeros((16, 128), F32))

    for k in offsets:
        to, at = peer(k)
        send(back.at[to], prior.at[me], s_scan.at[2], r_scan.at[2], **at)
    prior[me] = back[me]

    o_step(2)
    @pl.when(me > 0)
    def _():
        arrived(lead, r_halo)


    qi = lax.broadcasted_iota(jnp.int32, (WINDOW, 2 * WINDOW), 0)
    ki = lax.broadcasted_iota(jnp.int32, (WINDOW, 2 * WINDOW), 1)
    for slot in range(2):
        sink = jnp.exp(pack[slot, 2:3, 0:4])
        for n in range(2):
            allowed = jnp.logical_and(ki > qi, ki <= qi + WINDOW)
            if n == 0:
                allowed = jnp.logical_and(allowed, ki >= jnp.where(me == 0, WINDOW, 0))
            kv = att_kv[slot, pl.ds(WINDOW * n, 2 * WINDOW)]
            rows = att_q[pl.ds(ROWS * slot + WINDOW * n, WINDOW)]
            heads_in = [rows[:, HD * g : HD * g + HD] for g in range(4)]
            near_keys, near_values = kv[:, :HD], kv[:, HD:]
            score = [dot(q, near_keys, (((1,), (1,)), ((), ()))) for q in heads_in]
            expo = [jnp.exp(jnp.where(allowed, a * HD ** (-0.5), -1e30)) for a in score]
            total = [
                jnp.sum(e, axis=-1, keepdims=True) + sink[:, g : g + 1] for g, e in enumerate(expo)
            ]
            share = [(e * (1.0 / t)).astype(BF) for e, t in zip(expo, total)]
            outs = [dot(p, near_values) for p in share]
            hidden[slot, 1, pl.ds(WINDOW * n, WINDOW)] = jnp.concatenate(outs, axis=1).astype(BF)

    def hand_over(kind):
        for i in range(2):
            to = 2 * c + i
            for half in range(2):
                rows = pl.ds(WINDOW * half, WINDOW)
                src = hidden.at[i, kind, rows]
                dst = heads.at[x, kind, rows]
                here = jnp.logical_and(to == x, c == half)

                @pl.when(here)
                def _(src=src, dst=dst):
                    pltpu.make_async_copy(src, dst, r_hid.at[kind, x]).start()

                @pl.when(jnp.logical_not(here))
                def _(src=src, dst=dst, half=half, i=i):
                    send(src, dst, s_hid.at[kind, i, half], r_hid.at[kind, x], x=to, c=half)

    def pass_on(kind):
        rows = pl.ds(pl.multiple_of(WINDOW * c, WINDOW), WINDOW)
        for j in range(4):
            ref = heads.at[j, kind, rows]
            arrived(ref, r_hid.at[kind, j])
            send(ref, ref, s_pass, r_pass.at[kind, j], c=1 - c)

    def passed(kind):
        rows = pl.ds(pl.multiple_of(WINDOW * (1 - c), WINDOW), WINDOW)
        for j in range(4):
            arrived(heads.at[j, kind, rows], r_pass.at[kind, j])

    hand_over(1)

    o_step(3)
    arrived(prior.at[few], r_scan.at[2])
    for slot in range(2):
        for i in range(16):
            for half in range(2):
                state[slot, 16 * i : 16 * i + 16, 128 * half : 128 * half + 128] = prior[
                    slot * 32 + i * 2 + half
                ].astype(F32)

        @pl.when(me == 0)
        def _(slot=slot):
            state[slot] = start[slot]

        raw = scores[slot] + dot(queries[pl.ds(ROWS * slot, ROWS)], state[slot].astype(BF))
        centred = raw - jnp.mean(raw, axis=-1, keepdims=True)
        variance = jnp.mean(centred * centred, axis=-1, keepdims=True)
        shaped = centred * lax.rsqrt(variance + EPS) * pack[slot, 1:2, :]
        hidden[slot, 0] = shaped.astype(BF)

    hand_over(0)

    o_step(4)
    for d in range(2):
        rel = (2 * c + d + 3 - x) % 4
        arrived(o_near.at[:, :, rel], r_out.at[rel])

    @pl.when(at_home)
    def _():
        arrived(o_far.at[:, :, 3], r_own_far)

    arrived(o_far.at[1 - c, :, three], r_o_mirror)

    def product(kind, d):
        rel = (2 * c + d + 3 - x) % 4
        total = None
        for half in range(2):
            near_rows = o_near[half, kind, rel].reshape(256, 512)
            far_rows = o_far[half, pl.ds(32 * kind, 32), rel].reshape(256, 512)
            one = dot(heads[2 * half, kind], near_rows) + dot(heads[2 * half + 1, kind], far_rows)
            total = one if total is None else total + one
        return total

    pass_on(1)
    passed(1)
    for d in range(2):
        partial[d] = product(1, d)

    pass_on(0)
    passed(0)
    for d in range(2):
        out_ref[:, 512 * d : 512 * d + 512] = (partial[d] + product(0, d)).astype(BF)

    arrived(x_in.at[0], s_tok.at[0])
    arrived(tok, s_tok.at[2])
    arrived(w_all.at[pl.ds(0, 54), 0], s_w)
    arrived(w_all.at[few, 0], s_mirror)
    arrived(heads.at[pl.ds(0, 2)], s_pass)
    arrived(rates.at[few], s_scan.at[0])
    arrived(came.at[few], s_scan.at[1])
    arrived(prior.at[few], s_scan.at[2])

    @pl.when(jnp.logical_not(at_home))
    def _():
        arrived(tok, s_tok.at[1])
        arrived(o_near.at[0, :, pl.ds(0, 2)], s_small.at[5])

    @pl.when(at_home)
    def _():
        arrived(own, s_small.at[0])
        arrived(w_all.at[pl.ds(0, 18), 0], s_open)

    arrived(o_near.at[0, :, three], s_out)
    arrived(o_far.at[0, 0, three], s_slice)
    arrived(o_far.at[0, few, three], s_o)
    arrived(o_far.at[0, :, three], s_o_mirror)
    for i in range(2):
        mine = jnp.logical_and(at_home, x % 2 == i)

        @pl.when(jnp.logical_not(mine))
        def _(i=i):
            arrived(pack.at[i], s_small.at[1 + i])

        @pl.when(jnp.logical_and(me == 0, jnp.logical_not(mine)))
        def _(i=i):
            arrived(start.at[i], s_small.at[3 + i])

        for kind in range(2):
            for half in range(2):
                here = jnp.logical_and(2 * c + i == x, c == half)

                @pl.when(jnp.logical_not(here))
                def _(i=i, kind=kind, half=half):
                    rows = pl.ds(WINDOW * half, WINDOW)
                    arrived(hidden.at[i, kind, rows], s_hid.at[kind, i, half])

    @pl.when(me < 63)
    def _():
        arrived(tail, s_halo)


def shards(
    tokens,
    norm_gain,
    ret_query,
    ret_key,
    ret_value,
    att_query,
    att_key,
    att_value,
    log_decay,
    start_state,
    ret_gain,
    sink_logits,
    ret_out,
    att_out,
):
    steps = np.arange(128, dtype=np.float32) / np.float32(128)
    inverse = jnp.asarray((np.float32(1) / np.float32(10000) ** steps).reshape(1, 128))
    vmem = pl.BlockSpec(memory_space=pltpu.VMEM)
    hbm = pl.BlockSpec(memory_space=pl.ANY)
    dma = pltpu.SemaphoreType.DMA
    scratch = [
        pltpu.VMEM((ROWS, 1024), BF),
        pltpu.VMEM((2, 2, ROWS, 1024), BF),
        pltpu.VMEM((2 * ROWS, D), BF),
        pltpu.VMEM((64, 2, 16, COLS), BF),
        pltpu.VMEM((2, 8, 256), F32),
        pltpu.VMEM((2, 256, 256), F32),
        pltpu.VMEM((2, 2, 4, 32, 8, 512), BF),
        pltpu.VMEM((2, 64, 4, 8, 512), BF),
        pltpu.VMEM((2, 32, 128), BF),
        pltpu.VMEM((2, 256), F32),
        pltpu.VMEM((1, 512), F32),
        pltpu.VMEM((1, 8), F32),
        pltpu.VMEM((2, 8, 256), F32),
        pltpu.VMEM((1, D), F32),
        pltpu.VMEM((1, 128), F32),
        pltpu.VMEM((2, ROWS, ROWS), F32),
        pltpu.VMEM((2, ROWS, 128), F32),
        pltpu.VMEM((2, ROWS, 128), F32),
        pltpu.VMEM((2, ROWS, 512), F32),
        pltpu.VMEM((ROWS, 128), F32),
        pltpu.VMEM((ROWS, 128), F32),
        pltpu.VMEM((2 * ROWS, 256), BF),
        pltpu.VMEM((2 * ROWS, 256), BF),
        pltpu.VMEM((2 * ROWS, 256), BF),
        pltpu.VMEM((2 * ROWS, 256), BF),
        pltpu.VMEM((2, WINDOW + ROWS, 128), BF),
        pltpu.VMEM((2, 256, 256), F32),
        pltpu.VMEM((2, ROWS, 256), F32),
        pltpu.VMEM((64, 16, 128), BF),
        pltpu.VMEM((64, 16, 128), BF),
        pltpu.VMEM((64, 1, 128), F32),
        pltpu.VMEM((2, 1, 128), F32),
        pltpu.VMEM((64, 16, 128), BF),
        pltpu.VMEM((64, 16, 128), BF),
        pltpu.VMEM((2, 2, ROWS, 256), BF),
        pltpu.VMEM((4, 2, ROWS, 256), BF),
        dma((9,)),
        dma((3,)),
        dma((2, 2, CHUNKS)),
        dma((6,)),
        dma((2,)),
        dma((2,)),
        dma,
        dma,
        dma,
        dma((8,)),
        dma((2, 4, 8)),
        dma,
        dma,
        dma((3,)),
        dma((3,)),
        dma,
        dma,
        dma((2, 2, 2)),
        dma((2, 4)),
        dma,
        dma((2, 4)),
        dma,
        dma((4,)),
        dma,
        dma,
        dma((3,)),
        dma,
        dma((8,)),
        dma((2, 4, 2)),
        dma,
        dma,
    ]
    mixed = pl.pallas_call(
        layer_kernel,
        out_shape=pltpu.VMEM((ROWS, 1024), BF),
        in_specs=[hbm] * 15,
        out_specs=vmem,
        scratch_shapes=scratch,
        compiler_params=pltpu.CompilerParams(
            collective_id=0, has_side_effects=True, vmem_limit_bytes=60 * 1024 * 1024
        ),
    )(
        tokens[0],
        ret_key,
        ret_value,
        ret_query,
        att_query,
        att_key,
        att_value,
        log_decay[0],
        ret_gain.reshape(1, 512),
        sink_logits.reshape(1, 8),
        start_state[0],
        ret_out.reshape(64, 8, 512),
        att_out.reshape(64, 8, 512),
        norm_gain.reshape(1, D),
        inverse,
    )
    return mixed[None]


def solution(mesh):
    torus = Mesh(
        mesh.devices.reshape(8, 8, mesh.shape["fs"], mesh.shape["tp"]), ("z", "y", "x", "c")
    )
    across = P(SP, "c")
    in_specs = (
        P("x", SP, "c"),
        P(),
        across,
        across,
        across,
        across,
        across,
        across,
        P("x", "c", SP),
        P("x", "c", None, None),
        P("c"),
        P("c"),
        P("c", "x"),
        P("c", "x"),
    )
    return jax.shard_map(
        shards, mesh=torus, in_specs=in_specs, out_specs=P("x", SP, "c"), check_vma=False
    )
```

```python
import jax
import jax.numpy as jnp
import numpy as np
from jax import lax
from jax.experimental import pallas as pl
from jax.experimental.pallas import tpu as pltpu
from jax.sharding import Mesh
from jax.sharding import PartitionSpec as P

D = 2048
DK = 256
HD = 64
ROWS = 256
WINDOW = 128
COLS = 1152
CHUNKS = 4
SP = ("z", "y")
BF = jnp.bfloat16
F32 = jnp.float32
EPS = 1e-06
STEPS = (0, 7, 1, 6, 2, 5, 3, 4)


def dot(a, b, dims=(((1,), (0,)), ((), ())), precision=None):
    return lax.dot_general(a, b, dims, precision=precision, preferred_element_type=F32)


def layer_kernel(
    tok_ref,
    rk_ref,
    rv_ref,
    rq_ref,
    aq_ref,
    ak_ref,
    av_ref,
    decay_ref,
    ret_gain_ref,
    sink_ref,
    start_ref,
    ro_ref,
    ao_ref,
    gain_ref,
    inverse_ref,
    out_ref,
    tok,
    x_in,
    normed,
    w_all,
    pack,
    start,
    o_near,
    o_far,
    kv_raw,
    decay_raw,
    ret_gain_raw,
    sink_raw,
    pack_own,
    gain,
    inverse,
    inside,
    grow,
    fall,
    partial,
    cosine,
    sine,
    keys,
    values,
    queries,
    att_q,
    att_kv,
    state,
    scores,
    pieces,
    came,
    rates,
    own_rate,
    back,
    prior,
    hidden,
    heads,
    s_local,
    s_tok,
    r_tok,
    s_small,
    r_pack,
    r_start,
    s_open,
    s_w,
    r_own,
    r_near,
    r_far,
    s_mirror,
    r_mirror,
    s_scan,
    r_scan,
    s_halo,
    r_halo,
    s_hid,
    r_hid,
    s_pass,
    r_pass,
    s_out,
    r_out,
    r_own_far,
    s_slice,
    r_slice,
    s_relay,
    s_o_near,
    s_o,
    r_o_near,
    r_o_far,
    s_o_mirror,
    r_o_mirror,
):
    z, y = lax.axis_index("z"), lax.axis_index("y")
    x, c = lax.axis_index("x"), lax.axis_index("c")
    me = z * 8 + y
    home = x // 2
    at_home = c == home
    near = 1 - x % 2

    def send(src, dst, send_sem, recv_sem, **to):
        pltpu.make_async_remote_copy(
            src_ref=src, dst_ref=dst, send_sem=send_sem, recv_sem=recv_sem, device_id=to
        ).start()

    def arrived(ref, sem):
        pltpu.make_async_copy(ref, ref, sem).wait()

    def along_first(k):
        return {"z": (z + c * k) % 8, "y": (y + (1 - c) * k) % 8}

    def along_second(k):
        return {"z": (z + (1 - c) * k) % 8, "y": (y + c * k) % 8}

    barrier = pltpu.get_barrier_semaphore()
    friends = [{"x": (x + d) % 4, "c": h} for d in (1, 2, 3) for h in (0, 1)]
    friends += [{"c": 1 - c}]
    for k in range(1, 8):
        friends += [along_first(k), along_first(k) | {"c": home}]
    for k in (1, 7):
        friends += [along_second(k), along_second(k) | {"c": home}]
    for friend in friends:
        pl.semaphore_signal(barrier, inc=1, device_id=friend)

    own = w_all.at[me]
    odd = x % 2
    small = (
        (ak_ref, kv_raw.at[0]),
        (av_ref, kv_raw.at[1]),
        (decay_ref, decay_raw),
        (ret_gain_ref, ret_gain_raw),
        (sink_ref, sink_raw),
        (inverse_ref, inverse),
        (gain_ref, gain),
        (tok_ref, tok),
    )
    small = [
        pltpu.make_async_copy(src, dst, s_local.at[1 + n]) for n, (src, dst) in enumerate(small)
    ]
    loads = []
    for n, ref in enumerate((rk_ref, rv_ref, rq_ref, aq_ref)):
        cols = pl.ds(pl.multiple_of(odd * 256, 256), 256)
        for half in range(2):
            loads.append(
                pltpu.make_async_copy(
                    ref.at[pl.ds(16 * half, 16), cols],
                    own.at[half, :, pl.ds(256 * n, 256)],
                    s_local.at[0],
                )
            )
    for load in small[:2]:
        load.start()

    @pl.when(at_home)
    def _():
        for load in loads:
            load.start()

    for load in small[2:]:
        load.start()
    for load in small[:7]:
        load.wait()
    position = lax.broadcasted_iota(jnp.int32, (ROWS, 128), 0) + me * ROWS
    angle = position.astype(F32) * inverse[...]
    cosine[...] = jnp.cos(angle)
    sine[...] = jnp.sin(angle)
    pack_own[...] = jnp.zeros((2, 8, 256), F32)
    for i in range(2):
        pack_own[i, 0:1, :] = decay_raw[i : i + 1, :]
        pack_own[i, 1:2, :] = ret_gain_raw[:, 256 * i : 256 * i + 256]
        pack_own[i, 2:3, 0:4] = sink_raw[:, 4 * i : 4 * i + 4]

    @pl.when(at_home)
    def _():
        arrived(own.at[:, :, pl.ds(0, 1024)], s_local.at[0])
        both = [jnp.where(odd == 0, kv_raw[n, :, :HD], kv_raw[n, :, HD:]) for n in range(2)]
        both = jnp.concatenate(both, axis=1)
        for half in range(2):
            w_all[me, half, :, 1024:COLS] = both[16 * half : 16 * half + 16]

    small[7].wait()
    pl.semaphore_wait(barrier, jnp.where(at_home, 34, 16))

    @pl.when(at_home)
    def _():
        for k in (4, 3, 5, 2, 6, 1, 7):
            for h in range(2):
                ref = w_all.at[me, h]
                to = {"z": (z + h * k) % 8, "y": (y + (1 - h) * k) % 8, "c": h}
                send(ref, ref, s_open, r_near.at[8 - k], **to)
        for direction, k in ((0, 1), (1, 7)):
            for h in range(2):
                ref = w_all.at[me, h]
                to = {"z": (z + (1 - h) * k) % 8, "y": (y + h * k) % 8, "c": h}
                send(ref, ref, s_open, r_far.at[direction, 0, 0], **to)
        send(own, own, s_small.at[0], r_own, c=1 - c)

    for i in range(2):
        mine = jnp.logical_and(at_home, x % 2 == i)

        @pl.when(mine)
        def _(i=i):
            pltpu.make_async_copy(pack_own.at[i], pack.at[i], r_pack.at[i]).start()

        @pl.when(jnp.logical_not(mine))
        def _(i=i):
            send(
                pack_own.at[i],
                pack.at[x % 2],
                s_small.at[1 + i],
                r_pack.at[x % 2],
                x=2 * c + i,
                c=home,
            )

    piece = (
        pl.ds(pl.multiple_of((me % 32) // 2 * 16, 16), 16),
        pl.ds(pl.multiple_of(me % 2 * 128, 128), 128),
    )
    opens = x % 2 == me // 32
    for i in range(2):
        mine = jnp.logical_and(at_home, x % 2 == i)

        @pl.when(jnp.logical_and(opens, mine))
        def _(i=i):
            pltpu.make_async_copy(start_ref.at[i, *piece], start, r_start).start()

        @pl.when(jnp.logical_and(opens, jnp.logical_not(mine)))
        def _(i=i):
            send(
                start_ref.at[i, *piece],
                start,
                s_small.at[3 + i],
                r_start,
                x=2 * c + i,
                c=home,
            )

    three = pl.ds(0, 3)
    first_at = c * z + (1 - c) * y
    second_at = (1 - c) * z + c * y
    holder = first_at < 4
    line = second_at * 4 + first_at % 4

    def slices(ref):
        for d in (1, 2, 3):
            src = ref.at[48 + line % 16]
            send(src, o_far.at[c, line, 3 - d], s_slice, r_slice.at[3 - d], x=(x + d) % 4)

    @pl.when(jnp.logical_and(holder, line < 16))
    def _():
        slices(ro_ref)

    @pl.when(jnp.logical_and(holder, line >= 16))
    def _():
        slices(ao_ref)

    def o_group(kb):
        at = pl.multiple_of(((second_at + kb) % 8) * 4, 4)
        return o_far.at[c, pl.ds(at, 4), three]

    def o_forward(ref, direction, kb):
        send(ref, ref, s_o, r_o_far.at[direction, kb - 1], **along_second(7 if direction else 1))

    def o_mirror(ref):
        send(ref, ref, s_o_mirror, r_o_mirror, c=1 - c)

    def o_open():
        @pl.when(holder)
        def _():
            for d in range(3):
                arrived(o_far.at[c, line, d], r_slice.at[d])
            ref = o_far.at[c, line, three]
            for k in (4, 3, 5, 2, 6, 1, 7):
                send(ref, ref, s_o_near, r_o_near.at[first_at % 4], **along_first(k))

    def o_line():
        for k in range(4):
            @pl.when(first_at != k)
            def _(k=k):
                arrived(o_far.at[c, second_at * 4 + k, three], r_o_near.at[k])

        o_forward(o_group(0), 0, 1)
        o_forward(o_group(0), 1, 1)
        o_mirror(o_group(0))

    def o_step(kb):
        for direction, limit in ((0, 4), (1, 3)):
            if kb > limit:
                continue
            ref = o_group(kb if direction else 8 - kb)
            arrived(ref, r_o_far.at[direction, kb - 1])
            if kb < limit:
                o_forward(ref, direction, kb + 1)
            o_mirror(ref)

    part = ROWS // CHUNKS

    def token_rows(slot, half, q):
        return x_in.at[slot, half, pl.ds(part * q, part)]

    for q in range(CHUNKS):
        for d in (1, 3):
            send(
                tok.at[pl.ds(part * q, part)],
                token_rows(x % 2, c, q),
                s_tok.at[0],
                r_tok.at[x % 2, c, q],
                x=(x + d) % 4,
                c=home,
            )

    @pl.when(at_home)
    def _():
        for q in range(CHUNKS):
            pltpu.make_async_copy(
                tok.at[pl.ds(part * q, part)], token_rows(x % 2, c, q), r_tok.at[x % 2, c, q]
            ).start()

    @pl.when(jnp.logical_not(at_home))
    def _():
        for q in range(CHUNKS):
            send(
                tok.at[pl.ds(part * q, part)],
                token_rows(x % 2, c, q),
                s_tok.at[1],
                r_tok.at[x % 2, c, q],
                c=1 - c,
            )

    def block(ka, kb):
        zz = (z + c * ka + (1 - c) * kb) % 8
        yy = (y + (1 - c) * ka + c * kb) % 8
        return w_all.at[zz * 8 + yy, c]

    def mirror(ref):
        send(ref, ref, s_mirror, r_mirror, c=1 - c)

    def limits(n):
        return (4, 3) if n % 2 == 0 else (3, 4)

    def forward(ref, direction, kb, n):
        send(ref, ref, s_w, r_far.at[direction, kb - 1, n], **along_second(7 if direction else 1))

    arrived(pack.at[0], r_pack.at[0])
    arrived(pack.at[1], r_pack.at[1])
    ti = lax.broadcasted_iota(jnp.int32, (ROWS, ROWS), 0)
    tj = lax.broadcasted_iota(jnp.int32, (ROWS, ROWS), 1)
    exact = lax.Precision.HIGHEST

    def decays(slot):
        rows = pack[slot]
        lower = (ti >= tj).astype(F32)
        upper = (ti <= tj).astype(F32)
        down = dot(lower, rows, (((1,), (1,)), ((), ())), exact)[:, 0:1]
        across = dot(rows, upper, precision=exact)[0:1, :]
        last = down[ROWS - 1 : ROWS, :]
        inside[slot] = jnp.where(ti >= tj, jnp.exp(jnp.where(ti >= tj, down - across, 0.0)), 0.0)
        grow[slot] = jnp.broadcast_to(jnp.exp(down), (ROWS, 128))
        fall[slot] = jnp.broadcast_to(jnp.exp(last - down), (ROWS, 128))
        own_rate[slot] = jnp.broadcast_to(jnp.exp(last), (1, 128))

    for n in range(1, 8):
        ka = STEPS[n]
        ref = block(ka, 0)
        arrived(ref, r_near.at[ka])
        forward(ref, 0, 1, n)
        forward(ref, 1, 1, n)
        mirror(ref)
        if n == 1:
            o_open()
        if n == 2:
            decays(0)
        if n == 4:
            decays(1)

    onward = at_home == (x % 2 == 0)
    relay_half = jnp.where(onward, 1, 0)
    relay_to = (x + jnp.where(onward, 3, 1)) % 4

    def relay(q):
        ref = token_rows(near, relay_half, q)
        arrived(ref, r_tok.at[near, relay_half, q])
        send(ref, ref, s_tok.at[2], r_tok.at[near, relay_half, q], x=relay_to)

    def norm_rows(slot, t):
        if t % 2 == 0:
            q = t // 2

            @pl.when(slot == near)
            def _():
                arrived(token_rows(near, 1 - relay_half, q), r_tok.at[near, 1 - relay_half, q])

            @pl.when(slot != near)
            def _():
                for half in range(2):
                    arrived(token_rows(1 - near, half, q), r_tok.at[1 - near, half, q])

        rows = pl.ds(32 * t, 32)
        a = x_in[slot, 0, rows].astype(F32)
        b = x_in[slot, 1, rows].astype(F32)
        total = jnp.sum(a * a, axis=-1, keepdims=True) + jnp.sum(b * b, axis=-1, keepdims=True)
        scale = lax.rsqrt(total * (1.0 / D) + EPS)
        to = pl.ds(pl.multiple_of(slot * ROWS + 32 * t, 32), 32)
        normed[to, 0:1024] = (a * scale * gain[:, 0:1024]).astype(BF)
        normed[to, 1024:2048] = (b * scale * gain[:, 1024:2048]).astype(BF)

    def ring(kb, n):
        for direction in range(2):
            limit = limits(n)[direction]
            if kb > limit:
                continue
            ref = block(STEPS[n], kb if direction else 8 - kb)
            arrived(ref, r_far.at[direction, kb - 1, n])
            if kb < limit:
                forward(ref, direction, kb + 1, n)
            mirror(ref)

    relay(0)
    for n in range(8):
        ring(1, n)
    relay(1)

    def send_along_x():
        low, high = pl.ds(0, 48), pl.ds(48, 16)
        for n, ref in enumerate((ro_ref, ao_ref)):
            for d in (1, 3):
                send(
                    ref.at[low],
                    o_near.at[c, n, 3 - d],
                    s_out,
                    r_out.at[3 - d, c, n],
                    x=(x + d) % 4,
                    c=home,
                )
            pairs = (
                (ref.at[low], o_near.at[c, n, 3], r_out.at[3, c, n]),
                (ref.at[high], o_far.at[c, pl.ds(16 * n, 16), 3], r_own_far),
            )

            @pl.when(at_home)
            def _(pairs=pairs):
                for src, dst, sem in pairs:
                    pltpu.make_async_copy(src, dst, sem).start()

            @pl.when(jnp.logical_not(at_home))
            def _(pairs=pairs):
                for src, dst, sem in pairs:
                    send(src, dst, s_small.at[5], sem, c=1 - c)

    def o_relay(n):
        at = jnp.where(onward, 0, 2)
        src = o_near.at[relay_half, n, at]
        arrived(src, r_out.at[at, relay_half, n])
        dst = o_near.at[relay_half, n, 1]
        send(src, dst, s_relay, r_out.at[1, relay_half, n], x=relay_to)

    for n in range(8):
        ring(2, n)
        if n == 3:
            relay(2)
    for n in range(8):
        ring(3, n)
        if n == 3:
            relay(3)
            send_along_x()
    o_line()
    for n in range(8):
        ring(4, n)
        norm_rows(near, n)
    for n in range(8):
        norm_rows(1 - near, n)
    few = pl.ds(0, 63)
    arrived(w_all.at[few, 0], r_mirror)

    @pl.when(jnp.logical_not(at_home))
    def _():
        arrived(own, r_own)

    def project(at, width):
        w = w_all[:, :, :, at : at + width].reshape(D, width)
        return dot(normed[...], w).astype(BF)

    keys[...] = project(0, 256)
    values[...] = project(256, 256)

    def rotated(ref, slot):
        rows = ref[pl.ds(ROWS * slot, ROWS)].astype(F32)
        front, rear = rows[:, :128], rows[:, 128:]
        return (
            front * cosine[...] - rear * sine[...],
            front * sine[...] + rear * cosine[...],
        )

    for slot in range(2):
        front, rear = [part * DK ** (-0.5) for part in rotated(keys, slot)]
        v = values[pl.ds(ROWS * slot, ROWS)]
        left = jnp.concatenate(
            [(front * fall[slot]).astype(BF), (rear * fall[slot]).astype(BF)], axis=1
        )
        state[slot] = dot(left, v, (((0,), (0,)), ((), ())))
        keys[pl.ds(ROWS * slot, ROWS)] = jnp.concatenate(
            [front.astype(BF), rear.astype(BF)], axis=1
        )

        for i in range(16):
            for half in range(2):
                pieces[slot * 32 + i * 2 + half] = state[
                    slot, 16 * i : 16 * i + 16, 128 * half : 128 * half + 128
                ].astype(BF)

    o_step(1)
    def place(index):
        return {"z": index // 8, "y": index % 8}

    def reach(k):
        return min(k // 8, 8 - k // 8) + min(k % 8, 8 - k % 8)

    offsets = sorted(range(1, 64), key=lambda k: (-reach(k), k))

    def peer(k):
        zz, yy = (z + k // 8) % 8, (y + k % 8) % 8
        return zz * 8 + yy, {"z": zz, "y": yy}

    for k in offsets:
        to, at = peer(k)
        send(pieces.at[to], came.at[me], s_scan.at[1], r_scan.at[1], **at)
    for k in offsets:
        to, at = peer(k)
        send(own_rate.at[to // 32], rates.at[me], s_scan.at[0], r_scan.at[0], **at)
    came[me] = pieces[me]
    rates[me] = own_rate[me // 32]

    att_kv[:, pl.ds(WINDOW, ROWS)] = project(1024, 128).reshape(2, ROWS, 128)
    tail = att_kv.at[:, pl.ds(ROWS, WINDOW)]
    lead = att_kv.at[:, pl.ds(0, WINDOW)]

    @pl.when(me < 63)
    def _():
        send(tail, lead, s_halo, r_halo, **place(me + 1))

    @pl.when(me == 0)
    def _():
        att_kv[:, pl.ds(0, WINDOW)] = jnp.zeros((2, WINDOW, 128), BF)

    both = project(512, 512)
    queries[...] = both[:, :256]
    att_q[...] = both[:, 256:]

    o_step(2)
    o_relay(0)
    for slot in range(2):
        front, rear = rotated(queries, slot)
        q = jnp.concatenate([front.astype(BF), rear.astype(BF)], axis=1)
        k = keys[pl.ds(ROWS * slot, ROWS)]
        raw = dot(q, k, (((1,), (1,)), ((), ()))) * inside[slot]
        scores[slot] = dot(raw.astype(BF), values[pl.ds(ROWS * slot, ROWS)])
        queries[pl.ds(ROWS * slot, ROWS)] = jnp.concatenate(
            [(front * grow[slot]).astype(BF), (rear * grow[slot]).astype(BF)], axis=1
        )

    o_relay(1)
    o_step(3)
    arrived(rates.at[few], r_scan.at[0])
    arrived(came.at[few], r_scan.at[1])

    def advance(k, carried):
        back[k] = carried.astype(BF)
        return carried * rates[k] + came[k].astype(F32)

    arrived(start, r_start)
    lax.fori_loop(0, 64, advance, start[...])

    for k in offsets:
        to, at = peer(k)
        send(back.at[to], prior.at[me], s_scan.at[2], r_scan.at[2], **at)
    prior[me] = back[me]

    @pl.when(me > 0)
    def _():
        arrived(lead, r_halo)


    qi = lax.broadcasted_iota(jnp.int32, (WINDOW, 2 * WINDOW), 0)
    ki = lax.broadcasted_iota(jnp.int32, (WINDOW, 2 * WINDOW), 1)
    for slot in range(2):
        sink = jnp.exp(pack[slot, 2:3, 0:4])
        for n in range(2):
            allowed = jnp.logical_and(ki > qi, ki <= qi + WINDOW)
            if n == 0:
                allowed = jnp.logical_and(allowed, ki >= jnp.where(me == 0, WINDOW, 0))
            kv = att_kv[slot, pl.ds(WINDOW * n, 2 * WINDOW)]
            rows = att_q[pl.ds(ROWS * slot + WINDOW * n, WINDOW)]
            heads_in = [rows[:, HD * g : HD * g + HD] for g in range(4)]
            near_keys, near_values = kv[:, :HD], kv[:, HD:]
            score = [dot(q, near_keys, (((1,), (1,)), ((), ()))) for q in heads_in]
            expo = [jnp.exp(jnp.where(allowed, a * HD ** (-0.5), -1e30)) for a in score]
            total = [
                jnp.sum(e, axis=-1, keepdims=True) + sink[:, g : g + 1] for g, e in enumerate(expo)
            ]
            share = [(e * (1.0 / t)).astype(BF) for e, t in zip(expo, total)]
            outs = [dot(p, near_values) for p in share]
            hidden[slot, 1, pl.ds(WINDOW * n, WINDOW)] = jnp.concatenate(outs, axis=1).astype(BF)

    def hand_over(kind):
        for i in range(2):
            to = 2 * c + i
            for half in range(2):
                rows = pl.ds(WINDOW * half, WINDOW)
                src = hidden.at[i, kind, rows]
                dst = heads.at[x, kind, rows]
                here = jnp.logical_and(to == x, c == half)

                @pl.when(here)
                def _(src=src, dst=dst):
                    pltpu.make_async_copy(src, dst, r_hid.at[kind, x]).start()

                @pl.when(jnp.logical_not(here))
                def _(src=src, dst=dst, half=half, i=i):
                    send(src, dst, s_hid.at[kind, i, half], r_hid.at[kind, x], x=to, c=half)

    def pass_on(kind):
        rows = pl.ds(pl.multiple_of(WINDOW * c, WINDOW), WINDOW)
        for j in range(4):
            ref = heads.at[j, kind, rows]
            arrived(ref, r_hid.at[kind, j])
            send(ref, ref, s_pass, r_pass.at[kind, j], c=1 - c)

    def passed(kind):
        rows = pl.ds(pl.multiple_of(WINDOW * (1 - c), WINDOW), WINDOW)
        for j in range(4):
            arrived(heads.at[j, kind, rows], r_pass.at[kind, j])

    hand_over(1)

    o_step(4)
    arrived(prior.at[few], r_scan.at[2])
    for slot in range(2):
        for i in range(16):
            for half in range(2):
                state[slot, 16 * i : 16 * i + 16, 128 * half : 128 * half + 128] = prior[
                    slot * 32 + i * 2 + half
                ].astype(F32)

        raw = scores[slot] + dot(queries[pl.ds(ROWS * slot, ROWS)], state[slot].astype(BF))
        centred = raw - jnp.mean(raw, axis=-1, keepdims=True)
        variance = jnp.mean(centred * centred, axis=-1, keepdims=True)
        shaped = centred * lax.rsqrt(variance + EPS) * pack[slot, 1:2, :]
        hidden[slot, 0] = shaped.astype(BF)

    hand_over(0)

    for d in range(2):
        rel = (2 * c + d + 3 - x) % 4
        for half in range(2):
            relayed = jnp.logical_and(rel == jnp.where(onward, 0, 2), relay_half == half)

            @pl.when(jnp.logical_not(relayed))
            def _(rel=rel, half=half):
                for n in range(2):
                    arrived(o_near.at[half, n, rel], r_out.at[rel, half, n])

    @pl.when(at_home)
    def _():
        arrived(o_far.at[:, :, 3], r_own_far)

    arrived(o_far.at[1 - c, :, three], r_o_mirror)

    def product(kind, d):
        rel = (2 * c + d + 3 - x) % 4
        total = None
        for half in range(2):
            even = o_near[half, kind, rel, 0:32].reshape(256, 512)
            front = o_near[half, kind, rel, 32:48].reshape(128, 512)
            rear = o_far[half, pl.ds(16 * kind, 16), rel].reshape(128, 512)
            odd_rows = jnp.concatenate([front, rear], axis=0)
            one = dot(heads[2 * half, kind], even) + dot(heads[2 * half + 1, kind], odd_rows)
            total = one if total is None else total + one
        return total

    pass_on(1)
    passed(1)
    for d in range(2):
        partial[d] = product(1, d)

    pass_on(0)
    passed(0)
    for d in range(2):
        out_ref[:, 512 * d : 512 * d + 512] = (partial[d] + product(0, d)).astype(BF)

    arrived(x_in.at[0], s_tok.at[0])
    arrived(tok, s_tok.at[2])
    arrived(w_all.at[pl.ds(0, 54), 0], s_w)
    arrived(w_all.at[few, 0], s_mirror)
    arrived(heads.at[pl.ds(0, 2)], s_pass)
    arrived(rates.at[few], s_scan.at[0])
    arrived(came.at[few], s_scan.at[1])
    arrived(prior.at[few], s_scan.at[2])

    @pl.when(jnp.logical_not(at_home))
    def _():
        arrived(tok, s_tok.at[1])
        arrived(o_far.at[:, :, pl.ds(0, 2)], s_small.at[5])

    @pl.when(at_home)
    def _():
        arrived(own, s_small.at[0])
        arrived(w_all.at[pl.ds(0, 18), 0], s_open)

    arrived(o_near.at[0, :, pl.ds(0, 2)], s_out)
    arrived(o_near.at[0, :, 1], s_relay)
    arrived(o_far.at[0, pl.ds(0, 28), three], s_o)

    @pl.when(holder)
    def _():
        arrived(o_far.at[0, 0, three], s_slice)
        arrived(o_far.at[0, pl.ds(0, 7), three], s_o_near)

    arrived(o_far.at[0, :, three], s_o_mirror)
    for i in range(2):
        mine = jnp.logical_and(at_home, x % 2 == i)

        @pl.when(jnp.logical_not(mine))
        def _(i=i):
            arrived(pack.at[i], s_small.at[1 + i])

        @pl.when(jnp.logical_and(opens, jnp.logical_not(mine)))
        def _(i=i):
            arrived(start, s_small.at[3 + i])

        for kind in range(2):
            for half in range(2):
                here = jnp.logical_and(2 * c + i == x, c == half)

                @pl.when(jnp.logical_not(here))
                def _(i=i, kind=kind, half=half):
                    rows = pl.ds(WINDOW * half, WINDOW)
                    arrived(hidden.at[i, kind, rows], s_hid.at[kind, i, half])

    @pl.when(me < 63)
    def _():
        arrived(tail, s_halo)


def shards(
    tokens,
    norm_gain,
    ret_query,
    ret_key,
    ret_value,
    att_query,
    att_key,
    att_value,
    log_decay,
    start_state,
    ret_gain,
    sink_logits,
    ret_out,
    att_out,
):
    steps = np.arange(128, dtype=np.float32) / np.float32(128)
    inverse = jnp.asarray((np.float32(1) / np.float32(10000) ** steps).reshape(1, 128))
    vmem = pl.BlockSpec(memory_space=pltpu.VMEM)
    hbm = pl.BlockSpec(memory_space=pl.ANY)
    dma = pltpu.SemaphoreType.DMA
    scratch = [
        pltpu.VMEM((ROWS, 1024), BF),
        pltpu.VMEM((2, 2, ROWS, 1024), BF),
        pltpu.VMEM((2 * ROWS, D), BF),
        pltpu.VMEM((64, 2, 16, COLS), BF),
        pltpu.VMEM((2, 8, 256), F32),
        pltpu.VMEM((16, 128), F32),
        pltpu.VMEM((2, 2, 4, 48, 8, 512), BF),
        pltpu.VMEM((2, 32, 4, 8, 512), BF),
        pltpu.VMEM((2, 32, 128), BF),
        pltpu.VMEM((2, 256), F32),
        pltpu.VMEM((1, 512), F32),
        pltpu.VMEM((1, 8), F32),
        pltpu.VMEM((2, 8, 256), F32),
        pltpu.VMEM((1, D), F32),
        pltpu.VMEM((1, 128), F32),
        pltpu.VMEM((2, ROWS, ROWS), F32),
        pltpu.VMEM((2, ROWS, 128), F32),
        pltpu.VMEM((2, ROWS, 128), F32),
        pltpu.VMEM((2, ROWS, 512), F32),
        pltpu.VMEM((ROWS, 128), F32),
        pltpu.VMEM((ROWS, 128), F32),
        pltpu.VMEM((2 * ROWS, 256), BF),
        pltpu.VMEM((2 * ROWS, 256), BF),
        pltpu.VMEM((2 * ROWS, 256), BF),
        pltpu.VMEM((2 * ROWS, 256), BF),
        pltpu.VMEM((2, WINDOW + ROWS, 128), BF),
        pltpu.VMEM((2, 256, 256), F32),
        pltpu.VMEM((2, ROWS, 256), F32),
        pltpu.VMEM((64, 16, 128), BF),
        pltpu.VMEM((64, 16, 128), BF),
        pltpu.VMEM((64, 1, 128), F32),
        pltpu.VMEM((2, 1, 128), F32),
        pltpu.VMEM((64, 16, 128), BF),
        pltpu.VMEM((64, 16, 128), BF),
        pltpu.VMEM((2, 2, ROWS, 256), BF),
        pltpu.VMEM((4, 2, ROWS, 256), BF),
        dma((9,)),
        dma((3,)),
        dma((2, 2, CHUNKS)),
        dma((6,)),
        dma((2,)),
        dma,
        dma,
        dma,
        dma,
        dma((8,)),
        dma((2, 4, 8)),
        dma,
        dma,
        dma((3,)),
        dma((3,)),
        dma,
        dma,
        dma((2, 2, 2)),
        dma((2, 4)),
        dma,
        dma((2, 4)),
        dma,
        dma((4, 2, 2)),
        dma,
        dma,
        dma((3,)),
        dma,
        dma,
        dma,
        dma((4,)),
        dma((2, 4)),
        dma,
        dma,
    ]
    mixed = pl.pallas_call(
        layer_kernel,
        out_shape=pltpu.VMEM((ROWS, 1024), BF),
        in_specs=[hbm] * 15,
        out_specs=vmem,
        scratch_shapes=scratch,
        compiler_params=pltpu.CompilerParams(
            collective_id=0, has_side_effects=True, vmem_limit_bytes=60 * 1024 * 1024
        ),
    )(
        tokens[0],
        ret_key,
        ret_value,
        ret_query,
        att_query,
        att_key,
        att_value,
        log_decay[0],
        ret_gain.reshape(1, 512),
        sink_logits.reshape(1, 8),
        start_state[0],
        ret_out.reshape(64, 8, 512),
        att_out.reshape(64, 8, 512),
        norm_gain.reshape(1, D),
        inverse,
    )
    return mixed[None]


def solution(mesh):
    torus = Mesh(
        mesh.devices.reshape(8, 8, mesh.shape["fs"], mesh.shape["tp"]), ("z", "y", "x", "c")
    )
    across = P(SP, "c")
    in_specs = (
        P("x", SP, "c"),
        P(),
        across,
        across,
        across,
        across,
        across,
        across,
        P("x", "c", SP),
        P("x", "c", None, None),
        P("c"),
        P("c"),
        P("c", "x"),
        P("c", "x"),
    )
    return jax.shard_map(
        shards, mesh=torus, in_specs=in_specs, out_specs=P("x", SP, "c"), check_vma=False
    )
```

```python
import jax
import jax.numpy as jnp
import numpy as np
from jax import lax
from jax.experimental import pallas as pl
from jax.experimental.pallas import tpu as pltpu
from jax.sharding import Mesh
from jax.sharding import PartitionSpec as P

D = 2048
DK = 256
HD = 64
ROWS = 256
WINDOW = 128
COLS = 1152
CHUNKS = 4
SP = ("z", "y")
BF = jnp.bfloat16
F32 = jnp.float32
EPS = 1e-06
STEPS = (0, 7, 1, 6, 2, 5, 3, 4)


def dot(a, b, dims=(((1,), (0,)), ((), ())), precision=None):
    return lax.dot_general(a, b, dims, precision=precision, preferred_element_type=F32)


def layer_kernel(
    tok_ref,
    rk_ref,
    rv_ref,
    rq_ref,
    aq_ref,
    ak_ref,
    av_ref,
    decay_ref,
    ret_gain_ref,
    sink_ref,
    start_ref,
    ro_ref,
    ao_ref,
    gain_ref,
    inverse_ref,
    out_ref,
    tok,
    x_in,
    normed,
    w_all,
    pack,
    start,
    o_near,
    o_far,
    kv_raw,
    decay_raw,
    ret_gain_raw,
    sink_raw,
    pack_own,
    gain,
    inverse,
    inside,
    grow,
    fall,
    partial,
    cosine,
    sine,
    keys,
    values,
    queries,
    att_q,
    att_kv,
    state,
    scores,
    pieces,
    came,
    rates,
    own_rate,
    back,
    prior,
    hidden,
    heads,
    s_local,
    s_tok,
    r_tok,
    s_small,
    r_pack,
    r_start,
    s_open,
    s_w,
    r_own,
    r_near,
    r_far,
    s_mirror,
    r_mirror,
    s_scan,
    r_scan,
    s_halo,
    r_halo,
    s_hid,
    r_hid,
    s_pass,
    r_pass,
    s_out,
    r_out,
    r_own_far,
    s_slice,
    r_slice,
    s_relay,
    s_o_near,
    s_o,
    r_o_near,
    r_o_far,
    s_o_mirror,
    r_o_mirror,
):
    z, y = lax.axis_index("z"), lax.axis_index("y")
    x, c = lax.axis_index("x"), lax.axis_index("c")
    me = z * 8 + y
    home = x // 2
    at_home = c == home
    near = 1 - x % 2

    def send(src, dst, send_sem, recv_sem, **to):
        pltpu.make_async_remote_copy(
            src_ref=src, dst_ref=dst, send_sem=send_sem, recv_sem=recv_sem, device_id=to
        ).start()

    def arrived(ref, sem):
        pltpu.make_async_copy(ref, ref, sem).wait()

    def along_first(k):
        return {"z": (z + c * k) % 8, "y": (y + (1 - c) * k) % 8}

    def along_second(k):
        return {"z": (z + (1 - c) * k) % 8, "y": (y + c * k) % 8}

    barrier = pltpu.get_barrier_semaphore()
    friends = [{"x": (x + d) % 4, "c": h} for d in (1, 2, 3) for h in (0, 1)]
    friends += [{"c": 1 - c}]
    for k in range(1, 8):
        friends += [along_first(k), along_first(k) | {"c": home}]
    for k in (1, 7):
        friends += [along_second(k), along_second(k) | {"c": home}]
    for friend in friends:
        pl.semaphore_signal(barrier, inc=1, device_id=friend)

    own = w_all.at[me]
    odd = x % 2
    small = (
        (ak_ref, kv_raw.at[0]),
        (av_ref, kv_raw.at[1]),
        (decay_ref, decay_raw),
        (ret_gain_ref, ret_gain_raw),
        (sink_ref, sink_raw),
        (inverse_ref, inverse),
        (gain_ref, gain),
        (tok_ref, tok),
    )
    small = [
        pltpu.make_async_copy(src, dst, s_local.at[1 + n]) for n, (src, dst) in enumerate(small)
    ]
    loads = []
    for n, ref in enumerate((rk_ref, rv_ref, rq_ref, aq_ref)):
        cols = pl.ds(pl.multiple_of(odd * 256, 256), 256)
        for half in range(2):
            loads.append(
                pltpu.make_async_copy(
                    ref.at[pl.ds(16 * half, 16), cols],
                    own.at[half, :, pl.ds(256 * n, 256)],
                    s_local.at[0],
                )
            )
    for load in small[:2]:
        load.start()

    @pl.when(at_home)
    def _():
        for load in loads:
            load.start()

    for load in small[2:]:
        load.start()
    for load in small[:7]:
        load.wait()
    position = lax.broadcasted_iota(jnp.int32, (ROWS, 128), 0) + me * ROWS
    angle = position.astype(F32) * inverse[...]
    cosine[...] = jnp.cos(angle)
    sine[...] = jnp.sin(angle)
    pack_own[...] = jnp.zeros((2, 8, 256), F32)
    for i in range(2):
        pack_own[i, 0:1, :] = decay_raw[i : i + 1, :]
        pack_own[i, 1:2, :] = ret_gain_raw[:, 256 * i : 256 * i + 256]
        pack_own[i, 2:3, 0:4] = sink_raw[:, 4 * i : 4 * i + 4]

    @pl.when(at_home)
    def _():
        arrived(own.at[:, :, pl.ds(0, 1024)], s_local.at[0])
        both = [jnp.where(odd == 0, kv_raw[n, :, :HD], kv_raw[n, :, HD:]) for n in range(2)]
        both = jnp.concatenate(both, axis=1)
        for half in range(2):
            w_all[me, half, :, 1024:COLS] = both[16 * half : 16 * half + 16]

    small[7].wait()
    pl.semaphore_wait(barrier, jnp.where(at_home, 34, 16))

    @pl.when(at_home)
    def _():
        for k in (4, 3, 5, 2, 6, 1, 7):
            for h in range(2):
                ref = w_all.at[me, h]
                to = {"z": (z + h * k) % 8, "y": (y + (1 - h) * k) % 8, "c": h}
                send(ref, ref, s_open, r_near.at[8 - k], **to)
        for direction, k in ((0, 1), (1, 7)):
            for h in range(2):
                ref = w_all.at[me, h]
                to = {"z": (z + (1 - h) * k) % 8, "y": (y + h * k) % 8, "c": h}
                send(ref, ref, s_open, r_far.at[direction, 0, 0], **to)
        send(own, own, s_small.at[0], r_own, c=1 - c)

    for i in range(2):
        mine = jnp.logical_and(at_home, x % 2 == i)

        @pl.when(mine)
        def _(i=i):
            pltpu.make_async_copy(pack_own.at[i], pack.at[i], r_pack.at[i]).start()

        @pl.when(jnp.logical_not(mine))
        def _(i=i):
            send(
                pack_own.at[i],
                pack.at[x % 2],
                s_small.at[1 + i],
                r_pack.at[x % 2],
                x=2 * c + i,
                c=home,
            )

    piece = (
        pl.ds(pl.multiple_of(me // 4 * 16, 16), 16),
        pl.ds(pl.multiple_of(me // 2 % 2 * 128, 128), 128),
    )
    colour = (z + y) % 2
    opens = x % 2 == colour
    for i in range(2):
        mine = jnp.logical_and(at_home, x % 2 == i)

        @pl.when(jnp.logical_and(opens, mine))
        def _(i=i):
            pltpu.make_async_copy(start_ref.at[i, *piece], start, r_start).start()

        @pl.when(jnp.logical_and(opens, jnp.logical_not(mine)))
        def _(i=i):
            send(
                start_ref.at[i, *piece],
                start,
                s_small.at[3 + i],
                r_start,
                x=2 * c + i,
                c=home,
            )

    three = pl.ds(0, 3)
    first_at = c * z + (1 - c) * y
    second_at = (1 - c) * z + c * y
    holder = first_at < 4
    line = second_at * 4 + first_at % 4

    def slices(ref):
        for d in (1, 2, 3):
            src = ref.at[48 + line % 16]
            send(src, o_far.at[c, line, 3 - d], s_slice, r_slice.at[3 - d], x=(x + d) % 4)

    @pl.when(jnp.logical_and(holder, line < 16))
    def _():
        slices(ro_ref)

    @pl.when(jnp.logical_and(holder, line >= 16))
    def _():
        slices(ao_ref)

    def o_group(kb):
        at = pl.multiple_of(((second_at + kb) % 8) * 4, 4)
        return o_far.at[c, pl.ds(at, 4), three]

    def o_forward(ref, direction, kb):
        send(ref, ref, s_o, r_o_far.at[direction, kb - 1], **along_second(7 if direction else 1))

    def o_mirror(ref):
        send(ref, ref, s_o_mirror, r_o_mirror, c=1 - c)

    def o_open():
        @pl.when(holder)
        def _():
            for d in range(3):
                arrived(o_far.at[c, line, d], r_slice.at[d])
            ref = o_far.at[c, line, three]
            for k in (4, 3, 5, 2, 6, 1, 7):
                send(ref, ref, s_o_near, r_o_near.at[first_at % 4], **along_first(k))

    def o_line():
        for k in range(4):
            @pl.when(first_at != k)
            def _(k=k):
                arrived(o_far.at[c, second_at * 4 + k, three], r_o_near.at[k])

        o_forward(o_group(0), 0, 1)
        o_forward(o_group(0), 1, 1)
        o_mirror(o_group(0))

    def o_step(kb):
        for direction, limit in ((0, 4), (1, 3)):
            if kb > limit:
                continue
            ref = o_group(kb if direction else 8 - kb)
            arrived(ref, r_o_far.at[direction, kb - 1])
            if kb < limit:
                o_forward(ref, direction, kb + 1)
            o_mirror(ref)

    part = ROWS // CHUNKS

    def token_rows(slot, half, q):
        return x_in.at[slot, half, pl.ds(part * q, part)]

    for q in range(CHUNKS):
        for d in (1, 3):
            send(
                tok.at[pl.ds(part * q, part)],
                token_rows(x % 2, c, q),
                s_tok.at[0],
                r_tok.at[x % 2, c, q],
                x=(x + d) % 4,
                c=home,
            )

    @pl.when(at_home)
    def _():
        for q in range(CHUNKS):
            pltpu.make_async_copy(
                tok.at[pl.ds(part * q, part)], token_rows(x % 2, c, q), r_tok.at[x % 2, c, q]
            ).start()

    @pl.when(jnp.logical_not(at_home))
    def _():
        for q in range(CHUNKS):
            send(
                tok.at[pl.ds(part * q, part)],
                token_rows(x % 2, c, q),
                s_tok.at[1],
                r_tok.at[x % 2, c, q],
                c=1 - c,
            )

    def block(ka, kb):
        zz = (z + c * ka + (1 - c) * kb) % 8
        yy = (y + (1 - c) * ka + c * kb) % 8
        return w_all.at[zz * 8 + yy, c]

    def mirror(ref):
        send(ref, ref, s_mirror, r_mirror, c=1 - c)

    def limits(n):
        return (4, 3) if n % 2 == 0 else (3, 4)

    def forward(ref, direction, kb, n):
        send(ref, ref, s_w, r_far.at[direction, kb - 1, n], **along_second(7 if direction else 1))

    arrived(pack.at[0], r_pack.at[0])
    arrived(pack.at[1], r_pack.at[1])
    ti = lax.broadcasted_iota(jnp.int32, (ROWS, ROWS), 0)
    tj = lax.broadcasted_iota(jnp.int32, (ROWS, ROWS), 1)
    exact = lax.Precision.HIGHEST

    def decays(slot):
        rows = pack[slot]
        lower = (ti >= tj).astype(F32)
        upper = (ti <= tj).astype(F32)
        down = dot(lower, rows, (((1,), (1,)), ((), ())), exact)[:, 0:1]
        across = dot(rows, upper, precision=exact)[0:1, :]
        last = down[ROWS - 1 : ROWS, :]
        inside[slot] = jnp.where(ti >= tj, jnp.exp(jnp.where(ti >= tj, down - across, 0.0)), 0.0)
        grow[slot] = jnp.broadcast_to(jnp.exp(down), (ROWS, 128))
        fall[slot] = jnp.broadcast_to(jnp.exp(last - down), (ROWS, 128))
        own_rate[slot] = jnp.broadcast_to(jnp.exp(last), (1, 128))

    for n in range(1, 8):
        ka = STEPS[n]
        ref = block(ka, 0)
        arrived(ref, r_near.at[ka])
        forward(ref, 0, 1, n)
        forward(ref, 1, 1, n)
        mirror(ref)
        if n == 1:
            o_open()
        if n == 2:
            decays(0)
        if n == 4:
            decays(1)

    onward = at_home == (x % 2 == 0)
    relay_half = jnp.where(onward, 1, 0)
    relay_to = (x + jnp.where(onward, 3, 1)) % 4

    def relay(q):
        ref = token_rows(near, relay_half, q)
        arrived(ref, r_tok.at[near, relay_half, q])
        send(ref, ref, s_tok.at[2], r_tok.at[near, relay_half, q], x=relay_to)

    def norm_rows(slot, t):
        if t % 2 == 0:
            q = t // 2

            @pl.when(slot == near)
            def _():
                arrived(token_rows(near, 1 - relay_half, q), r_tok.at[near, 1 - relay_half, q])

            @pl.when(slot != near)
            def _():
                for half in range(2):
                    arrived(token_rows(1 - near, half, q), r_tok.at[1 - near, half, q])

        rows = pl.ds(32 * t, 32)
        a = x_in[slot, 0, rows].astype(F32)
        b = x_in[slot, 1, rows].astype(F32)
        total = jnp.sum(a * a, axis=-1, keepdims=True) + jnp.sum(b * b, axis=-1, keepdims=True)
        scale = lax.rsqrt(total * (1.0 / D) + EPS)
        to = pl.ds(pl.multiple_of(slot * ROWS + 32 * t, 32), 32)
        normed[to, 0:1024] = (a * scale * gain[:, 0:1024]).astype(BF)
        normed[to, 1024:2048] = (b * scale * gain[:, 1024:2048]).astype(BF)

    def ring(kb, n):
        for direction in range(2):
            limit = limits(n)[direction]
            if kb > limit:
                continue
            ref = block(STEPS[n], kb if direction else 8 - kb)
            arrived(ref, r_far.at[direction, kb - 1, n])
            if kb < limit:
                forward(ref, direction, kb + 1, n)
            mirror(ref)

    relay(0)
    for n in range(8):
        ring(1, n)
    relay(1)

    def send_along_x():
        low, high = pl.ds(0, 48), pl.ds(48, 16)
        for n, ref in enumerate((ro_ref, ao_ref)):
            for d in (1, 3):
                send(
                    ref.at[low],
                    o_near.at[c, n, 3 - d],
                    s_out,
                    r_out.at[3 - d, c, n],
                    x=(x + d) % 4,
                    c=home,
                )
            pairs = (
                (ref.at[low], o_near.at[c, n, 3], r_out.at[3, c, n]),
                (ref.at[high], o_far.at[c, pl.ds(16 * n, 16), 3], r_own_far),
            )

            @pl.when(at_home)
            def _(pairs=pairs):
                for src, dst, sem in pairs:
                    pltpu.make_async_copy(src, dst, sem).start()

            @pl.when(jnp.logical_not(at_home))
            def _(pairs=pairs):
                for src, dst, sem in pairs:
                    send(src, dst, s_small.at[5], sem, c=1 - c)

    def o_relay(n):
        at = jnp.where(onward, 0, 2)
        src = o_near.at[relay_half, n, at]
        arrived(src, r_out.at[at, relay_half, n])
        dst = o_near.at[relay_half, n, 1]
        send(src, dst, s_relay, r_out.at[1, relay_half, n], x=relay_to)

    for n in range(8):
        ring(2, n)
        if n == 3:
            relay(2)
    for n in range(8):
        ring(3, n)
        if n == 3:
            relay(3)
            send_along_x()
        if n >= 4:
            norm_rows(near, 2 * n - 8)
            norm_rows(near, 2 * n - 7)
    o_line()
    for n in range(8):
        ring(4, n)
        if n < 6:
            norm_rows(1 - near, n)
    for n in (6, 7):
        norm_rows(1 - near, n)
    few = pl.ds(0, 63)
    arrived(w_all.at[few, 0], r_mirror)

    @pl.when(jnp.logical_not(at_home))
    def _():
        arrived(own, r_own)

    def project(at, width):
        w = w_all[:, :, :, at : at + width].reshape(D, width)
        return dot(normed[...], w).astype(BF)

    keys[...] = project(0, 256)
    values[...] = project(256, 256)

    def rotated(ref, slot):
        rows = ref[pl.ds(ROWS * slot, ROWS)].astype(F32)
        front, rear = rows[:, :128], rows[:, 128:]
        return (
            front * cosine[...] - rear * sine[...],
            front * sine[...] + rear * cosine[...],
        )

    for slot in range(2):
        front, rear = [part * DK ** (-0.5) for part in rotated(keys, slot)]
        v = values[pl.ds(ROWS * slot, ROWS)]
        left = jnp.concatenate(
            [(front * fall[slot]).astype(BF), (rear * fall[slot]).astype(BF)], axis=1
        )
        state[slot] = dot(left, v, (((0,), (0,)), ((), ())))
        keys[pl.ds(ROWS * slot, ROWS)] = jnp.concatenate(
            [front.astype(BF), rear.astype(BF)], axis=1
        )

        for i in range(16):
            for half in range(2):
                pieces[slot * 32 + i * 2 + half] = state[
                    slot, 16 * i : 16 * i + 16, 128 * half : 128 * half + 128
                ].astype(BF)

    o_step(1)
    def place(index):
        return {"z": index // 8, "y": index % 8}

    def reach(k):
        return min(k // 8, 8 - k // 8) + min(k % 8, 8 - k % 8)

    offsets = sorted(
        (8 * i + j for i in range(8) for j in range(8) if (i + j) % 2 == 0),
        key=lambda k: (-reach(k), k),
    )

    def everyone(shade, visit):
        shift = (colour + shade) % 2
        for k in offsets:
            zz, yy = (z + k // 8) % 8, (y + k % 8 + shift) % 8
            to, at = zz * 8 + yy, {"z": zz, "y": yy}
            if k > 0:
                visit(to, at)
            else:
                pl.when(shift == 1)(lambda to=to, at=at: visit(to, at))

    for shade in range(2):

        def give(to, at, shade=shade):
            ref = pieces.at[32 * shade + to // 2]
            send(ref, came.at[me], s_scan.at[1], r_scan.at[1], **at)

        def tell(to, at, shade=shade):
            send(own_rate.at[shade], rates.at[me], s_scan.at[0], r_scan.at[0], **at)

        everyone(shade, give)
        everyone(shade, tell)
    mine_at = 32 * colour + me // 2
    came[me] = pieces[mine_at]
    rates[me] = own_rate[colour]

    att_kv[:, pl.ds(WINDOW, ROWS)] = project(1024, 128).reshape(2, ROWS, 128)
    tail = att_kv.at[:, pl.ds(ROWS, WINDOW)]
    lead = att_kv.at[:, pl.ds(0, WINDOW)]

    @pl.when(me < 63)
    def _():
        send(tail, lead, s_halo, r_halo, **place(me + 1))

    @pl.when(me == 0)
    def _():
        att_kv[:, pl.ds(0, WINDOW)] = jnp.zeros((2, WINDOW, 128), BF)

    both = project(512, 512)
    queries[...] = both[:, :256]
    att_q[...] = both[:, 256:]

    o_step(2)
    o_relay(0)
    for slot in range(2):
        front, rear = rotated(queries, slot)
        q = jnp.concatenate([front.astype(BF), rear.astype(BF)], axis=1)
        k = keys[pl.ds(ROWS * slot, ROWS)]
        raw = dot(q, k, (((1,), (1,)), ((), ()))) * inside[slot]
        scores[slot] = dot(raw.astype(BF), values[pl.ds(ROWS * slot, ROWS)])
        queries[pl.ds(ROWS * slot, ROWS)] = jnp.concatenate(
            [(front * grow[slot]).astype(BF), (rear * grow[slot]).astype(BF)], axis=1
        )

    o_relay(1)
    o_step(3)
    arrived(rates.at[few], r_scan.at[0])
    arrived(came.at[few], r_scan.at[1])

    def advance(k, carried):
        back[k] = carried.astype(BF)
        return carried * rates[k] + came[k].astype(F32)

    arrived(start, r_start)
    lax.fori_loop(0, 64, advance, start[...])

    for shade in range(2):
        everyone(
            shade,
            lambda to, at: send(
                back.at[to], prior.at[mine_at], s_scan.at[2], r_scan.at[2], **at
            ),
        )
    prior[mine_at] = back[me]
    @pl.when(me > 0)
    def _():
        arrived(lead, r_halo)


    qi = lax.broadcasted_iota(jnp.int32, (WINDOW, 2 * WINDOW), 0)
    ki = lax.broadcasted_iota(jnp.int32, (WINDOW, 2 * WINDOW), 1)
    for slot in range(2):
        sink = jnp.exp(pack[slot, 2:3, 0:4])
        for n in range(2):
            allowed = jnp.logical_and(ki > qi, ki <= qi + WINDOW)
            if n == 0:
                allowed = jnp.logical_and(allowed, ki >= jnp.where(me == 0, WINDOW, 0))
            kv = att_kv[slot, pl.ds(WINDOW * n, 2 * WINDOW)]
            rows = att_q[pl.ds(ROWS * slot + WINDOW * n, WINDOW)]
            heads_in = [rows[:, HD * g : HD * g + HD] for g in range(4)]
            near_keys, near_values = kv[:, :HD], kv[:, HD:]
            score = [dot(q, near_keys, (((1,), (1,)), ((), ()))) for q in heads_in]
            expo = [jnp.exp(jnp.where(allowed, a * HD ** (-0.5), -1e30)) for a in score]
            total = [
                jnp.sum(e, axis=-1, keepdims=True) + sink[:, g : g + 1] for g, e in enumerate(expo)
            ]
            share = [(e * (1.0 / t)).astype(BF) for e, t in zip(expo, total)]
            outs = [dot(p, near_values) for p in share]
            hidden[slot, 1, pl.ds(WINDOW * n, WINDOW)] = jnp.concatenate(outs, axis=1).astype(BF)

    def hand_over(kind):
        for i in range(2):
            to = 2 * c + i
            for half in range(2):
                rows = pl.ds(WINDOW * half, WINDOW)
                src = hidden.at[i, kind, rows]
                dst = heads.at[x, kind, rows]
                here = jnp.logical_and(to == x, c == half)

                @pl.when(here)
                def _(src=src, dst=dst):
                    pltpu.make_async_copy(src, dst, r_hid.at[kind, x]).start()

                @pl.when(jnp.logical_not(here))
                def _(src=src, dst=dst, half=half, i=i):
                    send(src, dst, s_hid.at[kind, i, half], r_hid.at[kind, x], x=to, c=half)

    def pass_on(kind):
        rows = pl.ds(pl.multiple_of(WINDOW * c, WINDOW), WINDOW)
        for j in range(4):
            ref = heads.at[j, kind, rows]
            arrived(ref, r_hid.at[kind, j])
            send(ref, ref, s_pass, r_pass.at[kind, j], c=1 - c)

    def passed(kind):
        rows = pl.ds(pl.multiple_of(WINDOW * (1 - c), WINDOW), WINDOW)
        for j in range(4):
            arrived(heads.at[j, kind, rows], r_pass.at[kind, j])

    hand_over(1)

    o_step(4)
    arrived(prior.at[few], r_scan.at[2])
    for slot in range(2):
        for i in range(16):
            for half in range(2):
                state[slot, 16 * i : 16 * i + 16, 128 * half : 128 * half + 128] = prior[
                    slot * 32 + i * 2 + half
                ].astype(F32)

        raw = scores[slot] + dot(queries[pl.ds(ROWS * slot, ROWS)], state[slot].astype(BF))
        centred = raw - jnp.mean(raw, axis=-1, keepdims=True)
        variance = jnp.mean(centred * centred, axis=-1, keepdims=True)
        shaped = centred * lax.rsqrt(variance + EPS) * pack[slot, 1:2, :]
        hidden[slot, 0] = shaped.astype(BF)

    hand_over(0)

    for d in range(2):
        rel = (2 * c + d + 3 - x) % 4
        for half in range(2):
            relayed = jnp.logical_and(rel == jnp.where(onward, 0, 2), relay_half == half)

            @pl.when(jnp.logical_not(relayed))
            def _(rel=rel, half=half):
                for n in range(2):
                    arrived(o_near.at[half, n, rel], r_out.at[rel, half, n])

    @pl.when(at_home)
    def _():
        arrived(o_far.at[:, :, 3], r_own_far)

    arrived(o_far.at[1 - c, :, three], r_o_mirror)

    def product(kind, d):
        rel = (2 * c + d + 3 - x) % 4
        total = None
        for half in range(2):
            even = o_near[half, kind, rel, 0:32].reshape(256, 512)
            front = o_near[half, kind, rel, 32:48].reshape(128, 512)
            rear = o_far[half, pl.ds(16 * kind, 16), rel].reshape(128, 512)
            odd_rows = jnp.concatenate([front, rear], axis=0)
            one = dot(heads[2 * half, kind], even) + dot(heads[2 * half + 1, kind], odd_rows)
            total = one if total is None else total + one
        return total

    pass_on(1)
    passed(1)
    for d in range(2):
        partial[d] = product(1, d)

    pass_on(0)
    passed(0)
    for d in range(2):
        out_ref[:, 512 * d : 512 * d + 512] = (partial[d] + product(0, d)).astype(BF)

    arrived(x_in.at[0], s_tok.at[0])
    arrived(tok, s_tok.at[2])
    arrived(w_all.at[pl.ds(0, 54), 0], s_w)
    arrived(w_all.at[few, 0], s_mirror)
    arrived(heads.at[pl.ds(0, 2)], s_pass)
    arrived(rates.at[few], s_scan.at[0])
    arrived(came.at[few], s_scan.at[1])
    arrived(prior.at[few], s_scan.at[2])

    @pl.when(jnp.logical_not(at_home))
    def _():
        arrived(tok, s_tok.at[1])
        arrived(o_far.at[:, :, pl.ds(0, 2)], s_small.at[5])

    @pl.when(at_home)
    def _():
        arrived(own, s_small.at[0])
        arrived(w_all.at[pl.ds(0, 18), 0], s_open)

    arrived(o_near.at[0, :, pl.ds(0, 2)], s_out)
    arrived(o_near.at[0, :, 1], s_relay)
    arrived(o_far.at[0, pl.ds(0, 28), three], s_o)

    @pl.when(holder)
    def _():
        arrived(o_far.at[0, 0, three], s_slice)
        arrived(o_far.at[0, pl.ds(0, 7), three], s_o_near)

    arrived(o_far.at[0, :, three], s_o_mirror)
    for i in range(2):
        mine = jnp.logical_and(at_home, x % 2 == i)

        @pl.when(jnp.logical_not(mine))
        def _(i=i):
            arrived(pack.at[i], s_small.at[1 + i])

        @pl.when(jnp.logical_and(opens, jnp.logical_not(mine)))
        def _(i=i):
            arrived(start, s_small.at[3 + i])

        for kind in range(2):
            for half in range(2):
                here = jnp.logical_and(2 * c + i == x, c == half)

                @pl.when(jnp.logical_not(here))
                def _(i=i, kind=kind, half=half):
                    rows = pl.ds(WINDOW * half, WINDOW)
                    arrived(hidden.at[i, kind, rows], s_hid.at[kind, i, half])

    @pl.when(me < 63)
    def _():
        arrived(tail, s_halo)


def shards(
    tokens,
    norm_gain,
    ret_query,
    ret_key,
    ret_value,
    att_query,
    att_key,
    att_value,
    log_decay,
    start_state,
    ret_gain,
    sink_logits,
    ret_out,
    att_out,
):
    steps = np.arange(128, dtype=np.float32) / np.float32(128)
    inverse = jnp.asarray((np.float32(1) / np.float32(10000) ** steps).reshape(1, 128))
    vmem = pl.BlockSpec(memory_space=pltpu.VMEM)
    hbm = pl.BlockSpec(memory_space=pl.ANY)
    dma = pltpu.SemaphoreType.DMA
    scratch = [
        pltpu.VMEM((ROWS, 1024), BF),
        pltpu.VMEM((2, 2, ROWS, 1024), BF),
        pltpu.VMEM((2 * ROWS, D), BF),
        pltpu.VMEM((64, 2, 16, COLS), BF),
        pltpu.VMEM((2, 8, 256), F32),
        pltpu.VMEM((16, 128), F32),
        pltpu.VMEM((2, 2, 4, 48, 8, 512), BF),
        pltpu.VMEM((2, 32, 4, 8, 512), BF),
        pltpu.VMEM((2, 32, 128), BF),
        pltpu.VMEM((2, 256), F32),
        pltpu.VMEM((1, 512), F32),
        pltpu.VMEM((1, 8), F32),
        pltpu.VMEM((2, 8, 256), F32),
        pltpu.VMEM((1, D), F32),
        pltpu.VMEM((1, 128), F32),
        pltpu.VMEM((2, ROWS, ROWS), F32),
        pltpu.VMEM((2, ROWS, 128), F32),
        pltpu.VMEM((2, ROWS, 128), F32),
        pltpu.VMEM((2, ROWS, 512), F32),
        pltpu.VMEM((ROWS, 128), F32),
        pltpu.VMEM((ROWS, 128), F32),
        pltpu.VMEM((2 * ROWS, 256), BF),
        pltpu.VMEM((2 * ROWS, 256), BF),
        pltpu.VMEM((2 * ROWS, 256), BF),
        pltpu.VMEM((2 * ROWS, 256), BF),
        pltpu.VMEM((2, WINDOW + ROWS, 128), BF),
        pltpu.VMEM((2, 256, 256), F32),
        pltpu.VMEM((2, ROWS, 256), F32),
        pltpu.VMEM((64, 16, 128), BF),
        pltpu.VMEM((64, 16, 128), BF),
        pltpu.VMEM((64, 1, 128), F32),
        pltpu.VMEM((2, 1, 128), F32),
        pltpu.VMEM((64, 16, 128), BF),
        pltpu.VMEM((64, 16, 128), BF),
        pltpu.VMEM((2, 2, ROWS, 256), BF),
        pltpu.VMEM((4, 2, ROWS, 256), BF),
        dma((9,)),
        dma((3,)),
        dma((2, 2, CHUNKS)),
        dma((6,)),
        dma((2,)),
        dma,
        dma,
        dma,
        dma,
        dma((8,)),
        dma((2, 4, 8)),
        dma,
        dma,
        dma((3,)),
        dma((3,)),
        dma,
        dma,
        dma((2, 2, 2)),
        dma((2, 4)),
        dma,
        dma((2, 4)),
        dma,
        dma((4, 2, 2)),
        dma,
        dma,
        dma((3,)),
        dma,
        dma,
        dma,
        dma((4,)),
        dma((2, 4)),
        dma,
        dma,
    ]
    mixed = pl.pallas_call(
        layer_kernel,
        out_shape=pltpu.VMEM((ROWS, 1024), BF),
        in_specs=[hbm] * 15,
        out_specs=vmem,
        scratch_shapes=scratch,
        compiler_params=pltpu.CompilerParams(
            collective_id=0, has_side_effects=True, vmem_limit_bytes=60 * 1024 * 1024
        ),
    )(
        tokens[0],
        ret_key,
        ret_value,
        ret_query,
        att_query,
        att_key,
        att_value,
        log_decay[0],
        ret_gain.reshape(1, 512),
        sink_logits.reshape(1, 8),
        start_state[0],
        ret_out.reshape(64, 8, 512),
        att_out.reshape(64, 8, 512),
        norm_gain.reshape(1, D),
        inverse,
    )
    return mixed[None]


def solution(mesh):
    torus = Mesh(
        mesh.devices.reshape(8, 8, mesh.shape["fs"], mesh.shape["tp"]), ("z", "y", "x", "c")
    )
    across = P(SP, "c")
    in_specs = (
        P("x", SP, "c"),
        P(),
        across,
        across,
        across,
        across,
        across,
        across,
        P("x", "c", SP),
        P("x", "c", None, None),
        P("c"),
        P("c"),
        P("c", "x"),
        P("c", "x"),
    )
    return jax.shard_map(
        shards, mesh=torus, in_specs=in_specs, out_specs=P("x", SP, "c"), check_vma=False
    )
```

```python
import jax
import jax.numpy as jnp
import numpy as np
from jax import lax
from jax.experimental import pallas as pl
from jax.experimental.pallas import tpu as pltpu
from jax.sharding import Mesh
from jax.sharding import PartitionSpec as P

D = 2048
DK = 256
HD = 64
ROWS = 256
WINDOW = 128
COLS = 1152
CHUNKS = 4
SP = ("z", "y")
BF = jnp.bfloat16
F32 = jnp.float32
EPS = 1e-06
STEPS = (0, 7, 1, 6, 2, 5, 3, 4)


def dot(a, b, dims=(((1,), (0,)), ((), ())), precision=None):
    return lax.dot_general(a, b, dims, precision=precision, preferred_element_type=F32)


def layer_kernel(
    tok_ref,
    rk_ref,
    rv_ref,
    rq_ref,
    aq_ref,
    ak_ref,
    av_ref,
    decay_ref,
    ret_gain_ref,
    sink_ref,
    start_ref,
    ro_ref,
    ao_ref,
    gain_ref,
    inverse_ref,
    out_ref,
    tok,
    x_in,
    normed,
    w_all,
    pack,
    start,
    o_near,
    o_far,
    kv_raw,
    decay_raw,
    ret_gain_raw,
    sink_raw,
    pack_own,
    gain,
    inverse,
    inside,
    grow,
    fall,
    partial,
    cosine,
    sine,
    keys,
    values,
    queries,
    att_q,
    att_kv,
    state,
    scores,
    pieces,
    came,
    rates,
    own_rate,
    back,
    prior,
    hidden,
    heads,
    s_local,
    s_tok,
    r_tok,
    s_small,
    r_pack,
    r_start,
    s_open,
    s_w,
    r_own,
    r_near,
    r_far,
    s_mirror,
    r_mirror,
    s_scan,
    r_scan,
    s_halo,
    r_halo,
    s_hid,
    r_hid,
    s_pass,
    r_pass,
    s_out,
    r_out,
    r_own_far,
    s_slice,
    r_slice,
    s_relay,
    s_o_near,
    s_o,
    r_o_near,
    r_o_far,
    s_o_mirror,
    r_o_mirror,
):
    z, y = lax.axis_index("z"), lax.axis_index("y")
    x, c = lax.axis_index("x"), lax.axis_index("c")
    me = z * 8 + y
    home = x // 2
    at_home = c == home
    near = 1 - x % 2

    def send(src, dst, send_sem, recv_sem, **to):
        pltpu.make_async_remote_copy(
            src_ref=src, dst_ref=dst, send_sem=send_sem, recv_sem=recv_sem, device_id=to
        ).start()

    def arrived(ref, sem):
        pltpu.make_async_copy(ref, ref, sem).wait()

    def along_first(k):
        return {"z": (z + c * k) % 8, "y": (y + (1 - c) * k) % 8}

    def along_second(k):
        return {"z": (z + (1 - c) * k) % 8, "y": (y + c * k) % 8}

    barrier = pltpu.get_barrier_semaphore()
    friends = [{"x": (x + d) % 4, "c": h} for d in (1, 2, 3) for h in (0, 1)]
    friends += [{"c": 1 - c}]
    for k in range(1, 8):
        friends += [along_first(k), along_first(k) | {"c": home}]
    for k in (1, 7):
        friends += [along_second(k), along_second(k) | {"c": home}]
    for friend in friends:
        pl.semaphore_signal(barrier, inc=1, device_id=friend)

    own = w_all.at[me]
    odd = x % 2
    small = (
        (ak_ref, kv_raw.at[0]),
        (av_ref, kv_raw.at[1]),
        (decay_ref, decay_raw),
        (ret_gain_ref, ret_gain_raw),
        (sink_ref, sink_raw),
        (inverse_ref, inverse),
        (gain_ref, gain),
        (tok_ref, tok),
    )
    small = [
        pltpu.make_async_copy(src, dst, s_local.at[1 + n]) for n, (src, dst) in enumerate(small)
    ]
    loads = []
    for n, ref in enumerate((rk_ref, rv_ref, rq_ref, aq_ref)):
        cols = pl.ds(pl.multiple_of(odd * 256, 256), 256)
        for half in range(2):
            loads.append(
                pltpu.make_async_copy(
                    ref.at[pl.ds(16 * half, 16), cols],
                    own.at[half, :, pl.ds(256 * n, 256)],
                    s_local.at[0],
                )
            )
    for load in small[:2]:
        load.start()

    @pl.when(at_home)
    def _():
        for load in loads:
            load.start()

    for load in small[2:]:
        load.start()
    for load in small[:7]:
        load.wait()
    position = lax.broadcasted_iota(jnp.int32, (ROWS, 128), 0) + me * ROWS
    angle = position.astype(F32) * inverse[...]
    cosine[...] = jnp.cos(angle)
    sine[...] = jnp.sin(angle)
    pack_own[...] = jnp.zeros((2, 8, 256), F32)
    for i in range(2):
        pack_own[i, 0:1, :] = decay_raw[i : i + 1, :]
        pack_own[i, 1:2, :] = ret_gain_raw[:, 256 * i : 256 * i + 256]
        pack_own[i, 2:3, 0:4] = sink_raw[:, 4 * i : 4 * i + 4]

    @pl.when(at_home)
    def _():
        arrived(own.at[:, :, pl.ds(0, 1024)], s_local.at[0])
        both = [jnp.where(odd == 0, kv_raw[n, :, :HD], kv_raw[n, :, HD:]) for n in range(2)]
        both = jnp.concatenate(both, axis=1)
        for half in range(2):
            w_all[me, half, :, 1024:COLS] = both[16 * half : 16 * half + 16]

    small[7].wait()
    pl.semaphore_wait(barrier, jnp.where(at_home, 34, 16))

    @pl.when(at_home)
    def _():
        for k in (4, 3, 5, 2, 6, 1, 7):
            for h in range(2):
                ref = w_all.at[me, h]
                to = {"z": (z + h * k) % 8, "y": (y + (1 - h) * k) % 8, "c": h}
                send(ref, ref, s_open, r_near.at[8 - k], **to)
        for direction, k in ((0, 1), (1, 7)):
            for h in range(2):
                ref = w_all.at[me, h]
                to = {"z": (z + (1 - h) * k) % 8, "y": (y + h * k) % 8, "c": h}
                send(ref, ref, s_open, r_far.at[direction, 0, 0], **to)
        send(own, own, s_small.at[0], r_own, c=1 - c)

    for i in range(2):
        mine = jnp.logical_and(at_home, x % 2 == i)

        @pl.when(mine)
        def _(i=i):
            pltpu.make_async_copy(pack_own.at[i], pack.at[i], r_pack.at[i]).start()

        @pl.when(jnp.logical_not(mine))
        def _(i=i):
            send(
                pack_own.at[i],
                pack.at[x % 2],
                s_small.at[1 + i],
                r_pack.at[x % 2],
                x=2 * c + i,
                c=home,
            )

    piece = (
        pl.ds(pl.multiple_of(me // 4 * 16, 16), 16),
        pl.ds(pl.multiple_of(me // 2 % 2 * 128, 128), 128),
    )
    colour = (z + y) % 2
    opens = x % 2 == colour
    for i in range(2):
        mine = jnp.logical_and(at_home, x % 2 == i)

        @pl.when(jnp.logical_and(opens, mine))
        def _(i=i):
            pltpu.make_async_copy(start_ref.at[i, *piece], start, r_start).start()

        @pl.when(jnp.logical_and(opens, jnp.logical_not(mine)))
        def _(i=i):
            send(
                start_ref.at[i, *piece],
                start,
                s_small.at[3 + i],
                r_start,
                x=2 * c + i,
                c=home,
            )

    three = pl.ds(0, 3)
    first_at = c * z + (1 - c) * y
    second_at = (1 - c) * z + c * y
    holder = first_at < 4
    line = second_at * 4 + first_at % 4

    def slices(ref):
        for d in (1, 2, 3):
            src = ref.at[48 + line % 16]
            send(src, o_far.at[c, line, 3 - d], s_slice, r_slice.at[3 - d], x=(x + d) % 4)

    @pl.when(jnp.logical_and(holder, line < 16))
    def _():
        slices(ro_ref)

    @pl.when(jnp.logical_and(holder, line >= 16))
    def _():
        slices(ao_ref)

    def o_group(kb):
        at = pl.multiple_of(((second_at + kb) % 8) * 4, 4)
        return o_far.at[c, pl.ds(at, 4), three]

    def o_forward(ref, direction, kb):
        send(ref, ref, s_o, r_o_far.at[direction, kb - 1], **along_second(7 if direction else 1))

    def o_mirror(ref):
        send(ref, ref, s_o_mirror, r_o_mirror, c=1 - c)

    def o_open():
        @pl.when(holder)
        def _():
            for d in range(3):
                arrived(o_far.at[c, line, d], r_slice.at[d])
            ref = o_far.at[c, line, three]
            for k in (4, 3, 5, 2, 6, 1, 7):
                send(ref, ref, s_o_near, r_o_near.at[first_at % 4], **along_first(k))

    def o_line():
        for k in range(4):
            @pl.when(first_at != k)
            def _(k=k):
                arrived(o_far.at[c, second_at * 4 + k, three], r_o_near.at[k])

        o_forward(o_group(0), 0, 1)
        o_forward(o_group(0), 1, 1)
        o_mirror(o_group(0))

    def o_step(kb):
        for direction, limit in ((0, 4), (1, 3)):
            if kb > limit:
                continue
            ref = o_group(kb if direction else 8 - kb)
            arrived(ref, r_o_far.at[direction, kb - 1])
            if kb < limit:
                o_forward(ref, direction, kb + 1)
            o_mirror(ref)

    part = ROWS // CHUNKS

    def token_rows(slot, half, q):
        return x_in.at[slot, half, pl.ds(part * q, part)]

    for q in range(CHUNKS):
        for d in (1, 3):
            send(
                tok.at[pl.ds(part * q, part)],
                token_rows(x % 2, c, q),
                s_tok.at[0],
                r_tok.at[x % 2, c, q],
                x=(x + d) % 4,
                c=home,
            )

    @pl.when(at_home)
    def _():
        for q in range(CHUNKS):
            pltpu.make_async_copy(
                tok.at[pl.ds(part * q, part)], token_rows(x % 2, c, q), r_tok.at[x % 2, c, q]
            ).start()

    @pl.when(jnp.logical_not(at_home))
    def _():
        for q in range(CHUNKS):
            send(
                tok.at[pl.ds(part * q, part)],
                token_rows(x % 2, c, q),
                s_tok.at[1],
                r_tok.at[x % 2, c, q],
                c=1 - c,
            )

    def block(ka, kb):
        zz = (z + c * ka + (1 - c) * kb) % 8
        yy = (y + (1 - c) * ka + c * kb) % 8
        return w_all.at[zz * 8 + yy, c]

    def mirror(ref):
        send(ref, ref, s_mirror, r_mirror, c=1 - c)

    def limits(n):
        return (4, 3) if n % 2 == 0 else (3, 4)

    def forward(ref, direction, kb, n):
        send(ref, ref, s_w, r_far.at[direction, kb - 1, n], **along_second(7 if direction else 1))

    arrived(pack.at[0], r_pack.at[0])
    arrived(pack.at[1], r_pack.at[1])
    ti = lax.broadcasted_iota(jnp.int32, (ROWS, ROWS), 0)
    tj = lax.broadcasted_iota(jnp.int32, (ROWS, ROWS), 1)
    exact = lax.Precision.HIGHEST

    def decays(slot):
        rows = pack[slot]
        lower = (ti >= tj).astype(F32)
        upper = (ti <= tj).astype(F32)
        down = dot(lower, rows, (((1,), (1,)), ((), ())), exact)[:, 0:1]
        across = dot(rows, upper, precision=exact)[0:1, :]
        last = down[ROWS - 1 : ROWS, :]
        inside[slot] = jnp.where(ti >= tj, jnp.exp(jnp.where(ti >= tj, down - across, 0.0)), 0.0)
        grow[slot] = jnp.broadcast_to(jnp.exp(down), (ROWS, 128))
        fall[slot] = jnp.broadcast_to(jnp.exp(last - down), (ROWS, 128))
        own_rate[slot] = jnp.broadcast_to(jnp.exp(last), (1, 128))

    for n in range(1, 8):
        ka = STEPS[n]
        ref = block(ka, 0)
        arrived(ref, r_near.at[ka])
        forward(ref, 0, 1, n)
        forward(ref, 1, 1, n)
        mirror(ref)
        if n == 1:
            o_open()
        if n == 2:
            decays(0)
        if n == 4:
            decays(1)

    onward = at_home == (x % 2 == 0)
    relay_half = jnp.where(onward, 1, 0)
    relay_to = (x + jnp.where(onward, 3, 1)) % 4

    def relay(q):
        ref = token_rows(near, relay_half, q)
        arrived(ref, r_tok.at[near, relay_half, q])
        send(ref, ref, s_tok.at[2], r_tok.at[near, relay_half, q], x=relay_to)

    def norm_rows(slot, t):
        if t % 2 == 0:
            q = t // 2

            @pl.when(slot == near)
            def _():
                arrived(token_rows(near, 1 - relay_half, q), r_tok.at[near, 1 - relay_half, q])

            @pl.when(slot != near)
            def _():
                for half in range(2):
                    arrived(token_rows(1 - near, half, q), r_tok.at[1 - near, half, q])

        rows = pl.ds(32 * t, 32)
        a = x_in[slot, 0, rows].astype(F32)
        b = x_in[slot, 1, rows].astype(F32)
        total = jnp.sum(a * a, axis=-1, keepdims=True) + jnp.sum(b * b, axis=-1, keepdims=True)
        scale = lax.rsqrt(total * (1.0 / D) + EPS)
        to = pl.ds(pl.multiple_of(slot * ROWS + 32 * t, 32), 32)
        normed[to, 0:1024] = (a * scale * gain[:, 0:1024]).astype(BF)
        normed[to, 1024:2048] = (b * scale * gain[:, 1024:2048]).astype(BF)

    def ring(kb, n):
        for direction in range(2):
            limit = limits(n)[direction]
            if kb > limit:
                continue
            ref = block(STEPS[n], kb if direction else 8 - kb)
            arrived(ref, r_far.at[direction, kb - 1, n])
            if kb < limit:
                forward(ref, direction, kb + 1, n)
            mirror(ref)

    relay(0)
    for n in range(8):
        ring(1, n)
    relay(1)

    def send_along_x():
        low, high = pl.ds(0, 48), pl.ds(48, 16)
        for n, ref in enumerate((ro_ref, ao_ref)):
            for d in (1, 3):
                send(
                    ref.at[low],
                    o_near.at[c, n, 3 - d],
                    s_out,
                    r_out.at[3 - d, c, n],
                    x=(x + d) % 4,
                    c=home,
                )
            pairs = (
                (ref.at[low], o_near.at[c, n, 3], r_out.at[3, c, n]),
                (ref.at[high], o_far.at[c, pl.ds(16 * n, 16), 3], r_own_far),
            )

            @pl.when(at_home)
            def _(pairs=pairs):
                for src, dst, sem in pairs:
                    pltpu.make_async_copy(src, dst, sem).start()

            @pl.when(jnp.logical_not(at_home))
            def _(pairs=pairs):
                for src, dst, sem in pairs:
                    send(src, dst, s_small.at[5], sem, c=1 - c)

    def o_relay(n):
        at = jnp.where(onward, 0, 2)
        src = o_near.at[relay_half, n, at]
        arrived(src, r_out.at[at, relay_half, n])
        dst = o_near.at[relay_half, n, 1]
        send(src, dst, s_relay, r_out.at[1, relay_half, n], x=relay_to)

    for n in range(8):
        ring(2, n)
        if n == 3:
            relay(2)
    for n in range(8):
        ring(3, n)
        if n == 3:
            relay(3)
            send_along_x()
        if n >= 4:
            norm_rows(near, 2 * n - 8)
            norm_rows(near, 2 * n - 7)
    o_line()
    for n in range(8):
        ring(4, n)
        if n < 6:
            norm_rows(1 - near, n)
    for n in (6, 7):
        norm_rows(1 - near, n)
    few = pl.ds(0, 63)
    arrived(w_all.at[few, 0], r_mirror)

    @pl.when(jnp.logical_not(at_home))
    def _():
        arrived(own, r_own)

    def project(at, width):
        w = w_all[:, :, :, at : at + width].reshape(D, width)
        return dot(normed[...], w).astype(BF)

    keys[...] = project(0, 256)
    values[...] = project(256, 256)

    def rotated(ref, slot):
        rows = ref[pl.ds(ROWS * slot, ROWS)].astype(F32)
        front, rear = rows[:, :128], rows[:, 128:]
        return (
            front * cosine[...] - rear * sine[...],
            front * sine[...] + rear * cosine[...],
        )

    for slot in range(2):
        front, rear = [part * DK ** (-0.5) for part in rotated(keys, slot)]
        v = values[pl.ds(ROWS * slot, ROWS)]
        left = jnp.concatenate(
            [(front * fall[slot]).astype(BF), (rear * fall[slot]).astype(BF)], axis=1
        )
        state[slot] = dot(left, v, (((0,), (0,)), ((), ())))
        keys[pl.ds(ROWS * slot, ROWS)] = jnp.concatenate(
            [front.astype(BF), rear.astype(BF)], axis=1
        )

        for i in range(16):
            for half in range(2):
                pieces[slot * 32 + i * 2 + half] = state[
                    slot, 16 * i : 16 * i + 16, 128 * half : 128 * half + 128
                ].astype(BF)

    o_step(1)
    def place(index):
        return {"z": index // 8, "y": index % 8}

    def reach(k):
        return min(k // 8, 8 - k // 8) + min(k % 8, 8 - k % 8)

    offsets = sorted(
        (8 * i + j for i in range(8) for j in range(8) if (i + j) % 2 == 0),
        key=lambda k: (-reach(k), k),
    )

    def everyone(shade, visit):
        shift = (colour + shade) % 2
        for k in offsets:
            zz, yy = (z + k // 8) % 8, (y + k % 8 + shift) % 8
            to, at = zz * 8 + yy, {"z": zz, "y": yy}
            if k > 0:
                visit(to, at)
            else:
                pl.when(shift == 1)(lambda to=to, at=at: visit(to, at))

    for shade in range(2):

        def give(to, at, shade=shade):
            ref = pieces.at[32 * shade + to // 2]
            send(ref, came.at[me], s_scan.at[1], r_scan.at[1], **at)

        def tell(to, at, shade=shade):
            send(own_rate.at[shade], rates.at[me], s_scan.at[0], r_scan.at[0], **at)

        everyone(shade, give)
        everyone(shade, tell)
    mine_at = 32 * colour + me // 2
    came[me] = pieces[mine_at]
    rates[me] = own_rate[colour]

    att_kv[:, pl.ds(WINDOW, ROWS)] = project(1024, 128).reshape(2, ROWS, 128)
    tail = att_kv.at[:, pl.ds(ROWS, WINDOW)]
    lead = att_kv.at[:, pl.ds(0, WINDOW)]

    @pl.when(me < 63)
    def _():
        send(tail, lead, s_halo, r_halo, **place(me + 1))

    @pl.when(me == 0)
    def _():
        att_kv[:, pl.ds(0, WINDOW)] = jnp.zeros((2, WINDOW, 128), BF)

    both = project(512, 512)
    queries[...] = both[:, :256]
    att_q[...] = both[:, 256:]

    o_step(2)
    o_relay(0)
    for slot in range(2):
        front, rear = rotated(queries, slot)
        q = jnp.concatenate([front.astype(BF), rear.astype(BF)], axis=1)
        k = keys[pl.ds(ROWS * slot, ROWS)]
        raw = dot(q, k, (((1,), (1,)), ((), ()))) * inside[slot]
        scores[slot] = dot(raw.astype(BF), values[pl.ds(ROWS * slot, ROWS)])
        queries[pl.ds(ROWS * slot, ROWS)] = jnp.concatenate(
            [(front * grow[slot]).astype(BF), (rear * grow[slot]).astype(BF)], axis=1
        )

    o_relay(1)
    o_step(3)
    arrived(rates.at[few], r_scan.at[0])
    arrived(came.at[few], r_scan.at[1])

    def advance(k, carried):
        back[k] = carried.astype(BF)
        return carried * rates[k] + came[k].astype(F32)

    arrived(start, r_start)
    lax.fori_loop(0, 64, advance, start[...])

    for shade in range(2):
        everyone(
            shade,
            lambda to, at: send(
                back.at[to], prior.at[mine_at], s_scan.at[2], r_scan.at[2], **at
            ),
        )
    prior[mine_at] = back[me]
    @pl.when(me > 0)
    def _():
        arrived(lead, r_halo)


    qi = lax.broadcasted_iota(jnp.int32, (WINDOW, 2 * WINDOW), 0)
    ki = lax.broadcasted_iota(jnp.int32, (WINDOW, 2 * WINDOW), 1)
    for slot in range(2):
        sink = jnp.exp(pack[slot, 2:3, 0:4])
        for n in range(2):
            allowed = jnp.logical_and(ki > qi, ki <= qi + WINDOW)
            if n == 0:
                allowed = jnp.logical_and(allowed, ki >= jnp.where(me == 0, WINDOW, 0))
            kv = att_kv[slot, pl.ds(WINDOW * n, 2 * WINDOW)]
            rows = att_q[pl.ds(ROWS * slot + WINDOW * n, WINDOW)]
            heads_in = [rows[:, HD * g : HD * g + HD] for g in range(4)]
            near_keys, near_values = kv[:, :HD], kv[:, HD:]
            score = [dot(q, near_keys, (((1,), (1,)), ((), ()))) for q in heads_in]
            expo = [jnp.exp(jnp.where(allowed, a * HD ** (-0.5), -1e30)) for a in score]
            total = [
                jnp.sum(e, axis=-1, keepdims=True) + sink[:, g : g + 1] for g, e in enumerate(expo)
            ]
            share = [(e * (1.0 / (t * 0.0625)) * 0.0625).astype(BF) for e, t in zip(expo, total)]
            outs = [dot(p, near_values) for p in share]
            hidden[slot, 1, pl.ds(WINDOW * n, WINDOW)] = jnp.concatenate(outs, axis=1).astype(BF)

    def hand_over(kind):
        for i in range(2):
            to = 2 * c + i
            for half in range(2):
                rows = pl.ds(WINDOW * half, WINDOW)
                src = hidden.at[i, kind, rows]
                dst = heads.at[x, kind, rows]
                here = jnp.logical_and(to == x, c == half)

                @pl.when(here)
                def _(src=src, dst=dst):
                    pltpu.make_async_copy(src, dst, r_hid.at[kind, x]).start()

                @pl.when(jnp.logical_not(here))
                def _(src=src, dst=dst, half=half, i=i):
                    send(src, dst, s_hid.at[kind, i, half], r_hid.at[kind, x], x=to, c=half)

    def pass_on(kind):
        rows = pl.ds(pl.multiple_of(WINDOW * c, WINDOW), WINDOW)
        for j in range(4):
            ref = heads.at[j, kind, rows]
            arrived(ref, r_hid.at[kind, j])
            send(ref, ref, s_pass, r_pass.at[kind, j], c=1 - c)

    def passed(kind):
        rows = pl.ds(pl.multiple_of(WINDOW * (1 - c), WINDOW), WINDOW)
        for j in range(4):
            arrived(heads.at[j, kind, rows], r_pass.at[kind, j])

    hand_over(1)

    o_step(4)
    arrived(prior.at[few], r_scan.at[2])
    for slot in range(2):
        for i in range(16):
            for half in range(2):
                state[slot, 16 * i : 16 * i + 16, 128 * half : 128 * half + 128] = prior[
                    slot * 32 + i * 2 + half
                ].astype(F32)

        raw = scores[slot] + dot(queries[pl.ds(ROWS * slot, ROWS)], state[slot].astype(BF))
        centred = raw - jnp.mean(raw, axis=-1, keepdims=True)
        variance = jnp.mean(centred * centred, axis=-1, keepdims=True)
        shaped = centred * lax.rsqrt(variance + EPS) * pack[slot, 1:2, :]
        hidden[slot, 0] = shaped.astype(BF)

    hand_over(0)

    for d in range(2):
        rel = (2 * c + d + 3 - x) % 4
        for half in range(2):
            relayed = jnp.logical_and(rel == jnp.where(onward, 0, 2), relay_half == half)

            @pl.when(jnp.logical_not(relayed))
            def _(rel=rel, half=half):
                for n in range(2):
                    arrived(o_near.at[half, n, rel], r_out.at[rel, half, n])

    @pl.when(at_home)
    def _():
        arrived(o_far.at[:, :, 3], r_own_far)

    arrived(o_far.at[1 - c, :, three], r_o_mirror)

    def product(kind, d):
        rel = (2 * c + d + 3 - x) % 4
        total = None
        for half in range(2):
            even = o_near[half, kind, rel, 0:32].reshape(256, 512)
            front = o_near[half, kind, rel, 32:48].reshape(128, 512)
            rear = o_far[half, pl.ds(16 * kind, 16), rel].reshape(128, 512)
            odd_rows = jnp.concatenate([front, rear], axis=0)
            one = dot(heads[2 * half, kind], even) + dot(heads[2 * half + 1, kind], odd_rows)
            total = one if total is None else total + one
        return total

    pass_on(1)
    passed(1)
    for d in range(2):
        partial[d] = product(1, d)

    pass_on(0)
    passed(0)
    for d in range(2):
        out_ref[:, 512 * d : 512 * d + 512] = (partial[d] + product(0, d)).astype(BF)

    arrived(x_in.at[0], s_tok.at[0])
    arrived(tok, s_tok.at[2])
    arrived(w_all.at[pl.ds(0, 54), 0], s_w)
    arrived(w_all.at[few, 0], s_mirror)
    arrived(heads.at[pl.ds(0, 2)], s_pass)
    arrived(rates.at[few], s_scan.at[0])
    arrived(came.at[few], s_scan.at[1])
    arrived(prior.at[few], s_scan.at[2])

    @pl.when(jnp.logical_not(at_home))
    def _():
        arrived(tok, s_tok.at[1])
        arrived(o_far.at[:, :, pl.ds(0, 2)], s_small.at[5])

    @pl.when(at_home)
    def _():
        arrived(own, s_small.at[0])
        arrived(w_all.at[pl.ds(0, 18), 0], s_open)

    arrived(o_near.at[0, :, pl.ds(0, 2)], s_out)
    arrived(o_near.at[0, :, 1], s_relay)
    arrived(o_far.at[0, pl.ds(0, 28), three], s_o)

    @pl.when(holder)
    def _():
        arrived(o_far.at[0, 0, three], s_slice)
        arrived(o_far.at[0, pl.ds(0, 7), three], s_o_near)

    arrived(o_far.at[0, :, three], s_o_mirror)
    for i in range(2):
        mine = jnp.logical_and(at_home, x % 2 == i)

        @pl.when(jnp.logical_not(mine))
        def _(i=i):
            arrived(pack.at[i], s_small.at[1 + i])

        @pl.when(jnp.logical_and(opens, jnp.logical_not(mine)))
        def _(i=i):
            arrived(start, s_small.at[3 + i])

        for kind in range(2):
            for half in range(2):
                here = jnp.logical_and(2 * c + i == x, c == half)

                @pl.when(jnp.logical_not(here))
                def _(i=i, kind=kind, half=half):
                    rows = pl.ds(WINDOW * half, WINDOW)
                    arrived(hidden.at[i, kind, rows], s_hid.at[kind, i, half])

    @pl.when(me < 63)
    def _():
        arrived(tail, s_halo)


def shards(
    tokens,
    norm_gain,
    ret_query,
    ret_key,
    ret_value,
    att_query,
    att_key,
    att_value,
    log_decay,
    start_state,
    ret_gain,
    sink_logits,
    ret_out,
    att_out,
):
    steps = np.arange(128, dtype=np.float32) / np.float32(128)
    inverse = jnp.asarray((np.float32(1) / np.float32(10000) ** steps).reshape(1, 128))
    vmem = pl.BlockSpec(memory_space=pltpu.VMEM)
    hbm = pl.BlockSpec(memory_space=pl.ANY)
    dma = pltpu.SemaphoreType.DMA
    scratch = [
        pltpu.VMEM((ROWS, 1024), BF),
        pltpu.VMEM((2, 2, ROWS, 1024), BF),
        pltpu.VMEM((2 * ROWS, D), BF),
        pltpu.VMEM((64, 2, 16, COLS), BF),
        pltpu.VMEM((2, 8, 256), F32),
        pltpu.VMEM((16, 128), F32),
        pltpu.VMEM((2, 2, 4, 48, 8, 512), BF),
        pltpu.VMEM((2, 32, 4, 8, 512), BF),
        pltpu.VMEM((2, 32, 128), BF),
        pltpu.VMEM((2, 256), F32),
        pltpu.VMEM((1, 512), F32),
        pltpu.VMEM((1, 8), F32),
        pltpu.VMEM((2, 8, 256), F32),
        pltpu.VMEM((1, D), F32),
        pltpu.VMEM((1, 128), F32),
        pltpu.VMEM((2, ROWS, ROWS), F32),
        pltpu.VMEM((2, ROWS, 128), F32),
        pltpu.VMEM((2, ROWS, 128), F32),
        pltpu.VMEM((2, ROWS, 512), F32),
        pltpu.VMEM((ROWS, 128), F32),
        pltpu.VMEM((ROWS, 128), F32),
        pltpu.VMEM((2 * ROWS, 256), BF),
        pltpu.VMEM((2 * ROWS, 256), BF),
        pltpu.VMEM((2 * ROWS, 256), BF),
        pltpu.VMEM((2 * ROWS, 256), BF),
        pltpu.VMEM((2, WINDOW + ROWS, 128), BF),
        pltpu.VMEM((2, 256, 256), F32),
        pltpu.VMEM((2, ROWS, 256), F32),
        pltpu.VMEM((64, 16, 128), BF),
        pltpu.VMEM((64, 16, 128), BF),
        pltpu.VMEM((64, 1, 128), F32),
        pltpu.VMEM((2, 1, 128), F32),
        pltpu.VMEM((64, 16, 128), BF),
        pltpu.VMEM((64, 16, 128), BF),
        pltpu.VMEM((2, 2, ROWS, 256), BF),
        pltpu.VMEM((4, 2, ROWS, 256), BF),
        dma((9,)),
        dma((3,)),
        dma((2, 2, CHUNKS)),
        dma((6,)),
        dma((2,)),
        dma,
        dma,
        dma,
        dma,
        dma((8,)),
        dma((2, 4, 8)),
        dma,
        dma,
        dma((3,)),
        dma((3,)),
        dma,
        dma,
        dma((2, 2, 2)),
        dma((2, 4)),
        dma,
        dma((2, 4)),
        dma,
        dma((4, 2, 2)),
        dma,
        dma,
        dma((3,)),
        dma,
        dma,
        dma,
        dma((4,)),
        dma((2, 4)),
        dma,
        dma,
    ]
    mixed = pl.pallas_call(
        layer_kernel,
        out_shape=pltpu.VMEM((ROWS, 1024), BF),
        in_specs=[hbm] * 15,
        out_specs=vmem,
        scratch_shapes=scratch,
        compiler_params=pltpu.CompilerParams(
            collective_id=0, has_side_effects=True, vmem_limit_bytes=60 * 1024 * 1024
        ),
    )(
        tokens[0],
        ret_key,
        ret_value,
        ret_query,
        att_query,
        att_key,
        att_value,
        log_decay[0],
        ret_gain.reshape(1, 512),
        sink_logits.reshape(1, 8),
        start_state[0],
        ret_out.reshape(64, 8, 512),
        att_out.reshape(64, 8, 512),
        norm_gain.reshape(1, D),
        inverse,
    )
    return mixed[None]


def solution(mesh):
    torus = Mesh(
        mesh.devices.reshape(8, 8, mesh.shape["fs"], mesh.shape["tp"]), ("z", "y", "x", "c")
    )
    across = P(SP, "c")
    in_specs = (
        P("x", SP, "c"),
        P(),
        across,
        across,
        across,
        across,
        across,
        across,
        P("x", "c", SP),
        P("x", "c", None, None),
        P("c"),
        P("c"),
        P("c", "x"),
        P("c", "x"),
    )
    return jax.shard_map(
        shards, mesh=torus, in_specs=in_specs, out_specs=P("x", SP, "c"), check_vma=False
    )
```
